32 devices in a mesh: tp: 8 (over z, core), dp: 4 (over y, x).
Axes of the slice: x: 2, y: 2, z: 4, core: 2. Of those that a mesh axis runs over, the one named last changes fastest.
Arguments:
- tokens: bfloat16 [128, 2048], P(None, 'dp'), may hold values from -21 to 21
- lengths: int32 [8], P('dp'), may hold values from 1 to 16, 42 in all
- input_norm_scale: float32 [2, 2048], P(None, 'dp'), may hold values from 0.1 to 1.9
- gate_input_weight: bfloat16 [2, 2048, 2, 2048], P(None, 'dp', None, 'tp'), may hold values from -0.125 to 0.125
- maps_weight: bfloat16 [2, 2048, 2, 512], P(None, 'dp', None, 'tp'), may hold values from -0.125 to 0.125
- step_weight: bfloat16 [2, 2048, 32], P(None, 'dp', 'tp'), may hold values from -0.125 to 0.125
- input_tap_weight: bfloat16 [2, 4, 2048], P(None, None, 'tp'), may hold values from -3 to 3
- map_tap_weight: bfloat16 [2, 4, 2, 512], P(None, None, None, 'tp'), may hold values from -3 to 3
- step_size_bias: float32 [2, 32], P(None, 'tp'), may hold values from -4 to -1
- decay_rate_logarithm: float32 [2, 32], P(None, 'tp'), may hold values from -2 to 2.5
- direct_path_weight: float32 [2, 32], P(None, 'tp'), may hold values from 0.25 to 2.5
- head_norm_scale: float32 [2, 2048], P(None, 'tp'), may hold values from 0.1 to 1.9
- output_weight: bfloat16 [2, 2048, 2048], P(None, 'tp', 'dp'), may hold values from -0.125 to 0.125
- convolution_input_cache: bfloat16 [2, 8, 3, 2048], P(None, 'dp', None, 'tp'), may hold values from -6 to 6
- convolution_map_cache: bfloat16 [2, 8, 3, 2, 512], P(None, 'dp', None, None, 'tp'), may hold values from -6 to 6
- recurrent_state: float32 [2, 8, 32, 64, 128], P(None, 'dp', 'tp'), may hold values from -6 to 6
- extra_log_decay: float32 [2, 8, 16, 32], P(None, 'dp', None, 'tp'), may hold values from -0.7 to 0, as said below
Outputs:
- stream_out: float32 [128, 2048], P(None, 'dp')
- conv_input_out: bfloat16 [2, 8, 3, 2048], P(None, 'dp', None, 'tp')
- conv_maps_out: bfloat16 [2, 8, 3, 2, 512], P(None, 'dp', None, None, 'tp')
- ssm_out: float32 [2, 8, 32, 64, 128], P(None, 'dp', 'tp')
The draws below stay inside these ranges and needn't reach their ends.
Inputs may be any that keep to these rules, and one draw needn't show every extreme that they name: `extra_log_decay`: zero at most slots, a drop of a fifth to a half of the state at a few.
All inputs are finite; a program needn't handle non-finite values. No bound on the sum of `lengths` on one device may be relied on, other than what follows from the above.
Results may differ from the reference program's by a relative error of at most 0.04.
Values may be sent and summed in bfloat16 or wider, within the bound.
A program may use at most 64 MiB of HBM per device.

```python
import math
import jax
import jax.numpy as jnp
import numpy as np
from jax import lax

D = 2048
STATE_HEADS = 32
P_SIZE = 64
N = 128
G = 4
CONV = 4
TOKEN_SLOTS = 16
MIXER_LAYERS = 2
INNER = 2048
GN = 512
SEQUENCE_COUNT = 8
TOKENS = 128
DP_ROWS = 512
N_DP = 4


def draw_tokens(key, part):
    random_key_first, random_key_second = jax.random.split(key, 2)
    base_draw = jnp.clip(jax.random.normal(random_key_first, (TOKENS, D), jnp.float32), -4.0, 4.0)
    column = jnp.exp(jnp.linspace(math.log(0.5), math.log(3.0), D)) * jax.random.uniform(random_key_second, (D,), jnp.float32, 0.7, 1.0)
    return (base_draw * column[None, :]).astype(jnp.bfloat16)


def draw_extra_log_decay(key, part):
    random_key_first, random_key_second = jax.random.split(key)
    spike_hits = jax.random.randint(random_key_first, (MIXER_LAYERS, SEQUENCE_COUNT, TOKEN_SLOTS, STATE_HEADS), 0, 12) == 0
    spike_depth = jax.random.uniform(random_key_second, (MIXER_LAYERS, SEQUENCE_COUNT, TOKEN_SLOTS, STATE_HEADS), jnp.float32, math.log(0.5), math.log(0.8))
    return jnp.where(spike_hits, spike_depth, 0.0).astype(jnp.float32)


def level_of(own_key, dims, cuts, smallest, largest):
    level, own = 1.0, jax.random.fold_in(own_key, 6)
    for axis_at, shards_of in cuts:
        steps = jnp.exp(jax.random.uniform(jax.random.fold_in(own, axis_at), (shards_of,), jnp.float32, smallest / len(cuts), largest / len(cuts)))
        level = level * jnp.repeat(steps, dims[axis_at] // shards_of).reshape([-1 if axis == axis_at else 1 for axis in range(len(dims))])
    return level


def split_up(number_of, total, reach, slope):
    loads = [(1 << 20) // math.isqrt(grade ** slope) + 1 for grade in range(2, number_of + 1)]
    surplus, holding = total - reach - (number_of - 1), [1] * (number_of - 1)
    while surplus > 0:
        candidates = [i for i in range(number_of - 1) if holding[i] < reach]
        mass, remaining = sum([loads[i] for i in candidates]), surplus
        for i in candidates:
            more = min(reach - holding[i], max(1, remaining * loads[i] // mass), surplus)
            holding[i] = holding[i] + more
            surplus = surplus - more
    return np.array([reach] + holding)


def ragged(stream_key, number_of, total, most, skew):
    if number_of == 2:
        one = jax.random.randint(stream_key, (), max(1, total - most), min(most, total - 1) + 1)
        return jnp.stack([one, total - one])
    sizes = jnp.asarray(split_up(number_of, total, most, skew), jnp.int32)
    twos = (number_of - 1) // 2
    source_of, taker = sizes[1:1 + 2 * twos:2], sizes[2:2 + 2 * twos:2]
    room = jnp.minimum(source_of - 1, most - taker)
    shifted = jax.random.randint(jax.random.fold_in(stream_key, 1), (twos,), 0, 1 << 20) % (room + 1)
    sizes = sizes.at[1:1 + 2 * twos:2].set(source_of - shifted).at[2:2 + 2 * twos:2].set(taker + shifted)
    return sizes[jax.random.permutation(jax.random.fold_in(stream_key, 2), number_of)]


def scatter_about(own_key, dims, spread, bound, pieces=(), held_as=jnp.bfloat16):
    gain = level_of(own_key, dims, pieces, -0.22, 0.18) if pieces else 1.0
    entries = jax.random.normal(own_key, dims, jnp.float32) * spread * gain
    return jnp.minimum(jnp.maximum(entries, -bound), bound).astype(held_as)


def setup_inputs(seed: int = 0) -> dict:
    arg_keys = jax.random.split(jax.random.key(seed), 18)
    return {
        "tokens": draw_tokens(jax.random.fold_in(arg_keys[17], 71), 0),
        "lengths": ragged(arg_keys[1], SEQUENCE_COUNT, SEQUENCE_COUNT * TOKEN_SLOTS // 3, TOKEN_SLOTS, 2).astype(jnp.int32),
        "input_norm_scale": jnp.clip(1.0 + 0.18 * jax.random.normal(arg_keys[2], (MIXER_LAYERS, D), jnp.float32), 0.1, 1.9),
        "gate_input_weight": scatter_about(arg_keys[3], (MIXER_LAYERS, D, 2, INNER), D ** -0.5, 0.125, ((1, 4), (3, 8))),
        "maps_weight": scatter_about(arg_keys[4], (MIXER_LAYERS, D, 2, GN), D ** -0.5, 0.125, ((1, 4), (3, 8))),
        "step_weight": scatter_about(arg_keys[5], (MIXER_LAYERS, D, STATE_HEADS), D ** -0.5, 0.125, ((1, 4), (2, 8))),
        "input_tap_weight": scatter_about(arg_keys[6], (MIXER_LAYERS, CONV, INNER), CONV ** -0.5, 3.0, ((2, 8),)),
        "map_tap_weight": scatter_about(arg_keys[7], (MIXER_LAYERS, CONV, 2, GN), CONV ** -0.5, 3.0, ((3, 8),)),
        "step_size_bias": jnp.clip(-4.0 + 3.0 * jax.random.uniform(arg_keys[8], (MIXER_LAYERS, STATE_HEADS), jnp.float32) ** level_of(arg_keys[8], (MIXER_LAYERS, STATE_HEADS), ((1, 8),), -0.2, 0.2), -4.0, -1.0),
        "decay_rate_logarithm": jnp.clip(-2.0 + 4.5 * jax.random.uniform(arg_keys[9], (MIXER_LAYERS, STATE_HEADS), jnp.float32) ** level_of(arg_keys[9], (MIXER_LAYERS, STATE_HEADS), ((1, 8),), -0.2, 0.2), -2.0, 2.5),
        "direct_path_weight": jnp.clip(jnp.exp(math.log(2.5) - 2.3025851 * jax.random.uniform(arg_keys[10], (MIXER_LAYERS, STATE_HEADS), jnp.float32) ** level_of(arg_keys[10], (MIXER_LAYERS, STATE_HEADS), ((1, 8),), -0.2, 0.2)), 0.25, 2.5),
        "head_norm_scale": jnp.clip(1.0 + 0.18 * jax.random.normal(arg_keys[11], (MIXER_LAYERS, INNER), jnp.float32), 0.1, 1.9),
        "output_weight": scatter_about(arg_keys[12], (MIXER_LAYERS, INNER, D), INNER ** -0.5, 0.125, ((1, 8), (2, 4))),
        "convolution_input_cache": scatter_about(arg_keys[13], (MIXER_LAYERS, SEQUENCE_COUNT, 3, INNER), 1.0, 6.0, ((1, 4), (3, 8))),
        "convolution_map_cache": scatter_about(arg_keys[14], (MIXER_LAYERS, SEQUENCE_COUNT, 3, 2, GN), 1.0, 6.0, ((1, 4), (4, 8))),
        "recurrent_state": scatter_about(arg_keys[15], (MIXER_LAYERS, SEQUENCE_COUNT, STATE_HEADS, P_SIZE, N), 1.0, 6.0, ((1, 4), (2, 8)), jnp.float32),
        "extra_log_decay": draw_extra_log_decay(jax.random.fold_in(arg_keys[17], 71), 0),
    }


epsilon = 1e-06
highest = lax.Precision.HIGHEST

def conv_step(previous, incoming, weights, lengths):
    padded = jnp.concatenate([previous, incoming], axis=1).astype(jnp.float32)
    taps = weights.shape[0]
    fresh_tokens = incoming.shape[1]
    filtered = padded[:, :fresh_tokens] * weights[0].astype(jnp.float32)
    for tap_index in range(1, taps):
        filtered = filtered + padded[:, tap_index:tap_index + fresh_tokens] * weights[tap_index].astype(jnp.float32)
    position = jnp.arange(fresh_tokens + taps - 1, dtype=jnp.int32)
    wanted = lengths[:, None] + jnp.arange(taps - 1, dtype=jnp.int32)[None, :]
    chooser = (position[None, None, :] == wanted[:, :, None]).astype(jnp.float32)
    kept_rows = jnp.einsum('skp,sp...->sk...', chooser, padded, precision=highest)
    return (jax.nn.silu(filtered), kept_rows.astype(jnp.bfloat16))

def ssd_block(head_input, head_gate, head_step_size, decay_logarithm, write_map, read_map, state_old, skip, gain_heads):
    decay_sum = jnp.cumsum(decay_logarithm, axis=1)
    slots = decay_logarithm.shape[1]
    causal = jnp.arange(slots)[:, None] >= jnp.arange(slots)[None, :]
    decay_gap = decay_sum[:, :, None, :] - decay_sum[:, None, :, :]
    segment = jnp.exp(jnp.where(causal[None, :, :, None], decay_gap, -jnp.inf))
    intersection = jnp.einsum('slhn,smhn->slmh', read_map, write_map, precision=highest)
    within = jnp.einsum('slmh,smh,smhp->slhp', intersection * segment, head_step_size, head_input, precision=highest)
    carried = jnp.einsum('slhn,shpn->slhp', read_map, state_old, precision=highest) * jnp.exp(decay_sum)[..., None]
    to_end = jnp.exp(decay_sum[:, -1:, :] - decay_sum)
    state_new = jnp.exp(decay_sum[:, -1])[..., None, None] * state_old + jnp.einsum('smhn,smh,smhp->shpn', write_map, to_end * head_step_size, head_input, precision=highest)
    mixed_out = within + carried + skip[:, None] * head_input
    mixed_out = mixed_out * jax.nn.silu(head_gate)
    mixed_out = mixed_out * lax.rsqrt(lax.optimization_barrier(jnp.mean(mixed_out * mixed_out, axis=-1, keepdims=True)) + epsilon) * gain_heads
    return (mixed_out, state_new)

def reference(tokens, lengths, input_norm_scale, gate_input_weight, maps_weight, step_weight, input_tap_weight, map_tap_weight, step_size_bias, decay_rate_logarithm, direct_path_weight, head_norm_scale, output_weight, convolution_input_cache, convolution_map_cache, recurrent_state, extra_log_decay):
    stream = tokens.astype(jnp.float32)
    active_mask = (jnp.arange(TOKEN_SLOTS, dtype=jnp.int32)[None, :] < lengths[:, None]).astype(jnp.float32)
    input_states, map_states, ssm_states = ([], [], [])
    per_group = STATE_HEADS // G
    for layer_number in range(MIXER_LAYERS):
        stream_f = stream
        factor = lax.rsqrt(lax.optimization_barrier(jnp.sum(stream_f * stream_f, axis=1, keepdims=True)) / D + epsilon)
        normed = (stream_f * input_norm_scale[layer_number]).astype(jnp.bfloat16)
        weight_all = jnp.concatenate([gate_input_weight[layer_number].reshape(D, 2 * INNER), maps_weight[layer_number].reshape(D, 2 * GN), step_weight[layer_number]], axis=1)
        total_cols = weight_all.shape[1]
        row_pieces = normed.reshape(TOKENS, N_DP, DP_ROWS).transpose(1, 0, 2)
        weight_pieces = weight_all.reshape(N_DP, DP_ROWS, total_cols)

        def add_block(running, pair_item):
            partial_prod = jnp.dot(pair_item[0], pair_item[1], preferred_element_type=jnp.float32)
            rounded = lax.optimization_barrier(partial_prod.astype(jnp.bfloat16))
            return (running + rounded.astype(jnp.float32), None)
        proj_sum, _ = lax.scan(add_block, jnp.zeros((TOKENS, total_cols), jnp.float32), (row_pieces, weight_pieces))
        projected = (proj_sum * factor).astype(jnp.bfloat16)
        gate_input = projected[:, :2 * INNER].reshape(SEQUENCE_COUNT, TOKEN_SLOTS, 2, INNER)
        map_input = projected[:, 2 * INNER:2 * INNER + 2 * GN].reshape(SEQUENCE_COUNT, TOKEN_SLOTS, 2, GN)
        step_raw = projected[:, 2 * INNER + 2 * GN:].reshape(SEQUENCE_COUNT, TOKEN_SLOTS, STATE_HEADS)
        conv_input, input_kept = conv_step(convolution_input_cache[layer_number], gate_input[:, :, 1], input_tap_weight[layer_number], lengths)
        maps_f, maps_kept = conv_step(convolution_map_cache[layer_number], map_input, map_tap_weight[layer_number], lengths)
        maps = maps_f.astype(jnp.bfloat16)
        write_groups = maps[:, :, 0].reshape(SEQUENCE_COUNT, TOKEN_SLOTS, N, G).transpose(0, 1, 3, 2)
        read_groups = maps[:, :, 1].reshape(SEQUENCE_COUNT, TOKEN_SLOTS, N, G).transpose(0, 1, 3, 2)
        write_map = jnp.repeat(write_groups, per_group, axis=2).astype(jnp.float32)
        read_map = jnp.repeat(read_groups, per_group, axis=2).astype(jnp.float32)
        head_step_size = jax.nn.softplus(step_raw.astype(jnp.float32) + step_size_bias[layer_number]) * active_mask[..., None]
        decay_logarithm = head_step_size * -jnp.exp(decay_rate_logarithm[layer_number]) + extra_log_decay[layer_number] * active_mask[..., None]
        head_input = conv_input.reshape(SEQUENCE_COUNT, TOKEN_SLOTS, STATE_HEADS, P_SIZE)
        head_gate = gate_input[:, :, 0].astype(jnp.float32).reshape(SEQUENCE_COUNT, TOKEN_SLOTS, STATE_HEADS, P_SIZE)
        mixed_out, state_new = ssd_block(head_input, head_gate, head_step_size, decay_logarithm, write_map, read_map, recurrent_state[layer_number], direct_path_weight[layer_number], head_norm_scale[layer_number].reshape(STATE_HEADS, P_SIZE))
        head_out = (mixed_out * active_mask[:, :, None, None]).astype(jnp.bfloat16).reshape(TOKENS, INNER)
        projected_out = jnp.dot(head_out, output_weight[layer_number], preferred_element_type=jnp.float32)
        stream = stream_f + projected_out
        input_states.append(input_kept)
        map_states.append(maps_kept)
        ssm_states.append(state_new)
    return (stream, jnp.stack(input_states), jnp.stack(map_states), jnp.stack(ssm_states))
```

```python
import functools

import jax
import jax.numpy as jnp
from jax import lax
from jax.experimental import pallas as pl
from jax.experimental.pallas import tpu as pltpu
from jax.sharding import PartitionSpec as P

EPS = 1e-06
LANES = 128
FRONT = 8
F32, BF16 = jnp.float32, jnp.bfloat16


def up(n):
    return -(-n // LANES) * LANES


def dot(a, b, ca=1, cb=0):
    return lax.dot_general(a, b, (((ca,), (cb,)), ((), ())), preferred_element_type=F32)


def thirds(a):
    high = a.astype(BF16)
    rest = a - high.astype(F32)
    middle = rest.astype(BF16)
    return high, middle, (rest - middle.astype(F32)).astype(BF16)


def grid(n_rows, n_cols):
    return (
        lax.broadcasted_iota(jnp.int32, (n_rows, n_cols), 0),
        lax.broadcasted_iota(jnp.int32, (n_rows, n_cols), 1),
    )


def over(a, n):
    return lax.shift_right_logical(a, jnp.full_like(a, n.bit_length() - 1))


def ones_where(cond):
    return jnp.where(cond, 1.0, 0.0).astype(BF16)


def far_first(k, me, n):
    upper = me // (n // 2)
    mirrored = n - 1 - me
    return upper * (k + (k - me + n) // n) + (1 - upper) * (n - 1 - k - (k - mirrored + n) // n)


def general_kernel(
    n_tp, n_dp, d_model, heads, groups, slots, seqs, hp_cols, map_cols,
    lens, x, scale, w_pair, w_maps, w_step, tap_u, tap_m, bias, rate, skip, gain, cache_u, cache_m, extra_t,
    state_hbm, wout_hbm,
    stream, kept, ssm,
    a_send, a_recv, m_send, m_recv, h_send, h_recv, o_send, o_recv, n_send, n_recv, padded, step_w, state, wout, taps, par, extra,
    a_ss, a_rs, m_ss, m_rs, h_ss, h_rs, o_ss, o_rs, n_ss, n_rs, s_sem, w_sem,
):
    tp, dp = lax.axis_index("tp"), lax.axis_index("dp")
    layers = w_pair.shape[0]
    rows = seqs * slots
    taps_n = tap_u.shape[1]
    keep = taps_n - 1
    zc = up(hp_cols)
    ng = map_cols // groups
    n_state = state.shape[-1]
    cut = stream.shape[0] // n_tp
    per = rows // cut
    head_size = hp_cols // heads

    state_copy = pltpu.make_async_copy(state_hbm, state, s_sem)
    wout_copy = pltpu.make_async_copy(wout_hbm, wout, w_sem)
    state_copy.start()
    wout_copy.start()
    barrier = pltpu.get_barrier_semaphore()
    for k in range(1, n_dp):
        pl.semaphore_signal(barrier, inc=1, device_id={"dp": lax.rem(dp + k, n_dp)})
    for k in range(1, n_tp):
        pl.semaphore_signal(barrier, inc=1, device_id={"tp": lax.rem(tp + k, n_tp)})

    stream[...] = x[...].astype(F32)
    slot = lax.broadcasted_iota(jnp.int32, (slots, 1), 0)
    mask = jnp.concatenate([(slot < lens[s]).astype(F32) for s in range(seqs)], axis=0)
    lane = lax.broadcasted_iota(jnp.int32, (1, LANES), 1)
    r, c = grid(rows, rows)
    causal = (over(r, slots) == over(c, slots)) & (c <= r)
    tri = ones_where(causal)
    r, c = grid(2 * map_cols, up(2 * map_cols))
    which = over(r, ng) & 1
    sel = ones_where(c == which * map_cols + groups * (r & (ng - 1)) + over(r, 2 * ng))
    r, c = grid(n_tp * 2 * ng, 2 * n_state)
    sel2 = ones_where(c == (over(r, ng) & 1) * n_state + over(r, 2 * ng) * ng + (r & (ng - 1)))
    r, c = grid(LANES, hp_cols)
    ex = ones_where(r == over(c, head_size))
    r, c = grid(hp_cols, LANES)
    ext = ones_where(c == over(r, head_size))
    r, c = grid(hp_cols, hp_cols)
    ones = ones_where(over(r, head_size) == over(c, head_size))
    r, c = grid(LANES, 2 * LANES)
    spread = ones_where(c == 2 * r)
    padded[...] = jnp.zeros_like(padded)
    step_w[...] = jnp.zeros_like(step_w)
    taps[...] = jnp.zeros_like(taps)
    par[...] = jnp.zeros_like(par)
    extra[...] = jnp.zeros_like(extra)
    for l in range(layers):
        step_w[l, :heads, :] = w_step[l]
        taps[l, :taps_n, :hp_cols] = tap_u[l].astype(F32)
        for t in range(taps_n):
            pair = tap_m[l, t].astype(F32)
            for which in range(2):
                at = zc + which * map_cols
                taps[l, t : t + 1, at : at + map_cols] = pair[which : which + 1]
        par[l, 0:1, :heads] = bias[l : l + 1, :]
        par[l, 1:2, :heads] = rate[l : l + 1, :]
        par[l, 2:3, :heads] = skip[l : l + 1, :]
        for s in range(seqs):
            extra[l, :heads, s * slots : (s + 1) * slots] = extra_t[l, s]
    extra_rows = [extra[l].T[:rows] for l in range(layers)]
    skip_x = [sum(dot(piece, ex) for piece in thirds(par[l]))[2:3] for l in range(layers)]
    sends = []

    def copy(src, dst, ss, rs, where):
        return pltpu.make_async_remote_copy(
            src_ref=src, dst_ref=dst, send_sem=ss, recv_sem=rs, device_id=where
        )

    for l in range(layers):
        st = stream[...]
        squares = jnp.sum(st * st, axis=1, keepdims=True)
        normed = (st * scale[l : l + 1, :]).astype(BF16)
        even = jnp.concatenate(
            [dot(normed[:, i : i + LANES], spread) for i in range(0, normed.shape[1], LANES)], axis=1
        )
        odd = pltpu.roll(even, 1, 1)
        pair = dot(jnp.concatenate([even.astype(BF16), odd.astype(BF16)], axis=0), w_pair[l])
        tokens = st.shape[0]
        tail = dot(normed, step_w[l], 1, 1)
        high = squares.astype(BF16).astype(F32)
        tail = jnp.where(lane == LANES - 2, high, jnp.where(lane == LANES - 1, squares - high, tail))
        part = jnp.concatenate(
            [pair[:tokens], pair[tokens:], dot(normed, w_maps[l], 1, 1), tail], axis=1
        ).astype(BF16)
        for b in range(n_dp):
            a_send[l, b] = part[b * rows : (b + 1) * rows]
        if l == 0:
            pl.semaphore_wait(barrier, n_dp - 1 + n_tp - 1)
        flights = []
        for k in range(1, n_dp):
            to = lax.rem(dp + k, n_dp)
            c = copy(a_send.at[l, to], a_recv.at[l, k - 1], a_ss.at[l, k - 1], a_rs.at[l, k - 1], {"dp": to})
            c.start()
            flights.append(c)
        sends += flights
        acc = a_send[l, dp].astype(F32)
        for k, c in enumerate(flights):
            c.wait_recv()
            acc = acc + a_recv[l, k].astype(F32)
        tail = acc[:, acc.shape[1] - LANES :]
        squares = tail[:, LANES - 2 : LANES - 1] + tail[:, LANES - 1 : LANES]
        factor = lax.rsqrt(squares / d_model + EPS)
        proj = (acc * factor).astype(BF16).astype(F32)

        conv_w = taps.shape[2]
        pieces = []
        for s in range(seqs):
            for t in range(keep):
                at = FRONT - keep + t
                padded[s, at : at + 1, :hp_cols] = cache_u[l, t].astype(F32)[s : s + 1]
                pair = cache_m[l, s, t].astype(F32)
                for which in range(2):
                    col = zc + which * map_cols
                    padded[s, at : at + 1, col : col + map_cols] = pair[which : which + 1]
            padded[s, FRONT : FRONT + slots, :] = proj[s * slots : (s + 1) * slots, zc : zc + conv_w]
            total = padded[s, FRONT - keep : FRONT - keep + slots, :] * taps[l, 0:1, :]
            for t in range(1, taps_n):
                at = FRONT - keep + t
                total = total + padded[s, at : at + slots, :] * taps[l, t : t + 1, :]
            pieces.append(total)
        filtered = jnp.concatenate(pieces, axis=0)
        filtered = filtered * jax.nn.sigmoid(filtered)
        maps = filtered[:, conv_w - up(2 * map_cols) :].astype(BF16)
        sorted_maps = dot(sel, maps, 1, 1)
        for g in range(groups):
            m_send[l, g] = sorted_maps[g * 2 * ng : (g + 1) * 2 * ng, :].astype(BF16)

        def group_of(rank):
            return rank * heads // (heads * n_tp // groups)

        flights = []
        for k in range(n_tp - 1):
            to = far_first(k, tp, n_tp)
            c = copy(m_send.at[l, group_of(to)], m_recv.at[l, tp], m_ss.at[l, k], m_rs.at[l, tp], {"tp": to})
            c.start()
            sends.append(c)
        m_recv[l, tp] = m_send[l, group_of(tp)]

        for s in range(seqs):
            pick = lax.broadcasted_iota(jnp.int32, (8, FRONT + slots), 0)
            place = lax.broadcasted_iota(jnp.int32, (8, FRONT + slots), 1)
            chooser = ((place == pick + lens[s] + (FRONT - keep)) & (pick < keep)).astype(BF16)
            kept[l, s] = dot(chooser, padded[s].astype(BF16)).astype(BF16)
        raw = proj[:, proj.shape[1] - LANES :] + par[l, 0:1, :]
        step = (jnp.maximum(raw, 0.0) + jnp.log1p(jnp.exp(-jnp.abs(raw)))) * mask
        step = jnp.where(lane < heads, step, 0.0)
        logdec = extra_rows[l] * mask - step * jnp.exp(par[l, 1:2, :])
        logdec = jnp.where(lane < heads, logdec, 0.0)
        parts = dot(tri, jnp.concatenate(thirds(logdec), axis=1))
        sums = parts[:, :LANES] + parts[:, LANES : 2 * LANES] + parts[:, 2 * LANES :]
        sums_t = sums.T
        step_t = step.T
        sums_parts, step_parts = thirds(sums), thirds(step)
        both = dot(jnp.concatenate(sums_parts + step_parts, axis=0), ex)
        sums_x = both[:rows] + both[rows : 2 * rows] + both[2 * rows : 3 * rows]
        step_x = both[3 * rows : 4 * rows] + both[4 * rows : 5 * rows] + both[5 * rows :]
        inp = filtered[:, :hp_cols]
        gate = proj[:, :hp_cols]
        last_x = jnp.concatenate(
            [
                jnp.broadcast_to(sums_x[(s + 1) * slots - 1 : (s + 1) * slots, :], (slots, hp_cols))
                for s in range(seqs)
            ],
            axis=0,
        )
        weighted = (jnp.exp(last_x - sums_x) * step_x * inp).astype(BF16)
        inp_b = inp.astype(BF16)
        grow = jnp.exp(sums_x)
        direct = skip_x[l] * inp
        gate = gate * jax.nn.sigmoid(gate)
        rows_sum = sum(dot(ext, piece, 1, 1) for piece in sums_parts)
        segs = []
        for h in range(heads):
            gap = sums[:, h : h + 1] - sums_t[h : h + 1, :]
            segs.append(jnp.exp(jnp.where(causal, gap, -jnp.inf)) * step_t[h : h + 1, :])

        if l == 0:
            state_copy.wait()
            wout_copy.wait()
        for k in range(1, n_tp):
            src = lax.rem(tp + n_tp - k, n_tp)
            copy(m_send.at[l, 0], m_recv.at[l, src], m_ss.at[l, 0], m_rs.at[l, src], {"tp": src}).wait_recv()
        got = m_recv[l].astype(F32).reshape(n_tp * 2 * ng, rows)
        both_maps = dot(got.T.astype(BF16), sel2).astype(BF16)
        b_map, c_map = both_maps[:, :n_state], both_maps[:, n_state:]
        cross = dot(c_map, b_map, 1, 1)
        within = jnp.concatenate(
            [
                dot((cross * segs[h]).astype(BF16), inp_b[:, h * head_size : (h + 1) * head_size])
                for h in range(heads)
            ],
            axis=1,
        )
        carried = jnp.concatenate(
            [
                dot(c_map[s * slots : (s + 1) * slots], state[l, s].astype(BF16), 1, 1)
                for s in range(seqs)
            ],
            axis=0,
        )
        read = (within + carried * grow + direct) * gate
        power = read * read
        p_hi = power.astype(BF16)
        p_lo = (power - p_hi.astype(F32)).astype(BF16)
        mean = (dot(p_hi, ones) + dot(p_lo, ones)) / head_size
        headout = (read * lax.rsqrt(mean + EPS) * gain[l : l + 1, :] * mask).astype(BF16)
        h_send[l] = headout
        flights = []
        for k in range(1, n_dp):
            to = lax.rem(dp + k, n_dp)
            c = copy(h_send.at[l], h_recv.at[l, k - 1], h_ss.at[l, k - 1], h_rs.at[l, k - 1], {"dp": to})
            c.start()
            flights.append(c)
        sends += flights

        def push(value, block):
            out = dot(value, wout[l]).astype(BF16)
            for i in range(per):
                to = block * per + i
                o_send[l, to] = out[i * cut : (i + 1) * cut]

                @pl.when(to != tp)
                def _():
                    copy(o_send.at[l, to], o_recv.at[l, tp], o_ss.at[l, to], o_rs.at[l, tp], {"tp": to}).start()

        push(headout, dp)
        for s in range(seqs):
            at = slice(s * slots, (s + 1) * slots)
            fresh = dot(weighted[at], b_map[at], 0, 0)
            end = (s + 1) * slots - 1
            ssm[l, s] = jnp.exp(rows_sum[:, end : end + 1]) * state[l, s] + fresh
        for k, c in enumerate(flights):
            c.wait_recv()
            push(h_recv[l, k], lax.rem(dp + n_dp - k - 1, n_dp))
        total = o_send[l, tp].astype(F32)
        for k in range(1, n_tp):
            src = lax.rem(tp + n_tp - k, n_tp)
            copy(o_send.at[l, src], o_recv.at[l, src], o_ss.at[l, src], o_rs.at[l, src], {"tp": src}).wait_recv()
            total = total + o_recv[l, src].astype(F32)
        fresh = total.astype(BF16)
        n_send[l] = fresh
        n_recv[l, tp] = fresh
        for k in range(n_tp - 1):
            to = far_first(k, tp, n_tp)
            c = copy(n_send.at[l], n_recv.at[l, tp], n_ss.at[l, k], n_rs.at[l, tp], {"tp": to})
            c.start()
            sends.append(c)
        for k in range(1, n_tp):
            src = lax.rem(tp + n_tp - k, n_tp)
            copy(n_send.at[l], n_recv.at[l, src], n_ss.at[l, 0], n_rs.at[l, src], {"tp": src}).wait_recv()
        stream[...] += n_recv[l].astype(F32).reshape(stream.shape)

    for c in sends:
        c.wait_send()
    for l in range(layers):
        for k in range(1, n_tp):
            to = lax.rem(tp + k, n_tp)
            copy(o_send.at[l, to], o_recv.at[l, tp], o_ss.at[l, to], o_rs.at[l, tp], {"tp": to}).wait_send()


def general_body(
    n_tp, n_dp,
    tokens, lengths, input_norm_scale, gate_input_weight, maps_weight, step_weight,
    input_tap_weight, map_tap_weight, step_size_bias, decay_rate_logarithm, direct_path_weight,
    head_norm_scale, output_weight, convolution_input_cache, convolution_map_cache,
    recurrent_state, extra_log_decay,
):
    layers, seqs, slots, heads = extra_log_decay.shape
    head_size, n_state = recurrent_state.shape[3:]
    hp_cols = heads * head_size
    map_cols = maps_weight.shape[3]
    groups = map_cols * n_tp // n_state
    ng = map_cols // groups
    rows = seqs * slots
    d_here = tokens.shape[1]
    keep = convolution_input_cache.shape[2]

    def wide(a):
        pad = up(a.shape[-1]) - a.shape[-1]
        return a if pad == 0 else jnp.pad(a, [(0, 0)] * (a.ndim - 1) + [(0, pad)])

    w_pair = wide(gate_input_weight.reshape(layers, 2 * d_here, hp_cols))
    w_maps = jnp.transpose(maps_weight, (0, 2, 3, 1)).reshape(layers, 2 * map_cols, d_here)
    if up(2 * map_cols) > 2 * map_cols:
        w_maps = jnp.pad(w_maps, ((0, 0), (0, up(2 * map_cols) - 2 * map_cols), (0, 0)))
    w_step = jnp.transpose(step_weight, (0, 2, 1))
    cache_u = jnp.transpose(convolution_input_cache, (0, 2, 1, 3))
    extra_t = jnp.transpose(extra_log_decay, (0, 1, 3, 2))
    state = recurrent_state.reshape(layers, seqs, hp_cols, n_state)

    vmem = pl.BlockSpec(memory_space=pltpu.VMEM)
    wide_cols = 2 * up(hp_cols) + up(2 * map_cols) + LANES
    anywhere = pl.BlockSpec(memory_space=pl.ANY)
    conv_w = up(hp_cols) + up(2 * map_cols)
    cut = tokens.shape[0] // n_tp
    sems = lambda n: pltpu.SemaphoreType.DMA((layers, n))
    args = [tokens, input_norm_scale, w_pair, w_maps, w_step, input_tap_weight,
        map_tap_weight, step_size_bias, decay_rate_logarithm, direct_path_weight, head_norm_scale,
        cache_u, convolution_map_cache, extra_t]
    stream, kept, ssm = pl.pallas_call(
        functools.partial(
            general_kernel, n_tp, n_dp, d_here * n_dp, heads, groups, slots, seqs, hp_cols, map_cols
        ),
        out_shape=(
            jax.ShapeDtypeStruct(tokens.shape, F32),
            jax.ShapeDtypeStruct((layers, seqs, 8, conv_w), BF16),
            jax.ShapeDtypeStruct(state.shape, F32),
        ),
        in_specs=[pl.BlockSpec(memory_space=pltpu.SMEM)] + [vmem] * len(args) + [anywhere] * 2,
        out_specs=(vmem, vmem, vmem),
        scratch_shapes=[
            pltpu.VMEM((layers, n_dp, rows, wide_cols), BF16),
            pltpu.VMEM((layers, n_dp - 1, rows, wide_cols), BF16),
            pltpu.VMEM((layers, groups, 2 * ng, rows), BF16),
            pltpu.VMEM((layers, n_tp, 2 * ng, rows), BF16),
            pltpu.VMEM((layers, rows, hp_cols), BF16),
            pltpu.VMEM((layers, n_dp - 1, rows, hp_cols), BF16),
            pltpu.VMEM((layers, n_tp, cut, d_here), BF16),
            pltpu.VMEM((layers, n_tp, cut, d_here), BF16),
            pltpu.VMEM((layers, cut, d_here), BF16),
            pltpu.VMEM((layers, n_tp, cut, d_here), BF16),
            pltpu.VMEM((seqs, FRONT + slots, conv_w), F32),
            pltpu.VMEM((layers, LANES, d_here), BF16),
            pltpu.VMEM(state.shape, F32),
            pltpu.VMEM(output_weight.shape, BF16),
            pltpu.VMEM((layers, 8, conv_w), F32),
            pltpu.VMEM((layers, 8, LANES), F32),
            pltpu.VMEM((layers, LANES, LANES), F32),
            sems(n_dp - 1), sems(n_dp - 1), sems(n_tp - 1), sems(n_tp), sems(n_dp - 1),
            sems(n_dp - 1), sems(n_tp), sems(n_tp), sems(n_tp - 1), sems(n_tp),
            pltpu.SemaphoreType.DMA, pltpu.SemaphoreType.DMA,
        ],
        compiler_params=pltpu.CompilerParams(
            collective_id=0, has_side_effects=True, vmem_limit_bytes=48 * 2**20
        ),
        name="mixer",
    )(lengths, *args, state, output_weight)
    conv_in = kept[:, :, :keep, :hp_cols]
    start = conv_w - up(2 * map_cols)
    conv_maps = kept[:, :, :keep, start : start + 2 * map_cols].reshape(
        layers, seqs, keep, 2, map_cols
    )
    return stream, conv_in, conv_maps, ssm.reshape(recurrent_state.shape)


def peers(n, order):
    return [k for k in order if 0 < k < n] + [k for k in range(1, n) if k not in order]


def kernel(
    n_tp, n_dp, d_model, groups, shapes,
    *refs,
):
    names = (
        "lens", "x", "scale", "gate", "w_maps", "w_step", "tap_u", "tap_m", "bias", "rate", "skip", "gain",
        "cache_u", "cache_m", "extra_t", "state", "wout",
    )
    hbm = dict(zip(names, refs[: len(names)]))
    (
        stream, kept_u, kept_m, ssm,
        lens, x, scale, w_gate, w_maps, w_step, tap_u, tap_m, bias, rate, skip, gain, cache_u, cache_m, extra_t, state,
        wout, in_sem, g_sem,
        a_send, a_recv, m_send, m_recv, c_send, c_recv, h_recv, o_send, o_recv, nb,
        padded, padded_m, mrow, mrows, step_w, w_sorted, taps, par, extra,
        a_ss, a_rs, m_ss, m_rs, c_ss, c_rs, h_ss, h_rs, o_ss, o_rs, n_ss, n_rs, w_ss, w_rs,
    ) = refs[len(names) :]
    layers, seqs, slots, heads, head_size, n_state, hp_cols, map_cols = shapes
    tp, dp = lax.axis_index("tp"), lax.axis_index("dp")
    rows = seqs * slots
    taps_n = tap_u.shape[1]
    keep = taps_n - 1
    ng = map_cols // groups
    pair_cols = 2 * ng
    quads = LANES // pair_cols
    d_here = x.shape[1]
    half = d_here // 2
    tokens = x.shape[0]
    side = lax.rem(tp, 2)
    zed = lax.div(tp, 2)
    n_z = n_tp // 2
    every = n_tp * n_dp
    me = dp * n_tp + tp
    dp_peers = peers(n_dp, (3, 1, 2))
    near_first = peers(n_dp, (1, 2, 3))
    z_peers = peers(n_z, (3, 2, 1))

    def remote(src, dst, ss, rs, where):
        return pltpu.make_async_remote_copy(
            src_ref=src, dst_ref=dst, send_sem=ss, recv_sem=rs, device_id=where
        )

    barrier = pltpu.get_barrier_semaphore()
    others = [
        (i, j) for i in [*peers(n_tp, (6, 7, 4, 5, 2, 3, 1)), 0] for j in [*dp_peers, 0] if i or j
    ]

    def at(i, j):
        return {"tp": jnp.bitwise_xor(tp, i), "dp": jnp.bitwise_xor(dp, j)}

    for i, j in others:
        pl.semaphore_signal(barrier, inc=1, device_id=at(i, j))

    local = {}
    pairs = dict(
        x=x, scale=scale, w_maps=w_maps, w_step=w_step, lens=lens, tap_u=tap_u, tap_m=tap_m, bias=bias, rate=rate,
        skip=skip, gain=gain, cache_u=cache_u, cache_m=cache_m, extra_t=extra_t, state=state,
    )
    for n, name in enumerate(pairs):
        local[name] = pltpu.make_async_copy(hbm[name], pairs[name], in_sem.at[n])
    mine = pl.ds(pl.multiple_of(side * half, LANES), half)
    theirs = pl.ds(pl.multiple_of((1 - side) * half, LANES), half)
    local["wout"] = pltpu.make_async_copy(hbm["wout"].at[:, :, mine], wout.at[:, 0], in_sem.at[len(pairs)])
    gate_copies = [
        [
            pltpu.make_async_copy(
                hbm["gate"].at[l, :, :, i : i + LANES], w_gate.at[l, i // LANES], g_sem.at[l, i // LANES]
            )
            for i in range(0, hp_cols, LANES)
        ]
        for l in range(layers)
    ]
    first = ("x", "scale", "w_maps", "w_step")
    for name in first:
        local[name].start()
    for c in gate_copies[0]:
        c.start()
    for name in local:
        if name not in first:
            local[name].start()
    for l in range(1, layers):
        for c in gate_copies[l]:
            c.start()

    lane = lax.broadcasted_iota(jnp.int32, (1, LANES), 1)
    r, c = grid(LANES, 4 * LANES)
    spread = ones_where(c == jnp.where(c < 2 * LANES, 2 * r, 2 * LANES + 2 * r + 1))
    r, c = grid(LANES, LANES)
    place = (c + LANES - ng * tp) & (LANES - 1)
    wanted = (over(place, ng) & 1) * map_cols + groups * (place & (ng - 1)) + over(place, pair_cols)
    sorter = ones_where(r == wanted)
    home = over((lane + LANES - ng * tp) & (LANES - 1), pair_cols)
    step_w[...] = jnp.zeros_like(step_w)
    gate_rows = w_gate.reshape(layers, hp_cols // LANES, 2 * d_here, LANES)

    def group_of(rank):
        return rank * groups // n_tp

    def project(l):
        st = stream[...]
        squares = jnp.sum(st * st, axis=1, keepdims=True)
        normed = (st * scale[l : l + 1, :]).astype(BF16)
        raw = dot(normed, w_sorted[l], 1, 1)
        turned = [raw if k == 0 else pltpu.roll(raw, k * pair_cols, 1) for k in range(quads)]
        turned = [t.reshape(n_dp, quads, 8, LANES) for t in turned]
        for g in range(groups):
            piece = turned[(0 - g) % quads][:, 0]
            for q in range(1, quads):
                piece = jnp.where((home == q)[None], turned[(q - g) % quads][:, q], piece)
            m_send[l, g] = piece.astype(BF16)
        return normed, squares, raw

    def send_maps(l):
        for i, j in others:
            to = at(i, j)
            remote(
                m_send.at[l, group_of(to["tp"]), to["dp"]], m_recv.at[l, me], m_ss.at[l], m_rs.at[l], to
            ).start()
        m_recv[l, me] = m_send[l, group_of(tp), dp]

    def project_rest(l, normed, squares, raw):
        spreads = [dot(normed[:, i : i + LANES], spread).astype(BF16) for i in range(0, d_here, LANES)]
        even = jnp.concatenate([s[:, : 2 * LANES] for s in spreads], axis=1)
        odd = jnp.concatenate([s[:, 2 * LANES :] for s in spreads], axis=1)
        for c in gate_copies[l]:
            c.wait()
        weight = jnp.concatenate([gate_rows[l, i] for i in range(hp_cols // LANES)], axis=1)
        both = dot(jnp.concatenate([odd, even], axis=0), weight)
        tail = dot(normed, step_w[l], 1, 1)
        high = squares.astype(BF16).astype(F32)
        tail = jnp.where(lane == LANES - 2, high, jnp.where(lane == LANES - 1, squares - high, tail))
        one = jnp.concatenate([both[:tokens], tail], axis=1).astype(BF16)
        two = jnp.concatenate([both[tokens:], raw], axis=1).astype(BF16)
        for b in range(n_dp):
            a_send[l, 0, b] = one[b * rows : (b + 1) * rows]
            a_send[l, 1, b] = two[b * rows : (b + 1) * rows]

    def send_rest(l):
        for p in range(2):
            for k in dp_peers:
                to = jnp.bitwise_xor(dp, k)
                remote(
                    a_send.at[l, p, to], a_recv.at[l, p, k - 1], a_ss.at[l, p, k - 1], a_rs.at[l, p, k - 1], {"dp": to}
                ).start()

    def await_rest(l, p):
        acc = a_send[l, p, dp].astype(F32)
        for k in dp_peers:
            remote(
                a_send.at[l, p, 0], a_recv.at[l, p, k - 1], a_ss.at[l, p, k - 1], a_rs.at[l, p, k - 1],
                {"dp": jnp.bitwise_xor(dp, k)},
            ).wait_recv()
        for k in range(1, n_dp):
            acc = acc + a_recv[l, p, k - 1].astype(F32)
        return acc

    sends = []
    for name in first:
        local[name].wait()
    for l in range(layers):
        step_w[l, :heads, :] = w_step[l]
    w_sorted[0] = dot(sorter, w_maps[0], 0, 0).astype(BF16)
    stream[...] = x[...].astype(F32)

    for l in range(layers):
        normed, squares, raw = project(l)
        if l == 0:
            project_rest(l, normed, squares, raw)
            pl.semaphore_wait(barrier, every - 1)
        send_maps(l)
        if l > 0:
            project_rest(l, normed, squares, raw)
        send_rest(l)

        if l == 0:
            for n in range(len(pairs) + 1):
                name = [*pairs, "wout"][n]
                if name not in first:
                    local[name].wait()
            swap = remote(hbm["wout"].at[:, :, theirs], wout.at[:, 1], w_ss, w_rs, {"tp": jnp.bitwise_xor(tp, 1)})
            swap.start()
            for i in range(1, layers):
                w_sorted[i] = dot(sorter, w_maps[i], 0, 0).astype(BF16)
            per_layer = seqs * keep + taps_n
            mrow[...] = jnp.zeros_like(mrow)
            for i in range(layers):
                for s in range(seqs):
                    for t in range(keep):
                        pair = cache_m[i, s, t].astype(F32)
                        n = i * per_layer + s * keep + t
                        for which in range(2):
                            mrow[which, n : n + 1, :map_cols] = pair[which : which + 1]
                for t in range(taps_n):
                    pair = tap_m[i, t].astype(F32)
                    n = i * per_layer + seqs * keep + t
                    for which in range(2):
                        mrow[which, n : n + 1, :map_cols] = pair[which : which + 1]
            n_rows = mrow.shape[1]
            r, c = grid(LANES, groups * LANES)
            n = (c & (LANES - 1)) - ng * tp
            chosen = (n >= 0) & (n < ng) & (r == groups * n + over(c, LANES))
            packed = dot(mrow[...].reshape(2 * n_rows, LANES).astype(BF16), ones_where(chosen)).astype(BF16)
            for g in range(groups):
                c_send[g] = packed[:, g * LANES : (g + 1) * LANES]
            for k in peers(n_tp, (6, 7, 4, 5, 2, 3, 1)):
                to = jnp.bitwise_xor(tp, k)
                c = remote(c_send.at[group_of(to)], c_recv.at[k], c_ss.at[k - 1], c_rs.at[k - 1], {"tp": to})
                c.start()
                sends.append(c)
            c_recv[0] = c_send[group_of(tp)]

            slot = lax.broadcasted_iota(jnp.int32, (slots, 1), 0)
            mask = jnp.concatenate([(slot < lens[s]).astype(F32) for s in range(seqs)], axis=0)
            r, c = grid(rows, rows)
            causal = (over(r, slots) == over(c, slots)) & (c <= r)
            tri = ones_where(causal)
            r, c = grid(LANES, hp_cols)
            ex = ones_where(r == over(c, head_size))
            r, c = grid(hp_cols, LANES)
            ext = ones_where(c == over(r, head_size))
            r, c = grid(hp_cols, hp_cols)
            ones = ones_where(over(r, head_size) == over(c, head_size))
            padded[...] = jnp.zeros_like(padded)
            padded_m[...] = jnp.zeros_like(padded_m)
            taps[...] = jnp.zeros_like(taps)
            par[...] = jnp.zeros_like(par)
            extra[...] = jnp.zeros_like(extra)
            for i in range(layers):
                taps[i, :taps_n, :] = tap_u[i].astype(F32)
                par[i, 0:1, :heads] = bias[i : i + 1, :]
                par[i, 1:2, :heads] = rate[i : i + 1, :]
                par[i, 2:3, :heads] = skip[i : i + 1, :]
                for s in range(seqs):
                    extra[i, :heads, s * slots : (s + 1) * slots] = extra_t[i, s]
                    for t in range(keep):
                        n = FRONT - keep + t
                        padded[i, s, n : n + 1, :] = cache_u[i, t].astype(F32)[s : s + 1]
            extra_rows = [extra[i].T[:rows] for i in range(layers)]
            skip_x = [sum(dot(piece, ex) for piece in thirds(par[i]))[2:3] for i in range(layers)]

        def convolve(pad, weights):
            pieces = []
            for s in range(seqs):
                total = pad[l, s, FRONT - keep : FRONT - keep + slots, :] * weights[0:1]
                for t in range(1, taps_n):
                    n = FRONT - keep + t
                    total = total + pad[l, s, n : n + slots, :] * weights[t : t + 1]
                pieces.append(total)
            out = jnp.concatenate(pieces, axis=0)
            return out * jax.nn.sigmoid(out)

        acc = await_rest(l, 0)
        tail = acc[:, hp_cols:]
        squares = tail[:, LANES - 2 : LANES - 1] + tail[:, LANES - 1 : LANES]
        factor = lax.rsqrt(squares / d_model + EPS)
        proj = (acc * factor).astype(BF16).astype(F32)
        for s in range(seqs):
            padded[l, s, FRONT : FRONT + slots, :] = proj[s * slots : (s + 1) * slots, :hp_cols]
        inp = convolve(padded, taps[l])
        raw_step = proj[:, hp_cols:] + par[l, 0:1, :]
        step = (jnp.maximum(raw_step, 0.0) + jnp.log1p(jnp.exp(-jnp.abs(raw_step)))) * mask
        step = jnp.where(lane < heads, step, 0.0)
        logdec = extra_rows[l] * mask - step * jnp.exp(par[l, 1:2, :])
        logdec = jnp.where(lane < heads, logdec, 0.0)
        parts = dot(tri, jnp.concatenate(thirds(logdec), axis=1))
        sums = parts[:, :LANES] + parts[:, LANES : 2 * LANES] + parts[:, 2 * LANES :]
        sums_t = sums.T
        step_t = step.T
        sums_parts, step_parts = thirds(sums), thirds(step)
        both = dot(jnp.concatenate(sums_parts + step_parts, axis=0), ex)
        sums_x = both[:rows] + both[rows : 2 * rows] + both[2 * rows : 3 * rows]
        step_x = both[3 * rows : 4 * rows] + both[4 * rows : 5 * rows] + both[5 * rows :]
        last_x = jnp.concatenate(
            [
                jnp.broadcast_to(sums_x[(s + 1) * slots - 1 : (s + 1) * slots, :], (slots, hp_cols))
                for s in range(seqs)
            ],
            axis=0,
        )
        weighted = (jnp.exp(last_x - sums_x) * step_x * inp).astype(BF16)
        inp_b = inp.astype(BF16)
        grow = jnp.exp(sums_x)
        direct = skip_x[l] * inp
        rows_sum = sum(dot(ext, piece, 1, 1) for piece in sums_parts)
        segs = []
        for h in range(heads):
            gap = sums[:, h : h + 1] - sums_t[h : h + 1, :]
            segs.append(jnp.exp(jnp.where(causal, gap, -jnp.inf)) * step_t[h : h + 1, :])

        if l == 0:
            for k in range(1, n_tp):
                remote(
                    c_send.at[0], c_recv.at[k], c_ss.at[k - 1], c_rs.at[k - 1], {"tp": jnp.bitwise_xor(tp, k)}
                ).wait_recv()
            total = c_recv[0].astype(F32)
            for k in range(1, n_tp):
                total = total + c_recv[k].astype(F32)
            mrows[...] = jnp.concatenate([total[:n_rows], total[n_rows:]], axis=1)
            for i in range(layers):
                for s in range(seqs):
                    n = i * per_layer + s * keep
                    padded_m[i, s, FRONT - keep : FRONT, :] = mrows[n : n + keep, :]
        remote(
            m_recv.at[l, 0 : every - 1], m_recv.at[l, 0 : every - 1], m_ss.at[l], m_rs.at[l], at(0, 1)
        ).wait_recv()
        got = m_recv[l].astype(F32).reshape(n_dp, n_tp, 8, LANES)
        got = sum(got[b] for b in range(n_dp))
        cell = over(lane, ng)
        columns = []
        for which in range(2):
            blocks = []
            for q in range(quads):
                n = 2 * q + which
                piece = got[0]
                for t in range(1, n_tp):
                    piece = jnp.where(cell == (n + t) % n_tp, got[t], piece)
                blocks.append(piece if n == 0 else pltpu.roll(piece, LANES - ng * n, 1))
            columns.append(jnp.concatenate(blocks, axis=0))
        proj_m = (jnp.concatenate(columns, axis=1) * factor).astype(BF16).astype(F32)
        for s in range(seqs):
            padded_m[l, s, FRONT : FRONT + slots, :] = proj_m[s * slots : (s + 1) * slots]
        n = l * per_layer + seqs * keep
        both_maps = convolve(padded_m, mrows[n : n + taps_n, :]).astype(BF16)
        b_map, c_map = both_maps[:, :n_state], both_maps[:, n_state:]
        cross = dot(c_map, b_map, 1, 1)
        within = jnp.concatenate(
            [
                dot((cross * segs[h]).astype(BF16), inp_b[:, h * head_size : (h + 1) * head_size])
                for h in range(heads)
            ],
            axis=1,
        )
        carried = jnp.concatenate(
            [
                dot(c_map[s * slots : (s + 1) * slots], state[l, s].astype(BF16), 1, 1)
                for s in range(seqs)
            ],
            axis=0,
        )
        acc = await_rest(l, 1)
        later = (acc * factor).astype(BF16).astype(F32)
        gate = later[:, :hp_cols]
        gate = gate * jax.nn.sigmoid(gate)
        read = (within + carried * grow + direct) * gate
        power = read * read
        p_hi = power.astype(BF16)
        p_lo = (power - p_hi.astype(F32)).astype(BF16)
        mean = (dot(p_hi, ones) + dot(p_lo, ones)) / head_size
        headout = (read * lax.rsqrt(mean + EPS) * gain[l : l + 1, :] * mask).astype(BF16)
        h_recv[l, 0, 0] = headout
        own = h_recv.at[l, 0, 0]
        targets = [(1, 0)] + [(i, k) for k in near_first for i in (0, 1)]
        for i, k in targets:
            remote(own, h_recv.at[l, i, k], h_ss.at[l, i, k], h_rs.at[l, i, k], at(i, k)).start()

        def heads_in(i, k):
            remote(own, h_recv.at[l, i, k], h_ss.at[l, i, k], h_rs.at[l, i, k], at(i, k)).wait_recv()

        def push(k):
            value = jnp.concatenate([h_recv[l, 0, k], h_recv[l, 1, k]], axis=1)
            block = jnp.bitwise_xor(dp, k)
            o_send[l, k] = dot(value, wout[l].reshape(2 * hp_cols, half)).astype(BF16)
            for j in z_peers:
                remote(
                    o_send.at[l, k], o_recv.at[l, j, k], o_ss.at[l, j - 1, k], o_rs.at[l, j - 1, k],
                    {"tp": jnp.bitwise_xor(tp, 2 * j)},
                ).start()

        if l == 0:
            swap.wait_recv()
        heads_in(1, 0)
        push(0)
        for s in range(seqs):
            span = slice(s * slots, (s + 1) * slots)
            fresh = dot(weighted[span], b_map[span], 0, 0)
            end = (s + 1) * slots - 1
            ssm[l, s] = jnp.exp(rows_sum[:, end : end + 1]) * state[l, s] + fresh
        for k in near_first:
            heads_in(0, k)
            heads_in(1, k)
            push(k)

        r, c = grid(LANES, LANES)
        own_maps = dot(later[:, hp_cols:].astype(BF16), ones_where(r == ((c + ng * tp) & (LANES - 1))))
        own_maps = own_maps.astype(BF16)
        r, c = grid(LANES, LANES)
        unsort = ones_where(
            c == (over(r, ng) & 1) * map_cols + groups * (r & (ng - 1)) + over(r, pair_cols)
        )
        own_maps = dot(own_maps, unsort)
        for s in range(seqs):
            pick = lax.broadcasted_iota(jnp.int32, (8, FRONT + slots), 0)
            spot = lax.broadcasted_iota(jnp.int32, (8, FRONT + slots), 1)
            chooser = ((spot == pick + lens[s] + (FRONT - keep)) & (pick < keep)).astype(BF16)
            kept = dot(chooser, padded[l, s].astype(BF16)).astype(BF16)
            r, c = grid(8, slots)
            later_pick = ones_where((c == r + lens[s] - keep) & (r < keep))
            maps_kept = dot(later_pick, own_maps[s * slots : (s + 1) * slots].astype(BF16))
            for t in range(keep):
                kept_u[l, t, s : s + 1, :] = kept[t : t + 1]
                old = jnp.zeros((1, LANES), F32)
                for n in range(keep):
                    flat = jnp.concatenate(
                        [cache_m[l, s, n].astype(F32)[which : which + 1] for which in range(2)], axis=1
                    )
                    old = jnp.where(t + lens[s] == n, flat, old)
                line = (maps_kept[t : t + 1] + old).astype(BF16)
                for which in range(2):
                    kept_m[l, s, t, which : which + 1, :] = line[:, which * map_cols : (which + 1) * map_cols]

        def gather(k):
            for j in z_peers:
                remote(
                    o_send.at[l, k], o_recv.at[l, j, k], o_ss.at[l, j - 1, k], o_rs.at[l, j - 1, k],
                    {"tp": jnp.bitwise_xor(tp, 2 * j)},
                ).wait_recv()
            o_recv[l, 0, k] = o_send[l, k]
            block = jnp.bitwise_xor(dp, k)
            total = o_recv[l, zed, k].astype(F32)
            for z in range(1, n_z):
                total = total + o_recv[l, jnp.bitwise_xor(zed, z), k].astype(F32)
            nb[l, side, block] = total.astype(BF16)
            remote(
                nb.at[l, side, block], nb.at[l, side, block], n_ss.at[l, k], n_rs.at[l, k], at(1, 0)
            ).start()

        order = [0, *near_first]
        for k in order:
            gather(k)
        for k in order:
            block = jnp.bitwise_xor(dp, k)
            remote(
                nb.at[l, side, block], nb.at[l, 1 - side, block], n_ss.at[l, k], n_rs.at[l, k], at(1, 0)
            ).wait_recv()
        for h in range(2):
            stream[:, h * half : (h + 1) * half] += nb[l, h].astype(F32).reshape(tokens, half)

    for c in sends:
        c.wait_send()
    swap.wait_send()
    for l in range(layers):
        for i, j in others:
            remote(m_send.at[l, 0, 0], m_recv.at[l, 0], m_ss.at[l], m_rs.at[l], at(i, j)).wait_send()
        for k in dp_peers:
            for p in range(2):
                remote(
                    a_send.at[l, p, 0], a_recv.at[l, p, k - 1], a_ss.at[l, p, k - 1], a_rs.at[l, p, k - 1], at(0, k)
                ).wait_send()
        for i, k in [(1, 0)] + [(i, k) for k in near_first for i in (0, 1)]:
            remote(
                h_recv.at[l, 0, 0], h_recv.at[l, i, k], h_ss.at[l, i, k], h_rs.at[l, i, k], at(i, k)
            ).wait_send()
        for k in range(n_dp):
            for j in z_peers:
                remote(
                    o_send.at[l, k], o_recv.at[l, j, k], o_ss.at[l, j - 1, k], o_rs.at[l, j - 1, k], at(2 * j, 0)
                ).wait_send()
            remote(nb.at[l, 0, 0], nb.at[l, 0, 0], n_ss.at[l, k], n_rs.at[l, k], at(1, 0)).wait_send()


def finish(stream, kept_u, kept_m, ssm, stream_out, kept_u_out, kept_m_out, ssm_out, sems):
    pairs = ((ssm, ssm_out), (stream, stream_out), (kept_u, kept_u_out), (kept_m, kept_m_out))
    copies = [pltpu.make_async_copy(a, b, sems.at[i]) for i, (a, b) in enumerate(pairs)]
    for c in copies:
        c.start()
    for c in copies:
        c.wait()


def fits(n_tp, n_dp, heads, hp_cols, map_cols, n_state, rows, d_here, keep):
    groups = map_cols * n_tp // n_state
    powers = all(n & (n - 1) == 0 for n in (n_tp, n_dp, groups, map_cols // groups))
    return (
        powers and n_tp > 1 and n_dp > 1 and n_tp * n_dp <= 64 and n_tp % groups == 0 and map_cols % groups == 0
        and hp_cols % LANES == 0 and 2 * map_cols == LANES and n_state == LANES
        and rows * 2 * (map_cols // groups) == 8 * LANES and d_here % (2 * LANES) == 0
        and keep <= FRONT and heads <= LANES - 2
    )


def body(n_tp, n_dp, *args):
    (
        tokens, lengths, input_norm_scale, gate_input_weight, maps_weight, step_weight,
        input_tap_weight, map_tap_weight, step_size_bias, decay_rate_logarithm, direct_path_weight,
        head_norm_scale, output_weight, convolution_input_cache, convolution_map_cache,
        recurrent_state, extra_log_decay,
    ) = args
    layers, seqs, slots, heads = extra_log_decay.shape
    head_size, n_state = recurrent_state.shape[3:]
    hp_cols = heads * head_size
    map_cols = maps_weight.shape[3]
    rows = seqs * slots
    d_here = tokens.shape[1]
    keep = convolution_input_cache.shape[2]
    if not fits(n_tp, n_dp, heads, hp_cols, map_cols, n_state, rows, d_here, keep):
        return general_body(n_tp, n_dp, *args)
    groups = map_cols * n_tp // n_state
    n_z = n_tp // 2
    taps_n = keep + 1
    n_rows = -(-layers * (seqs * keep + taps_n) // 8) * 8

    state = recurrent_state.reshape(layers, seqs, hp_cols, n_state)
    operands = [
        lengths, tokens, input_norm_scale, gate_input_weight,
        jnp.transpose(maps_weight, (0, 2, 3, 1)).reshape(layers, 2 * map_cols, d_here),
        jnp.transpose(step_weight, (0, 2, 1)),
        input_tap_weight, map_tap_weight, step_size_bias, decay_rate_logarithm, direct_path_weight, head_norm_scale,
        jnp.transpose(convolution_input_cache, (0, 2, 1, 3)), convolution_map_cache,
        jnp.transpose(extra_log_decay, (0, 1, 3, 2)), state, output_weight,
    ]
    vmem = pl.BlockSpec(memory_space=pltpu.VMEM)
    hbm = pl.BlockSpec(memory_space=pltpu.HBM)
    sems = lambda *n: pltpu.SemaphoreType.DMA((layers, *n))
    held = [pltpu.VMEM(a.shape, a.dtype) for a in operands[1:-1]]
    held[2] = pltpu.VMEM((layers, hp_cols // LANES, d_here, 2, LANES), BF16)
    results = (
        jax.ShapeDtypeStruct(tokens.shape, F32),
        jax.ShapeDtypeStruct((layers, keep, seqs, hp_cols), BF16),
        jax.ShapeDtypeStruct((layers, seqs, keep, 2, map_cols), BF16),
        jax.ShapeDtypeStruct(state.shape, F32),
    )
    made = pl.pallas_call(
        functools.partial(
            kernel, n_tp, n_dp, d_here * n_dp, groups,
            (layers, seqs, slots, heads, head_size, n_state, hp_cols, map_cols),
        ),
        out_shape=results,
        in_specs=[hbm] * len(operands),
        out_specs=(vmem,) * len(results),
        scratch_shapes=[
            pltpu.SMEM(lengths.shape, jnp.int32),
            *held,
            pltpu.VMEM((layers, 2, hp_cols, d_here // 2), BF16),
            pltpu.SemaphoreType.DMA((len(operands),)),
            sems(hp_cols // LANES),
            pltpu.VMEM((layers, 2, n_dp, rows, hp_cols + LANES), BF16),
            pltpu.VMEM((layers, 2, n_dp - 1, rows, hp_cols + LANES), BF16),
            pltpu.VMEM((layers, groups, n_dp, 8, LANES), BF16),
            pltpu.VMEM((layers, n_dp * n_tp, 8, LANES), BF16),
            pltpu.VMEM((groups, 2 * n_rows, LANES), BF16),
            pltpu.VMEM((n_tp, 2 * n_rows, LANES), BF16),
            pltpu.VMEM((layers, 2, n_dp, rows, hp_cols), BF16),
            pltpu.VMEM((layers, n_dp, rows, d_here // 2), BF16),
            pltpu.VMEM((layers, n_z, n_dp, rows, d_here // 2), BF16),
            pltpu.VMEM((layers, 2, n_dp, rows, d_here // 2), BF16),
            pltpu.VMEM((layers, seqs, FRONT + slots, hp_cols), F32),
            pltpu.VMEM((layers, seqs, FRONT + slots, 2 * n_state), F32),
            pltpu.VMEM((2, n_rows, LANES), F32),
            pltpu.VMEM((n_rows, 2 * n_state), F32),
            pltpu.VMEM((layers, LANES, d_here), BF16),
            pltpu.VMEM((layers, LANES, d_here), BF16),
            pltpu.VMEM((layers, 8, hp_cols), F32),
            pltpu.VMEM((layers, 8, LANES), F32),
            pltpu.VMEM((layers, LANES, LANES), F32),
            sems(2, n_dp - 1), sems(2, n_dp - 1),
            pltpu.SemaphoreType.DMA((layers,)), pltpu.SemaphoreType.DMA((layers,)),
            pltpu.SemaphoreType.DMA((n_tp - 1,)), pltpu.SemaphoreType.DMA((n_tp - 1,)),
            sems(2, n_dp), sems(2, n_dp),
            sems(n_z - 1, n_dp), sems(n_z - 1, n_dp),
            sems(n_dp), sems(n_dp),
            pltpu.SemaphoreType.DMA, pltpu.SemaphoreType.DMA,
        ],
        compiler_params=pltpu.CompilerParams(
            collective_id=0, has_side_effects=True, vmem_limit_bytes=32 * 2**20
        ),
        name="mixer",
    )(*[pltpu.with_memory_space_constraint(a, pltpu.HBM) for a in operands])
    stream, conv_in, conv_maps, ssm = pl.pallas_call(
        finish,
        out_shape=results,
        in_specs=[vmem] * len(results),
        out_specs=(hbm,) * len(results),
        scratch_shapes=[pltpu.SemaphoreType.DMA((len(results),))],
        compiler_params=pltpu.CompilerParams(vmem_limit_bytes=2**20),
        name="finish",
    )(*made)
    return stream, jnp.transpose(conv_in, (0, 2, 1, 3)), conv_maps, ssm.reshape(recurrent_state.shape)


def solution(mesh):
    placed = (
        P(None, "dp"),
        P("dp"),
        P(None, "dp"),
        P(None, "dp", None, "tp"),
        P(None, "dp", None, "tp"),
        P(None, "dp", "tp"),
        P(None, None, "tp"),
        P(None, None, None, "tp"),
        P(None, "tp"),
        P(None, "tp"),
        P(None, "tp"),
        P(None, "tp"),
        P(None, "tp", "dp"),
        P(None, "dp", None, "tp"),
        P(None, "dp", None, None, "tp"),
        P(None, "dp", "tp", None, None),
        P(None, "dp", None, "tp"),
    )
    return jax.shard_map(
        functools.partial(body, mesh.shape["tp"], mesh.shape["dp"]),
        mesh=mesh,
        in_specs=placed,
        out_specs=(
            P(None, "dp"),
            P(None, "dp", None, "tp"),
            P(None, "dp", None, None, "tp"),
            P(None, "dp", "tp", None, None),
        ),
        check_vma=False,
    )
```

```python
import functools

import jax
import jax.numpy as jnp
from jax import lax
from jax.experimental import pallas as pl
from jax.experimental.pallas import tpu as pltpu
from jax.sharding import PartitionSpec as P

EPS = 1e-06
LANES = 128
FRONT = 8
F32, BF16 = jnp.float32, jnp.bfloat16


def up(n):
    return -(-n // LANES) * LANES


def dot(a, b, ca=1, cb=0):
    return lax.dot_general(a, b, (((ca,), (cb,)), ((), ())), preferred_element_type=F32)


def thirds(a):
    high = a.astype(BF16)
    rest = a - high.astype(F32)
    middle = rest.astype(BF16)
    return high, middle, (rest - middle.astype(F32)).astype(BF16)


def grid(n_rows, n_cols):
    return (
        lax.broadcasted_iota(jnp.int32, (n_rows, n_cols), 0),
        lax.broadcasted_iota(jnp.int32, (n_rows, n_cols), 1),
    )


def over(a, n):
    return lax.shift_right_logical(a, jnp.full_like(a, n.bit_length() - 1))


def ones_where(cond):
    return jnp.where(cond, 1.0, 0.0).astype(BF16)


def far_first(k, me, n):
    upper = me // (n // 2)
    mirrored = n - 1 - me
    return upper * (k + (k - me + n) // n) + (1 - upper) * (n - 1 - k - (k - mirrored + n) // n)


def general_kernel(
    n_tp, n_dp, d_model, heads, groups, slots, seqs, hp_cols, map_cols,
    lens, x, scale, w_pair, w_maps, w_step, tap_u, tap_m, bias, rate, skip, gain, cache_u, cache_m, extra_t,
    state_hbm, wout_hbm,
    stream, kept, ssm,
    a_send, a_recv, m_send, m_recv, h_send, h_recv, o_send, o_recv, n_send, n_recv, padded, step_w, state, wout, taps, par, extra,
    a_ss, a_rs, m_ss, m_rs, h_ss, h_rs, o_ss, o_rs, n_ss, n_rs, s_sem, w_sem,
):
    tp, dp = lax.axis_index("tp"), lax.axis_index("dp")
    layers = w_pair.shape[0]
    rows = seqs * slots
    taps_n = tap_u.shape[1]
    keep = taps_n - 1
    zc = up(hp_cols)
    ng = map_cols // groups
    n_state = state.shape[-1]
    cut = stream.shape[0] // n_tp
    per = rows // cut
    head_size = hp_cols // heads

    state_copy = pltpu.make_async_copy(state_hbm, state, s_sem)
    wout_copy = pltpu.make_async_copy(wout_hbm, wout, w_sem)
    state_copy.start()
    wout_copy.start()
    barrier = pltpu.get_barrier_semaphore()
    for k in range(1, n_dp):
        pl.semaphore_signal(barrier, inc=1, device_id={"dp": lax.rem(dp + k, n_dp)})
    for k in range(1, n_tp):
        pl.semaphore_signal(barrier, inc=1, device_id={"tp": lax.rem(tp + k, n_tp)})

    stream[...] = x[...].astype(F32)
    slot = lax.broadcasted_iota(jnp.int32, (slots, 1), 0)
    mask = jnp.concatenate([(slot < lens[s]).astype(F32) for s in range(seqs)], axis=0)
    lane = lax.broadcasted_iota(jnp.int32, (1, LANES), 1)
    r, c = grid(rows, rows)
    causal = (over(r, slots) == over(c, slots)) & (c <= r)
    tri = ones_where(causal)
    r, c = grid(2 * map_cols, up(2 * map_cols))
    which = over(r, ng) & 1
    sel = ones_where(c == which * map_cols + groups * (r & (ng - 1)) + over(r, 2 * ng))
    r, c = grid(n_tp * 2 * ng, 2 * n_state)
    sel2 = ones_where(c == (over(r, ng) & 1) * n_state + over(r, 2 * ng) * ng + (r & (ng - 1)))
    r, c = grid(LANES, hp_cols)
    ex = ones_where(r == over(c, head_size))
    r, c = grid(hp_cols, LANES)
    ext = ones_where(c == over(r, head_size))
    r, c = grid(hp_cols, hp_cols)
    ones = ones_where(over(r, head_size) == over(c, head_size))
    r, c = grid(LANES, 2 * LANES)
    spread = ones_where(c == 2 * r)
    padded[...] = jnp.zeros_like(padded)
    step_w[...] = jnp.zeros_like(step_w)
    taps[...] = jnp.zeros_like(taps)
    par[...] = jnp.zeros_like(par)
    extra[...] = jnp.zeros_like(extra)
    for l in range(layers):
        step_w[l, :heads, :] = w_step[l]
        taps[l, :taps_n, :hp_cols] = tap_u[l].astype(F32)
        for t in range(taps_n):
            pair = tap_m[l, t].astype(F32)
            for which in range(2):
                at = zc + which * map_cols
                taps[l, t : t + 1, at : at + map_cols] = pair[which : which + 1]
        par[l, 0:1, :heads] = bias[l : l + 1, :]
        par[l, 1:2, :heads] = rate[l : l + 1, :]
        par[l, 2:3, :heads] = skip[l : l + 1, :]
        for s in range(seqs):
            extra[l, :heads, s * slots : (s + 1) * slots] = extra_t[l, s]
    extra_rows = [extra[l].T[:rows] for l in range(layers)]
    skip_x = [sum(dot(piece, ex) for piece in thirds(par[l]))[2:3] for l in range(layers)]
    sends = []

    def copy(src, dst, ss, rs, where):
        return pltpu.make_async_remote_copy(
            src_ref=src, dst_ref=dst, send_sem=ss, recv_sem=rs, device_id=where
        )

    for l in range(layers):
        st = stream[...]
        squares = jnp.sum(st * st, axis=1, keepdims=True)
        normed = (st * scale[l : l + 1, :]).astype(BF16)
        even = jnp.concatenate(
            [dot(normed[:, i : i + LANES], spread) for i in range(0, normed.shape[1], LANES)], axis=1
        )
        odd = pltpu.roll(even, 1, 1)
        pair = dot(jnp.concatenate([even.astype(BF16), odd.astype(BF16)], axis=0), w_pair[l])
        tokens = st.shape[0]
        tail = dot(normed, step_w[l], 1, 1)
        high = squares.astype(BF16).astype(F32)
        tail = jnp.where(lane == LANES - 2, high, jnp.where(lane == LANES - 1, squares - high, tail))
        part = jnp.concatenate(
            [pair[:tokens], pair[tokens:], dot(normed, w_maps[l], 1, 1), tail], axis=1
        ).astype(BF16)
        for b in range(n_dp):
            a_send[l, b] = part[b * rows : (b + 1) * rows]
        if l == 0:
            pl.semaphore_wait(barrier, n_dp - 1 + n_tp - 1)
        flights = []
        for k in range(1, n_dp):
            to = lax.rem(dp + k, n_dp)
            c = copy(a_send.at[l, to], a_recv.at[l, k - 1], a_ss.at[l, k - 1], a_rs.at[l, k - 1], {"dp": to})
            c.start()
            flights.append(c)
        sends += flights
        acc = a_send[l, dp].astype(F32)
        for k, c in enumerate(flights):
            c.wait_recv()
            acc = acc + a_recv[l, k].astype(F32)
        tail = acc[:, acc.shape[1] - LANES :]
        squares = tail[:, LANES - 2 : LANES - 1] + tail[:, LANES - 1 : LANES]
        factor = lax.rsqrt(squares / d_model + EPS)
        proj = (acc * factor).astype(BF16).astype(F32)

        conv_w = taps.shape[2]
        pieces = []
        for s in range(seqs):
            for t in range(keep):
                at = FRONT - keep + t
                padded[s, at : at + 1, :hp_cols] = cache_u[l, t].astype(F32)[s : s + 1]
                pair = cache_m[l, s, t].astype(F32)
                for which in range(2):
                    col = zc + which * map_cols
                    padded[s, at : at + 1, col : col + map_cols] = pair[which : which + 1]
            padded[s, FRONT : FRONT + slots, :] = proj[s * slots : (s + 1) * slots, zc : zc + conv_w]
            total = padded[s, FRONT - keep : FRONT - keep + slots, :] * taps[l, 0:1, :]
            for t in range(1, taps_n):
                at = FRONT - keep + t
                total = total + padded[s, at : at + slots, :] * taps[l, t : t + 1, :]
            pieces.append(total)
        filtered = jnp.concatenate(pieces, axis=0)
        filtered = filtered * jax.nn.sigmoid(filtered)
        maps = filtered[:, conv_w - up(2 * map_cols) :].astype(BF16)
        sorted_maps = dot(sel, maps, 1, 1)
        for g in range(groups):
            m_send[l, g] = sorted_maps[g * 2 * ng : (g + 1) * 2 * ng, :].astype(BF16)

        def group_of(rank):
            return rank * heads // (heads * n_tp // groups)

        flights = []
        for k in range(n_tp - 1):
            to = far_first(k, tp, n_tp)
            c = copy(m_send.at[l, group_of(to)], m_recv.at[l, tp], m_ss.at[l, k], m_rs.at[l, tp], {"tp": to})
            c.start()
            sends.append(c)
        m_recv[l, tp] = m_send[l, group_of(tp)]

        for s in range(seqs):
            pick = lax.broadcasted_iota(jnp.int32, (8, FRONT + slots), 0)
            place = lax.broadcasted_iota(jnp.int32, (8, FRONT + slots), 1)
            chooser = ((place == pick + lens[s] + (FRONT - keep)) & (pick < keep)).astype(BF16)
            kept[l, s] = dot(chooser, padded[s].astype(BF16)).astype(BF16)
        raw = proj[:, proj.shape[1] - LANES :] + par[l, 0:1, :]
        step = (jnp.maximum(raw, 0.0) + jnp.log1p(jnp.exp(-jnp.abs(raw)))) * mask
        step = jnp.where(lane < heads, step, 0.0)
        logdec = extra_rows[l] * mask - step * jnp.exp(par[l, 1:2, :])
        logdec = jnp.where(lane < heads, logdec, 0.0)
        parts = dot(tri, jnp.concatenate(thirds(logdec), axis=1))
        sums = parts[:, :LANES] + parts[:, LANES : 2 * LANES] + parts[:, 2 * LANES :]
        sums_t = sums.T
        step_t = step.T
        sums_parts, step_parts = thirds(sums), thirds(step)
        both = dot(jnp.concatenate(sums_parts + step_parts, axis=0), ex)
        sums_x = both[:rows] + both[rows : 2 * rows] + both[2 * rows : 3 * rows]
        step_x = both[3 * rows : 4 * rows] + both[4 * rows : 5 * rows] + both[5 * rows :]
        inp = filtered[:, :hp_cols]
        gate = proj[:, :hp_cols]
        last_x = jnp.concatenate(
            [
                jnp.broadcast_to(sums_x[(s + 1) * slots - 1 : (s + 1) * slots, :], (slots, hp_cols))
                for s in range(seqs)
            ],
            axis=0,
        )
        weighted = (jnp.exp(last_x - sums_x) * step_x * inp).astype(BF16)
        inp_b = inp.astype(BF16)
        grow = jnp.exp(sums_x)
        direct = skip_x[l] * inp
        gate = gate * jax.nn.sigmoid(gate)
        rows_sum = sum(dot(ext, piece, 1, 1) for piece in sums_parts)
        segs = []
        for h in range(heads):
            gap = sums[:, h : h + 1] - sums_t[h : h + 1, :]
            segs.append(jnp.exp(jnp.where(causal, gap, -jnp.inf)) * step_t[h : h + 1, :])

        if l == 0:
            state_copy.wait()
            wout_copy.wait()
        for k in range(1, n_tp):
            src = lax.rem(tp + n_tp - k, n_tp)
            copy(m_send.at[l, 0], m_recv.at[l, src], m_ss.at[l, 0], m_rs.at[l, src], {"tp": src}).wait_recv()
        got = m_recv[l].astype(F32).reshape(n_tp * 2 * ng, rows)
        both_maps = dot(got.T.astype(BF16), sel2).astype(BF16)
        b_map, c_map = both_maps[:, :n_state], both_maps[:, n_state:]
        cross = dot(c_map, b_map, 1, 1)
        within = jnp.concatenate(
            [
                dot((cross * segs[h]).astype(BF16), inp_b[:, h * head_size : (h + 1) * head_size])
                for h in range(heads)
            ],
            axis=1,
        )
        carried = jnp.concatenate(
            [
                dot(c_map[s * slots : (s + 1) * slots], state[l, s].astype(BF16), 1, 1)
                for s in range(seqs)
            ],
            axis=0,
        )
        read = (within + carried * grow + direct) * gate
        power = read * read
        p_hi = power.astype(BF16)
        p_lo = (power - p_hi.astype(F32)).astype(BF16)
        mean = (dot(p_hi, ones) + dot(p_lo, ones)) / head_size
        headout = (read * lax.rsqrt(mean + EPS) * gain[l : l + 1, :] * mask).astype(BF16)
        h_send[l] = headout
        flights = []
        for k in range(1, n_dp):
            to = lax.rem(dp + k, n_dp)
            c = copy(h_send.at[l], h_recv.at[l, k - 1], h_ss.at[l, k - 1], h_rs.at[l, k - 1], {"dp": to})
            c.start()
            flights.append(c)
        sends += flights

        def push(value, block):
            out = dot(value, wout[l]).astype(BF16)
            for i in range(per):
                to = block * per + i
                o_send[l, to] = out[i * cut : (i + 1) * cut]

                @pl.when(to != tp)
                def _():
                    copy(o_send.at[l, to], o_recv.at[l, tp], o_ss.at[l, to], o_rs.at[l, tp], {"tp": to}).start()

        push(headout, dp)
        for s in range(seqs):
            at = slice(s * slots, (s + 1) * slots)
            fresh = dot(weighted[at], b_map[at], 0, 0)
            end = (s + 1) * slots - 1
            ssm[l, s] = jnp.exp(rows_sum[:, end : end + 1]) * state[l, s] + fresh
        for k, c in enumerate(flights):
            c.wait_recv()
            push(h_recv[l, k], lax.rem(dp + n_dp - k - 1, n_dp))
        total = o_send[l, tp].astype(F32)
        for k in range(1, n_tp):
            src = lax.rem(tp + n_tp - k, n_tp)
            copy(o_send.at[l, src], o_recv.at[l, src], o_ss.at[l, src], o_rs.at[l, src], {"tp": src}).wait_recv()
            total = total + o_recv[l, src].astype(F32)
        fresh = total.astype(BF16)
        n_send[l] = fresh
        n_recv[l, tp] = fresh
        for k in range(n_tp - 1):
            to = far_first(k, tp, n_tp)
            c = copy(n_send.at[l], n_recv.at[l, tp], n_ss.at[l, k], n_rs.at[l, tp], {"tp": to})
            c.start()
            sends.append(c)
        for k in range(1, n_tp):
            src = lax.rem(tp + n_tp - k, n_tp)
            copy(n_send.at[l], n_recv.at[l, src], n_ss.at[l, 0], n_rs.at[l, src], {"tp": src}).wait_recv()
        stream[...] += n_recv[l].astype(F32).reshape(stream.shape)

    for c in sends:
        c.wait_send()
    for l in range(layers):
        for k in range(1, n_tp):
            to = lax.rem(tp + k, n_tp)
            copy(o_send.at[l, to], o_recv.at[l, tp], o_ss.at[l, to], o_rs.at[l, tp], {"tp": to}).wait_send()


def general_body(
    n_tp, n_dp,
    tokens, lengths, input_norm_scale, gate_input_weight, maps_weight, step_weight,
    input_tap_weight, map_tap_weight, step_size_bias, decay_rate_logarithm, direct_path_weight,
    head_norm_scale, output_weight, convolution_input_cache, convolution_map_cache,
    recurrent_state, extra_log_decay,
):
    layers, seqs, slots, heads = extra_log_decay.shape
    head_size, n_state = recurrent_state.shape[3:]
    hp_cols = heads * head_size
    map_cols = maps_weight.shape[3]
    groups = map_cols * n_tp // n_state
    ng = map_cols // groups
    rows = seqs * slots
    d_here = tokens.shape[1]
    keep = convolution_input_cache.shape[2]

    def wide(a):
        pad = up(a.shape[-1]) - a.shape[-1]
        return a if pad == 0 else jnp.pad(a, [(0, 0)] * (a.ndim - 1) + [(0, pad)])

    w_pair = wide(gate_input_weight.reshape(layers, 2 * d_here, hp_cols))
    w_maps = jnp.transpose(maps_weight, (0, 2, 3, 1)).reshape(layers, 2 * map_cols, d_here)
    if up(2 * map_cols) > 2 * map_cols:
        w_maps = jnp.pad(w_maps, ((0, 0), (0, up(2 * map_cols) - 2 * map_cols), (0, 0)))
    w_step = jnp.transpose(step_weight, (0, 2, 1))
    cache_u = jnp.transpose(convolution_input_cache, (0, 2, 1, 3))
    extra_t = jnp.transpose(extra_log_decay, (0, 1, 3, 2))
    state = recurrent_state.reshape(layers, seqs, hp_cols, n_state)

    vmem = pl.BlockSpec(memory_space=pltpu.VMEM)
    wide_cols = 2 * up(hp_cols) + up(2 * map_cols) + LANES
    anywhere = pl.BlockSpec(memory_space=pl.ANY)
    conv_w = up(hp_cols) + up(2 * map_cols)
    cut = tokens.shape[0] // n_tp
    sems = lambda n: pltpu.SemaphoreType.DMA((layers, n))
    args = [tokens, input_norm_scale, w_pair, w_maps, w_step, input_tap_weight,
        map_tap_weight, step_size_bias, decay_rate_logarithm, direct_path_weight, head_norm_scale,
        cache_u, convolution_map_cache, extra_t]
    stream, kept, ssm = pl.pallas_call(
        functools.partial(
            general_kernel, n_tp, n_dp, d_here * n_dp, heads, groups, slots, seqs, hp_cols, map_cols
        ),
        out_shape=(
            jax.ShapeDtypeStruct(tokens.shape, F32),
            jax.ShapeDtypeStruct((layers, seqs, 8, conv_w), BF16),
            jax.ShapeDtypeStruct(state.shape, F32),
        ),
        in_specs=[pl.BlockSpec(memory_space=pltpu.SMEM)] + [vmem] * len(args) + [anywhere] * 2,
        out_specs=(vmem, vmem, vmem),
        scratch_shapes=[
            pltpu.VMEM((layers, n_dp, rows, wide_cols), BF16),
            pltpu.VMEM((layers, n_dp - 1, rows, wide_cols), BF16),
            pltpu.VMEM((layers, groups, 2 * ng, rows), BF16),
            pltpu.VMEM((layers, n_tp, 2 * ng, rows), BF16),
            pltpu.VMEM((layers, rows, hp_cols), BF16),
            pltpu.VMEM((layers, n_dp - 1, rows, hp_cols), BF16),
            pltpu.VMEM((layers, n_tp, cut, d_here), BF16),
            pltpu.VMEM((layers, n_tp, cut, d_here), BF16),
            pltpu.VMEM((layers, cut, d_here), BF16),
            pltpu.VMEM((layers, n_tp, cut, d_here), BF16),
            pltpu.VMEM((seqs, FRONT + slots, conv_w), F32),
            pltpu.VMEM((layers, LANES, d_here), BF16),
            pltpu.VMEM(state.shape, F32),
            pltpu.VMEM(output_weight.shape, BF16),
            pltpu.VMEM((layers, 8, conv_w), F32),
            pltpu.VMEM((layers, 8, LANES), F32),
            pltpu.VMEM((layers, LANES, LANES), F32),
            sems(n_dp - 1), sems(n_dp - 1), sems(n_tp - 1), sems(n_tp), sems(n_dp - 1),
            sems(n_dp - 1), sems(n_tp), sems(n_tp), sems(n_tp - 1), sems(n_tp),
            pltpu.SemaphoreType.DMA, pltpu.SemaphoreType.DMA,
        ],
        compiler_params=pltpu.CompilerParams(
            collective_id=0, has_side_effects=True, vmem_limit_bytes=48 * 2**20
        ),
        name="mixer",
    )(lengths, *args, state, output_weight)
    conv_in = kept[:, :, :keep, :hp_cols]
    start = conv_w - up(2 * map_cols)
    conv_maps = kept[:, :, :keep, start : start + 2 * map_cols].reshape(
        layers, seqs, keep, 2, map_cols
    )
    return stream, conv_in, conv_maps, ssm.reshape(recurrent_state.shape)


def peers(n, order):
    return [k for k in order if 0 < k < n] + [k for k in range(1, n) if k not in order]


def kernel(
    n_tp, n_dp, d_model, groups, shapes,
    *refs,
):
    names = (
        "lens", "x", "scale", "gate", "w_maps", "w_step", "tap_u", "tap_m", "bias", "rate", "skip", "gain",
        "cache_u", "cache_m", "extra_t", "state", "wout",
    )
    hbm = dict(zip(names, refs[: len(names)]))
    (
        stream, kept_u, kept_m, ssm,
        lens, x, scale, w_gate, w_maps, w_step, tap_u, tap_m, bias, rate, skip, gain, cache_u, cache_m, extra_t, state,
        wout, in_sem, g_sem,
        t_send, t_recv, u_send, u_recv, z_send, z_recv, q_send, q_recv, m_send, m_recv, c_send, c_recv, h_recv, o_send, o_recv, nb,
        padded, padded_m, mrow, mrows, w_rows, w_sorted, w_flat, taps, par, extra,
        out_sem, a_rs, m_rs, c_rs, h_rs, o_rs, n_rs, w_rs, f_rs,
    ) = refs[len(names) :]
    layers, seqs, slots, heads, head_size, n_state, hp_cols, map_cols = shapes
    tp, dp = lax.axis_index("tp"), lax.axis_index("dp")
    rows = seqs * slots
    taps_n = tap_u.shape[1]
    keep = taps_n - 1
    ng = map_cols // groups
    pair_cols = 2 * ng
    quads = LANES // pair_cols
    d_here = x.shape[1]
    half = d_here // 2
    tokens = x.shape[0]
    side = lax.rem(tp, 2)
    zed = lax.div(tp, 2)
    n_z = n_tp // 2
    every = n_tp * n_dp
    me = dp * n_tp + tp
    dp_peers = peers(n_dp, (3, 1, 2))
    near_first = peers(n_dp, (1, 2, 3))
    z_peers = peers(n_z, (3, 2, 1))

    def remote(src, dst, arrived, where):
        return pltpu.make_async_remote_copy(
            src_ref=src, dst_ref=dst, send_sem=out_sem, recv_sem=arrived, device_id=where
        )

    def landed(block, arrived):
        remote(block, block, arrived, {"tp": jnp.bitwise_xor(tp, 1)}).wait_recv()

    barrier = pltpu.get_barrier_semaphore()
    others = [
        (i, j) for i in [*peers(n_tp, (6, 7, 4, 5, 2, 3, 1)), 0] for j in [*dp_peers, 0] if i or j
    ]

    def at(i, j):
        return {"tp": jnp.bitwise_xor(tp, i), "dp": jnp.bitwise_xor(dp, j)}

    for i, j in others:
        pl.semaphore_signal(barrier, inc=1, device_id=at(i, j))

    local = {}
    pairs = dict(
        x=x, scale=scale, w_maps=w_maps, w_step=w_step, lens=lens, tap_u=tap_u, tap_m=tap_m, bias=bias, rate=rate,
        skip=skip, gain=gain, cache_u=cache_u, cache_m=cache_m, extra_t=extra_t, state=state,
    )
    for n, name in enumerate(pairs):
        local[name] = pltpu.make_async_copy(hbm[name], pairs[name], in_sem.at[n])
    mine = pl.ds(pl.multiple_of(side * half, LANES), half)
    theirs = pl.ds(pl.multiple_of((1 - side) * half, LANES), half)
    local["wout"] = pltpu.make_async_copy(hbm["wout"].at[:, :, mine], wout.at[:, 0], in_sem.at[len(pairs)])
    gate_copies = [
        [
            pltpu.make_async_copy(
                hbm["gate"].at[l, :, :, i : i + LANES], w_gate.at[l, i // LANES], g_sem.at[l]
            )
            for i in range(0, hp_cols, LANES)
        ]
        for l in range(layers)
    ]
    first = ("x", "scale", "w_maps", "w_step")
    for name in first:
        local[name].start()
    for c in gate_copies[0]:
        c.start()
    for name in local:
        if name not in first:
            local[name].start()
    for l in range(1, layers):
        for c in gate_copies[l]:
            c.start()

    lane = lax.broadcasted_iota(jnp.int32, (1, LANES), 1)
    r, c = grid(LANES, 4 * LANES)
    spread = ones_where(c == jnp.where(c < 2 * LANES, 2 * r, 2 * LANES + 2 * r + 1))
    r, c = grid(LANES, LANES)
    place = (c + LANES - ng * tp) & (LANES - 1)
    wanted = (over(place, ng) & 1) * map_cols + groups * (place & (ng - 1)) + over(place, pair_cols)
    sorter = ones_where(r == wanted)
    home = over((lane + LANES - ng * tp) & (LANES - 1), pair_cols)
    for l in range(layers):
        w_rows[l, :LANES] = jnp.zeros_like(w_rows[l, :LANES])
    gate_rows = w_gate.reshape(layers, hp_cols // LANES, 2 * d_here, LANES)

    def group_of(rank):
        return rank * groups // n_tp

    def start_of(l):
        st = stream[...]
        squares = jnp.sum(st * st, axis=1, keepdims=True)
        return (st * scale[l : l + 1, :]).astype(BF16), squares

    def with_squares(tail, squares):
        high = squares.astype(BF16).astype(F32)
        return jnp.where(lane == LANES - 2, high, jnp.where(lane == LANES - 1, squares - high, tail))

    def fill(buffer, l, value):
        for b in range(n_dp):
            buffer[l, b, :, : value.shape[1]] = value[b * rows : (b + 1) * rows].astype(BF16)

    def pack_maps(l, raw):
        turned = [raw if k == 0 else pltpu.roll(raw, k * pair_cols, 1) for k in range(quads)]
        turned = [t.reshape(n_dp, quads, 8, LANES) for t in turned]
        for g in range(groups):
            piece = turned[(0 - g) % quads][:, 0]
            for q in range(1, quads):
                piece = jnp.where((home == q)[None], turned[(q - g) % quads][:, q], piece)
            m_send[l, g] = piece.astype(BF16)

    def send_maps(l):
        for i, j in others:
            to = at(i, j)
            remote(
                m_send.at[l, group_of(to["tp"]), to["dp"]], m_recv.at[l, me], m_rs, to
            ).start()
        m_recv[l, me] = m_send[l, group_of(tp), dp]

    def rows_of(rank, which):
        return pl.ds(pl.multiple_of(LANES + which * n_state + ng * rank, ng), ng)

    def pick_rows(rank, which):
        return pl.ds(pl.multiple_of(pair_cols * group_of(rank) + which * ng, ng), ng)

    def fetch(i, k, which):
        to = jnp.bitwise_xor(tp, k)
        n = 2 * (i - 1) + (k == 1)
        return remote(
            w_sorted.at[i, pick_rows(to, which)], w_rows.at[i, rows_of(tp, which)], f_rs.at[n], {"tp": to}
        )

    def relay(i, j, which):
        n = 2 * (i - 1) + 1
        block = w_rows.at[i, rows_of(jnp.bitwise_xor(tp, 2 * j), which)]
        return remote(block, block, f_rs.at[n], at(1, 0))

    def fetched(i, far):
        n = 2 * (i - 1) + 1 - far
        landed(w_rows.at[i, pl.ds(LANES, 2 * ng * (n_z - 1 if far else n_z))], f_rs.at[n])

    parts_of = ((t_send, t_recv), (u_send, u_recv), (z_send, z_recv), (q_send, q_recv))

    def part(l, p, k):
        send, recv = parts_of[p]
        to = jnp.bitwise_xor(dp, k)
        src, dst = send.at[l, to], recv.at[l, k - 1]
        if p == 0 and l == 0:
            src, dst = src.at[:, :LANES], dst.at[:, :LANES]
        return remote(src, dst, a_rs.at[l, p], {"dp": to})

    def send_part(l, p):
        for k in dp_peers:
            part(l, p, k).start()

    def await_part(l, p):
        send, recv = parts_of[p]
        width = LANES if p == 0 and l == 0 else send.shape[-1]
        landed(recv.at[l, :, :, :width], a_rs.at[l, p])
        acc = send[l, dp, :, :width].astype(F32)
        for k in range(1, n_dp):
            acc = acc + recv[l, k - 1, :, :width].astype(F32)
        return acc

    def flat_weight(l):
        return jnp.concatenate([gate_rows[l, i] for i in range(hp_cols // LANES)], axis=1)

    sends = []
    for name in first:
        local[name].wait()
    for l in range(layers):
        w_rows[l, :heads, :] = w_step[l]
    w_sorted[0] = dot(sorter, w_maps[0], 0, 0).astype(BF16)
    stream[...] = x[...].astype(F32)

    for l in range(layers):
        normed, squares = start_of(l)
        if l == 0:
            raw = dot(normed, w_sorted[l], 1, 1)
            pack_maps(l, raw)
            fill(t_send, l, with_squares(dot(normed, w_rows[l, :LANES], 1, 1), squares))
            spreads = [dot(normed[:, i : i + LANES], spread).astype(BF16) for i in range(0, d_here, LANES)]
            even = jnp.concatenate([s[:, : 2 * LANES] for s in spreads], axis=1)
            odd = jnp.concatenate([s[:, 2 * LANES :] for s in spreads], axis=1)
            pltpu.make_async_copy(w_gate.at[l], w_gate.at[l], g_sem.at[l]).wait()
            both = dot(jnp.concatenate([odd, even], axis=0), flat_weight(l))
            fill(u_send, l, both[:tokens])
            fill(z_send, l, both[tokens:])
            fill(q_send, l, raw)
            pl.semaphore_wait(barrier, every - 1)
            send_maps(l)
            for p in range(4):
                send_part(l, p)
        else:
            fetched(l, 0)
            tail = dot(normed, w_rows[l], 1, 1)
            fill(t_send, l, jnp.concatenate([with_squares(tail[:, :LANES], squares), tail[:, LANES:]], axis=1))
            send_part(l, 0)
            fill(u_send, l, dot(normed, w_flat[l - 1, 1]))
            send_part(l, 1)
            fill(z_send, l, dot(normed, w_flat[l - 1, 0]))
            send_part(l, 2)
            fill(q_send, l, dot(normed, w_sorted[l], 1, 1))
            send_part(l, 3)

        if l == 0:
            for n in range(len(pairs) + 1):
                name = [*pairs, "wout"][n]
                if name not in first:
                    local[name].wait()
            swap = remote(hbm["wout"].at[:, :, theirs], wout.at[:, 1], w_rs, {"tp": jnp.bitwise_xor(tp, 1)})
            swap.start()
            per_layer = seqs * keep + taps_n
            mrow[...] = jnp.zeros_like(mrow)
            for i in range(layers):
                for s in range(seqs):
                    for t in range(keep):
                        pair = cache_m[i, s, t].astype(F32)
                        n = i * per_layer + s * keep + t
                        for which in range(2):
                            mrow[which, n : n + 1, :map_cols] = pair[which : which + 1]
                for t in range(taps_n):
                    pair = tap_m[i, t].astype(F32)
                    n = i * per_layer + seqs * keep + t
                    for which in range(2):
                        mrow[which, n : n + 1, :map_cols] = pair[which : which + 1]
            n_rows = mrow.shape[1]
            r, c = grid(LANES, groups * LANES)
            n = (c & (LANES - 1)) - ng * tp
            chosen = (n >= 0) & (n < ng) & (r == groups * n + over(c, LANES))
            packed = dot(mrow[...].reshape(2 * n_rows, LANES).astype(BF16), ones_where(chosen)).astype(BF16)
            for g in range(groups):
                c_send[g] = packed[:, g * LANES : (g + 1) * LANES]
            for k in peers(n_tp, (6, 7, 4, 5, 2, 3, 1)):
                to = jnp.bitwise_xor(tp, k)
                c = remote(c_send.at[group_of(to)], c_recv.at[k], c_rs, {"tp": to})
                c.start()
                sends.append(c)
            c_recv[0] = c_send[group_of(tp)]
            r, c = grid(LANES, LANES)
            resort = ones_where(r == (over(c, ng) & 1) * map_cols + groups * (c & (ng - 1)) + over(c, pair_cols))
            for i in range(1, layers):
                w_sorted[i] = dot(resort, w_maps[i], 0, 0).astype(BF16)

            slot = lax.broadcasted_iota(jnp.int32, (slots, 1), 0)
            mask = jnp.concatenate([(slot < lens[s]).astype(F32) for s in range(seqs)], axis=0)
            r, c = grid(rows, rows)
            causal = (over(r, slots) == over(c, slots)) & (c <= r)
            tri = ones_where(causal)
            r, c = grid(LANES, hp_cols)
            ex = ones_where(r == over(c, head_size))
            r, c = grid(hp_cols, LANES)
            ext = ones_where(c == over(r, head_size))
            r, c = grid(hp_cols, hp_cols)
            ones = ones_where(over(r, head_size) == over(c, head_size))
            padded[...] = jnp.zeros_like(padded)
            padded_m[...] = jnp.zeros_like(padded_m)
            taps[...] = jnp.zeros_like(taps)
            par[...] = jnp.zeros_like(par)
            extra[...] = jnp.zeros_like(extra)
            for i in range(layers):
                taps[i, :taps_n, :] = tap_u[i].astype(F32)
                par[i, 0:1, :heads] = bias[i : i + 1, :]
                par[i, 1:2, :heads] = rate[i : i + 1, :]
                par[i, 2:3, :heads] = skip[i : i + 1, :]
                for s in range(seqs):
                    extra[i, :heads, s * slots : (s + 1) * slots] = extra_t[i, s]
                    for t in range(keep):
                        n = FRONT - keep + t
                        padded[i, s, n : n + 1, :] = cache_u[i, t].astype(F32)[s : s + 1]
            extra_rows = [extra[i].T[:rows] for i in range(layers)]
            skip_x = [sum(dot(piece, ex) for piece in thirds(par[i]))[2:3] for i in range(layers)]

        def convolve(pad, weights):
            pieces = []
            for s in range(seqs):
                total = pad[l, s, FRONT - keep : FRONT - keep + slots, :] * weights[0:1]
                for t in range(1, taps_n):
                    n = FRONT - keep + t
                    total = total + pad[l, s, n : n + slots, :] * weights[t : t + 1]
                pieces.append(total)
            out = jnp.concatenate(pieces, axis=0)
            return out * jax.nn.sigmoid(out)

        acc = await_part(l, 0)
        tail = acc[:, :LANES]
        squares = tail[:, LANES - 2 : LANES - 1] + tail[:, LANES - 1 : LANES]
        factor = lax.rsqrt(squares / d_model + EPS)
        raw_step = (tail * factor).astype(BF16).astype(F32) + par[l, 0:1, :]
        step = (jnp.maximum(raw_step, 0.0) + jnp.log1p(jnp.exp(-jnp.abs(raw_step)))) * mask
        step = jnp.where(lane < heads, step, 0.0)
        logdec = extra_rows[l] * mask - step * jnp.exp(par[l, 1:2, :])
        logdec = jnp.where(lane < heads, logdec, 0.0)
        parts = dot(tri, jnp.concatenate(thirds(logdec), axis=1))
        sums = parts[:, :LANES] + parts[:, LANES : 2 * LANES] + parts[:, 2 * LANES :]
        sums_t = sums.T
        step_t = step.T
        sums_parts, step_parts = thirds(sums), thirds(step)
        both = dot(jnp.concatenate(sums_parts + step_parts, axis=0), ex)
        sums_x = both[:rows] + both[rows : 2 * rows] + both[2 * rows : 3 * rows]
        step_x = both[3 * rows : 4 * rows] + both[4 * rows : 5 * rows] + both[5 * rows :]
        grow = jnp.exp(sums_x)
        segs = []
        for h in range(heads):
            gap = sums[:, h : h + 1] - sums_t[h : h + 1, :]
            segs.append(jnp.exp(jnp.where(causal, gap, -jnp.inf)) * step_t[h : h + 1, :])

        def filter_inputs():
            proj = (await_part(l, 1) * factor).astype(BF16).astype(F32)
            for s in range(seqs):
                padded[l, s, FRONT : FRONT + slots, :] = proj[s * slots : (s + 1) * slots]
            return convolve(padded, taps[l])

        def unpack_maps():
            landed(m_recv.at[l, 0 : every - 1], m_rs)
            got = m_recv[l].astype(F32).reshape(n_dp, n_tp, 8, LANES)
            got = sum(got[b] for b in range(n_dp))
            cell = over(lane, ng)
            columns = []
            for which in range(2):
                blocks = []
                for q in range(quads):
                    n = 2 * q + which
                    piece = got[0]
                    for t in range(1, n_tp):
                        piece = jnp.where(cell == (n + t) % n_tp, got[t], piece)
                    blocks.append(piece if n == 0 else pltpu.roll(piece, LANES - ng * n, 1))
                columns.append(jnp.concatenate(blocks, axis=0))
            return jnp.concatenate(columns, axis=1)

        def filter_maps(raw):
            proj = (raw * factor).astype(BF16).astype(F32)
            for s in range(seqs):
                padded_m[l, s, FRONT : FRONT + slots, :] = proj[s * slots : (s + 1) * slots]
            n = l * per_layer + seqs * keep
            maps = convolve(padded_m, mrows[n : n + taps_n, :]).astype(BF16)
            b_map, c_map = maps[:, :n_state], maps[:, n_state:]
            carried = jnp.concatenate(
                [
                    dot(c_map[s * slots : (s + 1) * slots], state[l, s].astype(BF16), 1, 1)
                    for s in range(seqs)
                ],
                axis=0,
            )
            return b_map, dot(c_map, b_map, 1, 1), carried * grow

        if l == 0:
            inp = filter_inputs()
            landed(c_recv.at[1:n_tp], c_rs)
            total = c_recv[0].astype(F32)
            for k in range(1, n_tp):
                total = total + c_recv[k].astype(F32)
            mrows[...] = jnp.concatenate([total[:n_rows], total[n_rows:]], axis=1)
            for i in range(layers):
                for s in range(seqs):
                    n = i * per_layer + s * keep
                    padded_m[i, s, FRONT - keep : FRONT, :] = mrows[n : n + keep, :]
            raw = unpack_maps()
            for i in range(1, layers):
                for k in [*[2 * j for j in z_peers], 1]:
                    for which in range(2):
                        fetch(i, k, which).start()
                for which in range(2):
                    w_rows[i, rows_of(tp, which), :] = w_sorted[i, pick_rows(tp, which), :]
            b_map, cross, carried = filter_maps(raw)
        else:
            b_map, cross, carried = filter_maps(acc[:, LANES:])
            inp = filter_inputs()
        inp_b = inp.astype(BF16)
        within = jnp.concatenate(
            [
                dot((cross * segs[h]).astype(BF16), inp_b[:, h * head_size : (h + 1) * head_size])
                for h in range(heads)
            ],
            axis=1,
        )
        inner = within + carried + skip_x[l] * inp
        acc = await_part(l, 2)
        gate = (acc * factor).astype(BF16).astype(F32)
        gate = gate * jax.nn.sigmoid(gate)
        read = inner * gate
        power = read * read
        p_hi = power.astype(BF16)
        p_lo = (power - p_hi.astype(F32)).astype(BF16)
        mean = (dot(p_hi, ones) + dot(p_lo, ones)) / head_size
        headout = (read * lax.rsqrt(mean + EPS) * gain[l : l + 1, :] * mask).astype(BF16)
        h_recv[l, 0, 0] = headout
        own = h_recv.at[l, 0, 0]
        targets = [(1, 0)] + [(i, k) for k in near_first for i in (0, 1)]
        for i, k in targets:
            remote(own, h_recv.at[l, i, k], h_rs.at[l, k], at(i, k)).start()

        def push(k):
            value = jnp.concatenate([h_recv[l, 0, k], h_recv[l, 1, k]], axis=1)
            block = jnp.bitwise_xor(dp, k)
            o_send[l, k] = dot(value, wout[l].reshape(2 * hp_cols, half)).astype(BF16)
            for j in z_peers:
                remote(
                    o_send.at[l, k], o_recv.at[l, j, k], o_rs.at[l, k],
                    {"tp": jnp.bitwise_xor(tp, 2 * j)},
                ).start()

        if l == 0:
            swap.wait_recv()
        landed(h_recv.at[l, 1, 0], h_rs.at[l, 0])
        push(0)
        last_x = jnp.concatenate(
            [
                jnp.broadcast_to(sums_x[(s + 1) * slots - 1 : (s + 1) * slots, :], (slots, hp_cols))
                for s in range(seqs)
            ],
            axis=0,
        )
        weighted = (jnp.exp(last_x - sums_x) * step_x * inp).astype(BF16)
        rows_sum = sum(dot(ext, piece, 1, 1) for piece in sums_parts)
        for s in range(seqs):
            span = slice(s * slots, (s + 1) * slots)
            fresh = dot(weighted[span], b_map[span], 0, 0)
            end = (s + 1) * slots - 1
            ssm[l, s] = jnp.exp(rows_sum[:, end : end + 1]) * state[l, s] + fresh
        if l + 1 < layers:
            pltpu.make_async_copy(w_gate.at[l + 1], w_gate.at[l + 1], g_sem.at[l + 1]).wait()
            weight = flat_weight(l + 1)
            r, c = grid(LANES, 2 * LANES)
            for which in range(2):
                picker = ones_where(c == 2 * r + which)
                for n in range(0, d_here, LANES):
                    w_flat[l, which, n : n + LANES] = dot(picker, weight[2 * n : 2 * (n + LANES)]).astype(BF16)
        for k in near_first:
            landed(h_recv.at[l, :, k], h_rs.at[l, k])
            push(k)

        r, c = grid(LANES, LANES)
        if l == 0:
            r = (r + LANES - ng * tp) & (LANES - 1)
        unsort = ones_where(
            c == (over(r, ng) & 1) * map_cols + groups * (r & (ng - 1)) + over(r, pair_cols)
        )
        own_maps = dot((await_part(l, 3) * factor).astype(BF16), unsort)
        for s in range(seqs):
            pick = lax.broadcasted_iota(jnp.int32, (8, FRONT + slots), 0)
            spot = lax.broadcasted_iota(jnp.int32, (8, FRONT + slots), 1)
            chooser = ((spot == pick + lens[s] + (FRONT - keep)) & (pick < keep)).astype(BF16)
            kept = dot(chooser, padded[l, s].astype(BF16)).astype(BF16)
            r, c = grid(8, slots)
            later_pick = ones_where((c == r + lens[s] - keep) & (r < keep))
            maps_kept = dot(later_pick, own_maps[s * slots : (s + 1) * slots].astype(BF16))
            for t in range(keep):
                kept_u[l, t, s : s + 1, :] = kept[t : t + 1]
                old = jnp.zeros((1, LANES), F32)
                for n in range(keep):
                    flat = jnp.concatenate(
                        [cache_m[l, s, n].astype(F32)[which : which + 1] for which in range(2)], axis=1
                    )
                    old = jnp.where(t + lens[s] == n, flat, old)
                line = (maps_kept[t : t + 1] + old).astype(BF16)
                for which in range(2):
                    kept_m[l, s, t, which : which + 1, :] = line[:, which * map_cols : (which + 1) * map_cols]

        def gather(k):
            landed(o_recv.at[l, 1:n_z, k], o_rs.at[l, k])
            o_recv[l, 0, k] = o_send[l, k]
            block = jnp.bitwise_xor(dp, k)
            total = o_recv[l, zed, k].astype(F32)
            for z in range(1, n_z):
                total = total + o_recv[l, jnp.bitwise_xor(zed, z), k].astype(F32)
            nb[l, side, block] = total.astype(BF16)
            remote(
                nb.at[l, side, block], nb.at[l, side, block], n_rs.at[l], at(1, 0)
            ).start()

        if l == 0:
            for i in range(1, layers):
                fetched(i, 1)
                for j in z_peers:
                    for which in range(2):
                        relay(i, j, which).start()
        order = [0, *near_first]
        for k in order:
            gather(k)
        landed(nb.at[l, 1 - side], n_rs.at[l])
        for h in range(2):
            stream[:, h * half : (h + 1) * half] += nb[l, h].astype(F32).reshape(tokens, half)

    for c in sends:
        c.wait_send()
    swap.wait_send()
    for l in range(layers):
        if l == 0:
            for i, j in others:
                remote(m_send.at[l, 0, 0], m_recv.at[l, 0], m_rs, at(i, j)).wait_send()
        else:
            for which in range(2):
                for k in [*[2 * j for j in z_peers], 1]:
                    fetch(l, k, which).wait_send()
                for j in z_peers:
                    relay(l, j, which).wait_send()
        for k in dp_peers:
            for p in range(4):
                part(l, p, k).wait_send()
        for i, k in [(1, 0)] + [(i, k) for k in near_first for i in (0, 1)]:
            remote(
                h_recv.at[l, 0, 0], h_recv.at[l, i, k], h_rs.at[l, k], at(i, k)
            ).wait_send()
        for k in range(n_dp):
            for j in z_peers:
                remote(
                    o_send.at[l, k], o_recv.at[l, j, k], o_rs.at[l, k], at(2 * j, 0)
                ).wait_send()
            remote(nb.at[l, 0, 0], nb.at[l, 0, 0], n_rs.at[l], at(1, 0)).wait_send()


def finish(stream, kept_u, kept_m, ssm, stream_out, kept_u_out, kept_m_out, ssm_out, sems):
    pairs = ((ssm, ssm_out), (stream, stream_out), (kept_u, kept_u_out), (kept_m, kept_m_out))
    copies = [pltpu.make_async_copy(a, b, sems.at[i]) for i, (a, b) in enumerate(pairs)]
    for c in copies:
        c.start()
    for c in copies:
        c.wait()


def fits(n_tp, n_dp, heads, hp_cols, map_cols, n_state, rows, d_here, keep):
    groups = map_cols * n_tp // n_state
    powers = all(n & (n - 1) == 0 for n in (n_tp, n_dp, groups, map_cols // groups))
    return (
        powers and n_tp > 1 and n_dp > 1 and n_tp * n_dp <= 64 and n_tp % groups == 0 and map_cols % groups == 0
        and hp_cols % LANES == 0 and 2 * map_cols == LANES and n_state == LANES
        and rows * 2 * (map_cols // groups) == 8 * LANES and d_here % (2 * LANES) == 0
        and keep <= FRONT and heads <= LANES - 2
    )


def body(n_tp, n_dp, *args):
    (
        tokens, lengths, input_norm_scale, gate_input_weight, maps_weight, step_weight,
        input_tap_weight, map_tap_weight, step_size_bias, decay_rate_logarithm, direct_path_weight,
        head_norm_scale, output_weight, convolution_input_cache, convolution_map_cache,
        recurrent_state, extra_log_decay,
    ) = args
    layers, seqs, slots, heads = extra_log_decay.shape
    head_size, n_state = recurrent_state.shape[3:]
    hp_cols = heads * head_size
    map_cols = maps_weight.shape[3]
    rows = seqs * slots
    d_here = tokens.shape[1]
    keep = convolution_input_cache.shape[2]
    if not fits(n_tp, n_dp, heads, hp_cols, map_cols, n_state, rows, d_here, keep):
        return general_body(n_tp, n_dp, *args)
    groups = map_cols * n_tp // n_state
    n_z = n_tp // 2
    taps_n = keep + 1
    n_rows = -(-layers * (seqs * keep + taps_n) // 8) * 8

    state = recurrent_state.reshape(layers, seqs, hp_cols, n_state)
    operands = [
        lengths, tokens, input_norm_scale, gate_input_weight,
        jnp.transpose(maps_weight, (0, 2, 3, 1)).reshape(layers, 2 * map_cols, d_here),
        jnp.transpose(step_weight, (0, 2, 1)),
        input_tap_weight, map_tap_weight, step_size_bias, decay_rate_logarithm, direct_path_weight, head_norm_scale,
        jnp.transpose(convolution_input_cache, (0, 2, 1, 3)), convolution_map_cache,
        jnp.transpose(extra_log_decay, (0, 1, 3, 2)), state, output_weight,
    ]
    vmem = pl.BlockSpec(memory_space=pltpu.VMEM)
    hbm = pl.BlockSpec(memory_space=pltpu.HBM)
    sems = lambda *n: pltpu.SemaphoreType.DMA((layers, *n))
    held = [pltpu.VMEM(a.shape, a.dtype) for a in operands[1:-1]]
    held[2] = pltpu.VMEM((layers, hp_cols // LANES, d_here, 2, LANES), BF16)
    results = (
        jax.ShapeDtypeStruct(tokens.shape, F32),
        jax.ShapeDtypeStruct((layers, keep, seqs, hp_cols), BF16),
        jax.ShapeDtypeStruct((layers, seqs, keep, 2, map_cols), BF16),
        jax.ShapeDtypeStruct(state.shape, F32),
    )
    made = pl.pallas_call(
        functools.partial(
            kernel, n_tp, n_dp, d_here * n_dp, groups,
            (layers, seqs, slots, heads, head_size, n_state, hp_cols, map_cols),
        ),
        out_shape=results,
        in_specs=[hbm] * len(operands),
        out_specs=(vmem,) * len(results),
        scratch_shapes=[
            pltpu.SMEM(lengths.shape, jnp.int32),
            *held,
            pltpu.VMEM((layers, 2, hp_cols, d_here // 2), BF16),
            pltpu.SemaphoreType.DMA((len(operands),)),
            sems(),
            *[
                pltpu.VMEM((layers, n, rows, width), BF16)
                for width in (LANES + 2 * n_state, hp_cols, hp_cols, LANES)
                for n in (n_dp, n_dp - 1)
            ],
            pltpu.VMEM((layers, groups, n_dp, 8, LANES), BF16),
            pltpu.VMEM((layers, n_dp * n_tp, 8, LANES), BF16),
            pltpu.VMEM((groups, 2 * n_rows, LANES), BF16),
            pltpu.VMEM((n_tp, 2 * n_rows, LANES), BF16),
            pltpu.VMEM((layers, 2, n_dp, rows, hp_cols), BF16),
            pltpu.VMEM((layers, n_dp, rows, d_here // 2), BF16),
            pltpu.VMEM((layers, n_z, n_dp, rows, d_here // 2), BF16),
            pltpu.VMEM((layers, 2, n_dp, rows, d_here // 2), BF16),
            pltpu.VMEM((layers, seqs, FRONT + slots, hp_cols), F32),
            pltpu.VMEM((layers, seqs, FRONT + slots, 2 * n_state), F32),
            pltpu.VMEM((2, n_rows, LANES), F32),
            pltpu.VMEM((n_rows, 2 * n_state), F32),
            pltpu.VMEM((layers, LANES + 2 * n_state, d_here), BF16),
            pltpu.VMEM((layers, LANES, d_here), BF16),
            pltpu.VMEM((max(layers - 1, 1), 2, d_here, hp_cols), BF16),
            pltpu.VMEM((layers, 8, hp_cols), F32),
            pltpu.VMEM((layers, 8, LANES), F32),
            pltpu.VMEM((layers, LANES, LANES), F32),
            pltpu.SemaphoreType.DMA,
            sems(4),
            pltpu.SemaphoreType.DMA,
            pltpu.SemaphoreType.DMA,
            sems(n_dp),
            sems(n_dp),
            sems(),
            pltpu.SemaphoreType.DMA,
            pltpu.SemaphoreType.DMA((2 * max(layers - 1, 1),)),
        ],
        compiler_params=pltpu.CompilerParams(
            collective_id=0, has_side_effects=True, vmem_limit_bytes=32 * 2**20
        ),
        name="mixer",
    )(*[pltpu.with_memory_space_constraint(a, pltpu.HBM) for a in operands])
    stream, conv_in, conv_maps, ssm = pl.pallas_call(
        finish,
        out_shape=results,
        in_specs=[vmem] * len(results),
        out_specs=(hbm,) * len(results),
        scratch_shapes=[pltpu.SemaphoreType.DMA((len(results),))],
        compiler_params=pltpu.CompilerParams(vmem_limit_bytes=2**20),
        name="finish",
    )(*made)
    return stream, jnp.transpose(conv_in, (0, 2, 1, 3)), conv_maps, ssm.reshape(recurrent_state.shape)


def solution(mesh):
    placed = (
        P(None, "dp"),
        P("dp"),
        P(None, "dp"),
        P(None, "dp", None, "tp"),
        P(None, "dp", None, "tp"),
        P(None, "dp", "tp"),
        P(None, None, "tp"),
        P(None, None, None, "tp"),
        P(None, "tp"),
        P(None, "tp"),
        P(None, "tp"),
        P(None, "tp"),
        P(None, "tp", "dp"),
        P(None, "dp", None, "tp"),
        P(None, "dp", None, None, "tp"),
        P(None, "dp", "tp", None, None),
        P(None, "dp", None, "tp"),
    )
    return jax.shard_map(
        functools.partial(body, mesh.shape["tp"], mesh.shape["dp"]),
        mesh=mesh,
        in_specs=placed,
        out_specs=(
            P(None, "dp"),
            P(None, "dp", None, "tp"),
            P(None, "dp", None, None, "tp"),
            P(None, "dp", "tp", None, None),
        ),
        check_vma=False,
    )
```

```python
import functools

import jax
import jax.numpy as jnp
from jax import lax
from jax.experimental import pallas as pl
from jax.experimental.pallas import tpu as pltpu
from jax.sharding import PartitionSpec as P

EPS = 1e-06
LANES = 128
FRONT = 8
F32, BF16 = jnp.float32, jnp.bfloat16


def up(n):
    return -(-n // LANES) * LANES


def dot(a, b, ca=1, cb=0):
    return lax.dot_general(a, b, (((ca,), (cb,)), ((), ())), preferred_element_type=F32)


def thirds(a):
    high = a.astype(BF16)
    rest = a - high.astype(F32)
    middle = rest.astype(BF16)
    return high, middle, (rest - middle.astype(F32)).astype(BF16)


def grid(n_rows, n_cols):
    return (
        lax.broadcasted_iota(jnp.int32, (n_rows, n_cols), 0),
        lax.broadcasted_iota(jnp.int32, (n_rows, n_cols), 1),
    )


def over(a, n):
    return lax.shift_right_logical(a, jnp.full_like(a, n.bit_length() - 1))


def ones_where(cond):
    return jnp.where(cond, 1.0, 0.0).astype(BF16)


def far_first(k, me, n):
    upper = me // (n // 2)
    mirrored = n - 1 - me
    return upper * (k + (k - me + n) // n) + (1 - upper) * (n - 1 - k - (k - mirrored + n) // n)


def general_kernel(
    n_tp, n_dp, d_model, heads, groups, slots, seqs, hp_cols, map_cols,
    lens, x, scale, w_pair, w_maps, w_step, tap_u, tap_m, bias, rate, skip, gain, cache_u, cache_m, extra_t,
    state_hbm, wout_hbm,
    stream, kept, ssm,
    a_send, a_recv, m_send, m_recv, h_send, h_recv, o_send, o_recv, n_send, n_recv, padded, step_w, state, wout, taps, par, extra,
    a_ss, a_rs, m_ss, m_rs, h_ss, h_rs, o_ss, o_rs, n_ss, n_rs, s_sem, w_sem,
):
    tp, dp = lax.axis_index("tp"), lax.axis_index("dp")
    layers = w_pair.shape[0]
    rows = seqs * slots
    taps_n = tap_u.shape[1]
    keep = taps_n - 1
    zc = up(hp_cols)
    ng = map_cols // groups
    n_state = state.shape[-1]
    cut = stream.shape[0] // n_tp
    per = rows // cut
    head_size = hp_cols // heads

    state_copy = pltpu.make_async_copy(state_hbm, state, s_sem)
    wout_copy = pltpu.make_async_copy(wout_hbm, wout, w_sem)
    state_copy.start()
    wout_copy.start()
    barrier = pltpu.get_barrier_semaphore()
    for k in range(1, n_dp):
        pl.semaphore_signal(barrier, inc=1, device_id={"dp": lax.rem(dp + k, n_dp)})
    for k in range(1, n_tp):
        pl.semaphore_signal(barrier, inc=1, device_id={"tp": lax.rem(tp + k, n_tp)})

    stream[...] = x[...].astype(F32)
    slot = lax.broadcasted_iota(jnp.int32, (slots, 1), 0)
    mask = jnp.concatenate([(slot < lens[s]).astype(F32) for s in range(seqs)], axis=0)
    lane = lax.broadcasted_iota(jnp.int32, (1, LANES), 1)
    r, c = grid(rows, rows)
    causal = (over(r, slots) == over(c, slots)) & (c <= r)
    tri = ones_where(causal)
    r, c = grid(2 * map_cols, up(2 * map_cols))
    which = over(r, ng) & 1
    sel = ones_where(c == which * map_cols + groups * (r & (ng - 1)) + over(r, 2 * ng))
    r, c = grid(n_tp * 2 * ng, 2 * n_state)
    sel2 = ones_where(c == (over(r, ng) & 1) * n_state + over(r, 2 * ng) * ng + (r & (ng - 1)))
    r, c = grid(LANES, hp_cols)
    ex = ones_where(r == over(c, head_size))
    r, c = grid(hp_cols, LANES)
    ext = ones_where(c == over(r, head_size))
    r, c = grid(hp_cols, hp_cols)
    ones = ones_where(over(r, head_size) == over(c, head_size))
    r, c = grid(LANES, 2 * LANES)
    spread = ones_where(c == 2 * r)
    padded[...] = jnp.zeros_like(padded)
    step_w[...] = jnp.zeros_like(step_w)
    taps[...] = jnp.zeros_like(taps)
    par[...] = jnp.zeros_like(par)
    extra[...] = jnp.zeros_like(extra)
    for l in range(layers):
        step_w[l, :heads, :] = w_step[l]
        taps[l, :taps_n, :hp_cols] = tap_u[l].astype(F32)
        for t in range(taps_n):
            pair = tap_m[l, t].astype(F32)
            for which in range(2):
                at = zc + which * map_cols
                taps[l, t : t + 1, at : at + map_cols] = pair[which : which + 1]
        par[l, 0:1, :heads] = bias[l : l + 1, :]
        par[l, 1:2, :heads] = rate[l : l + 1, :]
        par[l, 2:3, :heads] = skip[l : l + 1, :]
        for s in range(seqs):
            extra[l, :heads, s * slots : (s + 1) * slots] = extra_t[l, s]
    extra_rows = [extra[l].T[:rows] for l in range(layers)]
    skip_x = [sum(dot(piece, ex) for piece in thirds(par[l]))[2:3] for l in range(layers)]
    sends = []

    def copy(src, dst, ss, rs, where):
        return pltpu.make_async_remote_copy(
            src_ref=src, dst_ref=dst, send_sem=ss, recv_sem=rs, device_id=where
        )

    for l in range(layers):
        st = stream[...]
        squares = jnp.sum(st * st, axis=1, keepdims=True)
        normed = (st * scale[l : l + 1, :]).astype(BF16)
        even = jnp.concatenate(
            [dot(normed[:, i : i + LANES], spread) for i in range(0, normed.shape[1], LANES)], axis=1
        )
        odd = pltpu.roll(even, 1, 1)
        pair = dot(jnp.concatenate([even.astype(BF16), odd.astype(BF16)], axis=0), w_pair[l])
        tokens = st.shape[0]
        tail = dot(normed, step_w[l], 1, 1)
        high = squares.astype(BF16).astype(F32)
        tail = jnp.where(lane == LANES - 2, high, jnp.where(lane == LANES - 1, squares - high, tail))
        part = jnp.concatenate(
            [pair[:tokens], pair[tokens:], dot(normed, w_maps[l], 1, 1), tail], axis=1
        ).astype(BF16)
        for b in range(n_dp):
            a_send[l, b] = part[b * rows : (b + 1) * rows]
        if l == 0:
            pl.semaphore_wait(barrier, n_dp - 1 + n_tp - 1)
        flights = []
        for k in range(1, n_dp):
            to = lax.rem(dp + k, n_dp)
            c = copy(a_send.at[l, to], a_recv.at[l, k - 1], a_ss.at[l, k - 1], a_rs.at[l, k - 1], {"dp": to})
            c.start()
            flights.append(c)
        sends += flights
        acc = a_send[l, dp].astype(F32)
        for k, c in enumerate(flights):
            c.wait_recv()
            acc = acc + a_recv[l, k].astype(F32)
        tail = acc[:, acc.shape[1] - LANES :]
        squares = tail[:, LANES - 2 : LANES - 1] + tail[:, LANES - 1 : LANES]
        factor = lax.rsqrt(squares / d_model + EPS)
        proj = (acc * factor).astype(BF16).astype(F32)

        conv_w = taps.shape[2]
        pieces = []
        for s in range(seqs):
            for t in range(keep):
                at = FRONT - keep + t
                padded[s, at : at + 1, :hp_cols] = cache_u[l, t].astype(F32)[s : s + 1]
                pair = cache_m[l, s, t].astype(F32)
                for which in range(2):
                    col = zc + which * map_cols
                    padded[s, at : at + 1, col : col + map_cols] = pair[which : which + 1]
            padded[s, FRONT : FRONT + slots, :] = proj[s * slots : (s + 1) * slots, zc : zc + conv_w]
            total = padded[s, FRONT - keep : FRONT - keep + slots, :] * taps[l, 0:1, :]
            for t in range(1, taps_n):
                at = FRONT - keep + t
                total = total + padded[s, at : at + slots, :] * taps[l, t : t + 1, :]
            pieces.append(total)
        filtered = jnp.concatenate(pieces, axis=0)
        filtered = filtered * jax.nn.sigmoid(filtered)
        maps = filtered[:, conv_w - up(2 * map_cols) :].astype(BF16)
        sorted_maps = dot(sel, maps, 1, 1)
        for g in range(groups):
            m_send[l, g] = sorted_maps[g * 2 * ng : (g + 1) * 2 * ng, :].astype(BF16)

        def group_of(rank):
            return rank * heads // (heads * n_tp // groups)

        flights = []
        for k in range(n_tp - 1):
            to = far_first(k, tp, n_tp)
            c = copy(m_send.at[l, group_of(to)], m_recv.at[l, tp], m_ss.at[l, k], m_rs.at[l, tp], {"tp": to})
            c.start()
            sends.append(c)
        m_recv[l, tp] = m_send[l, group_of(tp)]

        for s in range(seqs):
            pick = lax.broadcasted_iota(jnp.int32, (8, FRONT + slots), 0)
            place = lax.broadcasted_iota(jnp.int32, (8, FRONT + slots), 1)
            chooser = ((place == pick + lens[s] + (FRONT - keep)) & (pick < keep)).astype(BF16)
            kept[l, s] = dot(chooser, padded[s].astype(BF16)).astype(BF16)
        raw = proj[:, proj.shape[1] - LANES :] + par[l, 0:1, :]
        step = (jnp.maximum(raw, 0.0) + jnp.log1p(jnp.exp(-jnp.abs(raw)))) * mask
        step = jnp.where(lane < heads, step, 0.0)
        logdec = extra_rows[l] * mask - step * jnp.exp(par[l, 1:2, :])
        logdec = jnp.where(lane < heads, logdec, 0.0)
        parts = dot(tri, jnp.concatenate(thirds(logdec), axis=1))
        sums = parts[:, :LANES] + parts[:, LANES : 2 * LANES] + parts[:, 2 * LANES :]
        sums_t = sums.T
        step_t = step.T
        sums_parts, step_parts = thirds(sums), thirds(step)
        both = dot(jnp.concatenate(sums_parts + step_parts, axis=0), ex)
        sums_x = both[:rows] + both[rows : 2 * rows] + both[2 * rows : 3 * rows]
        step_x = both[3 * rows : 4 * rows] + both[4 * rows : 5 * rows] + both[5 * rows :]
        inp = filtered[:, :hp_cols]
        gate = proj[:, :hp_cols]
        last_x = jnp.concatenate(
            [
                jnp.broadcast_to(sums_x[(s + 1) * slots - 1 : (s + 1) * slots, :], (slots, hp_cols))
                for s in range(seqs)
            ],
            axis=0,
        )
        weighted = (jnp.exp(last_x - sums_x) * step_x * inp).astype(BF16)
        inp_b = inp.astype(BF16)
        grow = jnp.exp(sums_x)
        direct = skip_x[l] * inp
        gate = gate * jax.nn.sigmoid(gate)
        rows_sum = sum(dot(ext, piece, 1, 1) for piece in sums_parts)
        segs = []
        for h in range(heads):
            gap = sums[:, h : h + 1] - sums_t[h : h + 1, :]
            segs.append(jnp.exp(jnp.where(causal, gap, -jnp.inf)) * step_t[h : h + 1, :])

        if l == 0:
            state_copy.wait()
            wout_copy.wait()
        for k in range(1, n_tp):
            src = lax.rem(tp + n_tp - k, n_tp)
            copy(m_send.at[l, 0], m_recv.at[l, src], m_ss.at[l, 0], m_rs.at[l, src], {"tp": src}).wait_recv()
        got = m_recv[l].astype(F32).reshape(n_tp * 2 * ng, rows)
        both_maps = dot(got.T.astype(BF16), sel2).astype(BF16)
        b_map, c_map = both_maps[:, :n_state], both_maps[:, n_state:]
        cross = dot(c_map, b_map, 1, 1)
        within = jnp.concatenate(
            [
                dot((cross * segs[h]).astype(BF16), inp_b[:, h * head_size : (h + 1) * head_size])
                for h in range(heads)
            ],
            axis=1,
        )
        carried = jnp.concatenate(
            [
                dot(c_map[s * slots : (s + 1) * slots], state[l, s].astype(BF16), 1, 1)
                for s in range(seqs)
            ],
            axis=0,
        )
        read = (within + carried * grow + direct) * gate
        power = read * read
        p_hi = power.astype(BF16)
        p_lo = (power - p_hi.astype(F32)).astype(BF16)
        mean = (dot(p_hi, ones) + dot(p_lo, ones)) / head_size
        headout = (read * lax.rsqrt(mean + EPS) * gain[l : l + 1, :] * mask).astype(BF16)
        h_send[l] = headout
        flights = []
        for k in range(1, n_dp):
            to = lax.rem(dp + k, n_dp)
            c = copy(h_send.at[l], h_recv.at[l, k - 1], h_ss.at[l, k - 1], h_rs.at[l, k - 1], {"dp": to})
            c.start()
            flights.append(c)
        sends += flights

        def push(value, block):
            out = dot(value, wout[l]).astype(BF16)
            for i in range(per):
                to = block * per + i
                o_send[l, to] = out[i * cut : (i + 1) * cut]

                @pl.when(to != tp)
                def _():
                    copy(o_send.at[l, to], o_recv.at[l, tp], o_ss.at[l, to], o_rs.at[l, tp], {"tp": to}).start()

        push(headout, dp)
        for s in range(seqs):
            at = slice(s * slots, (s + 1) * slots)
            fresh = dot(weighted[at], b_map[at], 0, 0)
            end = (s + 1) * slots - 1
            ssm[l, s] = jnp.exp(rows_sum[:, end : end + 1]) * state[l, s] + fresh
        for k, c in enumerate(flights):
            c.wait_recv()
            push(h_recv[l, k], lax.rem(dp + n_dp - k - 1, n_dp))
        total = o_send[l, tp].astype(F32)
        for k in range(1, n_tp):
            src = lax.rem(tp + n_tp - k, n_tp)
            copy(o_send.at[l, src], o_recv.at[l, src], o_ss.at[l, src], o_rs.at[l, src], {"tp": src}).wait_recv()
            total = total + o_recv[l, src].astype(F32)
        fresh = total.astype(BF16)
        n_send[l] = fresh
        n_recv[l, tp] = fresh
        for k in range(n_tp - 1):
            to = far_first(k, tp, n_tp)
            c = copy(n_send.at[l], n_recv.at[l, tp], n_ss.at[l, k], n_rs.at[l, tp], {"tp": to})
            c.start()
            sends.append(c)
        for k in range(1, n_tp):
            src = lax.rem(tp + n_tp - k, n_tp)
            copy(n_send.at[l], n_recv.at[l, src], n_ss.at[l, 0], n_rs.at[l, src], {"tp": src}).wait_recv()
        stream[...] += n_recv[l].astype(F32).reshape(stream.shape)

    for c in sends:
        c.wait_send()
    for l in range(layers):
        for k in range(1, n_tp):
            to = lax.rem(tp + k, n_tp)
            copy(o_send.at[l, to], o_recv.at[l, tp], o_ss.at[l, to], o_rs.at[l, tp], {"tp": to}).wait_send()


def general_body(
    n_tp, n_dp,
    tokens, lengths, input_norm_scale, gate_input_weight, maps_weight, step_weight,
    input_tap_weight, map_tap_weight, step_size_bias, decay_rate_logarithm, direct_path_weight,
    head_norm_scale, output_weight, convolution_input_cache, convolution_map_cache,
    recurrent_state, extra_log_decay,
):
    layers, seqs, slots, heads = extra_log_decay.shape
    head_size, n_state = recurrent_state.shape[3:]
    hp_cols = heads * head_size
    map_cols = maps_weight.shape[3]
    groups = map_cols * n_tp // n_state
    ng = map_cols // groups
    rows = seqs * slots
    d_here = tokens.shape[1]
    keep = convolution_input_cache.shape[2]

    def wide(a):
        pad = up(a.shape[-1]) - a.shape[-1]
        return a if pad == 0 else jnp.pad(a, [(0, 0)] * (a.ndim - 1) + [(0, pad)])

    w_pair = wide(gate_input_weight.reshape(layers, 2 * d_here, hp_cols))
    w_maps = jnp.transpose(maps_weight, (0, 2, 3, 1)).reshape(layers, 2 * map_cols, d_here)
    if up(2 * map_cols) > 2 * map_cols:
        w_maps = jnp.pad(w_maps, ((0, 0), (0, up(2 * map_cols) - 2 * map_cols), (0, 0)))
    w_step = jnp.transpose(step_weight, (0, 2, 1))
    cache_u = jnp.transpose(convolution_input_cache, (0, 2, 1, 3))
    extra_t = jnp.transpose(extra_log_decay, (0, 1, 3, 2))
    state = recurrent_state.reshape(layers, seqs, hp_cols, n_state)

    vmem = pl.BlockSpec(memory_space=pltpu.VMEM)
    wide_cols = 2 * up(hp_cols) + up(2 * map_cols) + LANES
    anywhere = pl.BlockSpec(memory_space=pl.ANY)
    conv_w = up(hp_cols) + up(2 * map_cols)
    cut = tokens.shape[0] // n_tp
    sems = lambda n: pltpu.SemaphoreType.DMA((layers, n))
    args = [tokens, input_norm_scale, w_pair, w_maps, w_step, input_tap_weight,
        map_tap_weight, step_size_bias, decay_rate_logarithm, direct_path_weight, head_norm_scale,
        cache_u, convolution_map_cache, extra_t]
    stream, kept, ssm = pl.pallas_call(
        functools.partial(
            general_kernel, n_tp, n_dp, d_here * n_dp, heads, groups, slots, seqs, hp_cols, map_cols
        ),
        out_shape=(
            jax.ShapeDtypeStruct(tokens.shape, F32),
            jax.ShapeDtypeStruct((layers, seqs, 8, conv_w), BF16),
            jax.ShapeDtypeStruct(state.shape, F32),
        ),
        in_specs=[pl.BlockSpec(memory_space=pltpu.SMEM)] + [vmem] * len(args) + [anywhere] * 2,
        out_specs=(vmem, vmem, vmem),
        scratch_shapes=[
            pltpu.VMEM((layers, n_dp, rows, wide_cols), BF16),
            pltpu.VMEM((layers, n_dp - 1, rows, wide_cols), BF16),
            pltpu.VMEM((layers, groups, 2 * ng, rows), BF16),
            pltpu.VMEM((layers, n_tp, 2 * ng, rows), BF16),
            pltpu.VMEM((layers, rows, hp_cols), BF16),
            pltpu.VMEM((layers, n_dp - 1, rows, hp_cols), BF16),
            pltpu.VMEM((layers, n_tp, cut, d_here), BF16),
            pltpu.VMEM((layers, n_tp, cut, d_here), BF16),
            pltpu.VMEM((layers, cut, d_here), BF16),
            pltpu.VMEM((layers, n_tp, cut, d_here), BF16),
            pltpu.VMEM((seqs, FRONT + slots, conv_w), F32),
            pltpu.VMEM((layers, LANES, d_here), BF16),
            pltpu.VMEM(state.shape, F32),
            pltpu.VMEM(output_weight.shape, BF16),
            pltpu.VMEM((layers, 8, conv_w), F32),
            pltpu.VMEM((layers, 8, LANES), F32),
            pltpu.VMEM((layers, LANES, LANES), F32),
            sems(n_dp - 1), sems(n_dp - 1), sems(n_tp - 1), sems(n_tp), sems(n_dp - 1),
            sems(n_dp - 1), sems(n_tp), sems(n_tp), sems(n_tp - 1), sems(n_tp),
            pltpu.SemaphoreType.DMA, pltpu.SemaphoreType.DMA,
        ],
        compiler_params=pltpu.CompilerParams(
            collective_id=0, has_side_effects=True, vmem_limit_bytes=48 * 2**20
        ),
        name="mixer",
    )(lengths, *args, state, output_weight)
    conv_in = kept[:, :, :keep, :hp_cols]
    start = conv_w - up(2 * map_cols)
    conv_maps = kept[:, :, :keep, start : start + 2 * map_cols].reshape(
        layers, seqs, keep, 2, map_cols
    )
    return stream, conv_in, conv_maps, ssm.reshape(recurrent_state.shape)


def peers(n, order):
    return [k for k in order if 0 < k < n] + [k for k in range(1, n) if k not in order]


def kernel(
    n_tp, n_dp, d_model, groups, shapes,
    *refs,
):
    names = (
        "lens", "x", "scale", "gate", "w_maps", "w_step", "tap_u", "tap_m", "bias", "rate", "skip", "gain",
        "cache_u", "cache_m", "extra_t", "state", "wout",
    )
    hbm = dict(zip(names, refs[: len(names)]))
    (
        stream, kept_u, kept_m, ssm,
        lens, x, scale, w_gate, w_maps, w_step, tap_u, tap_m, bias, rate, skip, gain, cache_u, cache_m, extra_t, state,
        wout, in_sem, g_sem,
        t_send, t_recv, u_send, u_recv, z_send, z_recv, q_send, q_recv, m_send, m_recv, c_send, c_recv, h_recv, o_send, o_recv, nb,
        padded, padded_m, mrow, mrows, w_rows, w_sorted, w_flat, taps, par, extra,
        out_sem, a_rs, m_rs, c_rs, h_rs, o_rs, n_rs, w_rs, f_rs,
    ) = refs[len(names) :]
    layers, seqs, slots, heads, head_size, n_state, hp_cols, map_cols = shapes
    tp, dp = lax.axis_index("tp"), lax.axis_index("dp")
    rows = seqs * slots
    taps_n = tap_u.shape[1]
    keep = taps_n - 1
    ng = map_cols // groups
    pair_cols = 2 * ng
    quads = LANES // pair_cols
    d_here = x.shape[1]
    half = d_here // 2
    tokens = x.shape[0]
    side = lax.rem(tp, 2)
    zed = lax.div(tp, 2)
    n_z = n_tp // 2
    every = n_tp * n_dp
    me = dp * n_tp + tp
    dp_peers = peers(n_dp, (3, 1, 2))
    turns = peers(n_dp, (1, 2, 3))
    z_peers = peers(n_z, (3, 2, 1))

    def remote(src, dst, arrived, where):
        return pltpu.make_async_remote_copy(
            src_ref=src, dst_ref=dst, send_sem=out_sem, recv_sem=arrived, device_id=where
        )

    def landed(block, arrived):
        remote(block, block, arrived, {"tp": jnp.bitwise_xor(tp, 1)}).wait_recv()

    barrier = pltpu.get_barrier_semaphore()
    others = [
        (i, j) for i in [*peers(n_tp, (6, 7, 4, 5, 2, 3, 1)), 0] for j in [*dp_peers, 0] if i or j
    ]

    def at(i, j):
        return {"tp": jnp.bitwise_xor(tp, i), "dp": jnp.bitwise_xor(dp, j)}

    for i, j in others:
        pl.semaphore_signal(barrier, inc=1, device_id=at(i, j))

    local = {}
    pairs = dict(
        x=x, scale=scale, w_maps=w_maps, w_step=w_step, lens=lens, tap_u=tap_u, tap_m=tap_m, bias=bias, rate=rate,
        skip=skip, gain=gain, cache_u=cache_u, cache_m=cache_m, extra_t=extra_t, state=state,
    )
    for n, name in enumerate(pairs):
        local[name] = pltpu.make_async_copy(hbm[name], pairs[name], in_sem.at[n])
    mine = pl.ds(pl.multiple_of(side * half, LANES), half)
    theirs = pl.ds(pl.multiple_of((1 - side) * half, LANES), half)
    local["wout"] = pltpu.make_async_copy(hbm["wout"].at[:, :, mine], wout.at[:, 0], in_sem.at[len(pairs)])
    gate_copies = [
        [
            pltpu.make_async_copy(
                hbm["gate"].at[l, :, :, i : i + LANES], w_gate.at[l, i // LANES], g_sem.at[l]
            )
            for i in range(0, hp_cols, LANES)
        ]
        for l in range(layers)
    ]
    first = ("x", "scale", "w_maps", "w_step")
    for name in first:
        local[name].start()
    for c in gate_copies[0]:
        c.start()
    for name in local:
        if name not in first:
            local[name].start()
    for l in range(1, layers):
        for c in gate_copies[l]:
            c.start()

    lane = lax.broadcasted_iota(jnp.int32, (1, LANES), 1)
    r, c = grid(LANES, 4 * LANES)
    spread = ones_where(c == jnp.where(c < 2 * LANES, 2 * r, 2 * LANES + 2 * r + 1))
    r, c = grid(LANES, LANES)
    place = (c + LANES - ng * tp) & (LANES - 1)
    wanted = (over(place, ng) & 1) * map_cols + groups * (place & (ng - 1)) + over(place, pair_cols)
    sorter = ones_where(r == wanted)
    home = over((lane + LANES - ng * tp) & (LANES - 1), pair_cols)
    for l in range(layers):
        w_rows[l, :LANES] = jnp.zeros_like(w_rows[l, :LANES])
    gate_rows = w_gate.reshape(layers, hp_cols // LANES, 2 * d_here, LANES)

    def group_of(rank):
        return rank * groups // n_tp

    def with_squares(tail, squares):
        high = squares.astype(BF16).astype(F32)
        return jnp.where(lane == LANES - 2, high, jnp.where(lane == LANES - 1, squares - high, tail))

    def fill(buffer, l, value):
        for b in range(n_dp):
            buffer[l, b, :, : value.shape[1]] = value[b * rows : (b + 1) * rows].astype(BF16)

    def pack_maps(l, raw):
        turned = [raw if k == 0 else pltpu.roll(raw, k * pair_cols, 1) for k in range(quads)]
        turned = [t.reshape(n_dp, quads, 8, LANES) for t in turned]
        for g in range(groups):
            piece = turned[(0 - g) % quads][:, 0]
            for q in range(1, quads):
                piece = jnp.where((home == q)[None], turned[(q - g) % quads][:, q], piece)
            m_send[l, g] = piece.astype(BF16)

    def send_maps(l):
        for i, j in others:
            to = at(i, j)
            remote(
                m_send.at[l, group_of(to["tp"]), to["dp"]], m_recv.at[l, me], m_rs, to
            ).start()
        m_recv[l, me] = m_send[l, group_of(tp), dp]

    def rows_of(rank, which):
        return pl.ds(pl.multiple_of(LANES + which * n_state + ng * rank, ng), ng)

    def pick_rows(rank, which):
        return pl.ds(pl.multiple_of(pair_cols * group_of(rank) + which * ng, ng), ng)

    def fetch(i, k, which):
        to = jnp.bitwise_xor(tp, k)
        n = 2 * (i - 1) + (k == 1)
        return remote(
            w_sorted.at[i, pick_rows(to, which)], w_rows.at[i, rows_of(tp, which)], f_rs.at[n], {"tp": to}
        )

    def relay(i, j, which):
        n = 2 * (i - 1) + 1
        block = w_rows.at[i, rows_of(jnp.bitwise_xor(tp, 2 * j), which)]
        return remote(block, block, f_rs.at[n], at(1, 0))

    def fetched(i, far):
        n = 2 * (i - 1) + 1 - far
        landed(w_rows.at[i, pl.ds(LANES, 2 * ng * (n_z - 1 if far else n_z))], f_rs.at[n])

    parts_of = ((t_send, t_recv), (u_send, u_recv), (z_send, z_recv), (q_send, q_recv))

    def part(l, p, k):
        send, recv = parts_of[p]
        to = jnp.bitwise_xor(dp, k)
        src, dst = send.at[l, to], recv.at[l, k - 1]
        if p == 0 and l == 0:
            src, dst = src.at[:, :LANES], dst.at[:, :LANES]
        return remote(src, dst, a_rs.at[l, p], {"dp": to})

    def send_part(l, p):
        for k in dp_peers:
            part(l, p, k).start()

    def await_part(l, p):
        send, recv = parts_of[p]
        width = LANES if p == 0 and l == 0 else send.shape[-1]
        landed(recv.at[l, :, :, :width], a_rs.at[l, p])
        acc = send[l, dp, :, :width].astype(F32)
        for k in range(1, n_dp):
            acc = acc + recv[l, k - 1, :, :width].astype(F32)
        return acc

    def flat_weight(l):
        return jnp.concatenate([gate_rows[l, i] for i in range(hp_cols // LANES)], axis=1)

    sends = []
    for name in first:
        local[name].wait()
    for l in range(layers):
        w_rows[l, :heads, :] = w_step[l]
    w_sorted[0] = dot(sorter, w_maps[0], 0, 0).astype(BF16)
    stream[...] = x[...].astype(F32)

    for l in range(layers):
        if l == 0:
            st = stream[...]
            squares = jnp.sum(st * st, axis=1, keepdims=True)
            normed = (st * scale[l : l + 1, :]).astype(BF16)
            raw = dot(normed, w_sorted[l], 1, 1)
            pack_maps(l, raw)
            fill(t_send, l, with_squares(dot(normed, w_rows[l, :LANES], 1, 1), squares))
            spreads = [dot(normed[:, i : i + LANES], spread).astype(BF16) for i in range(0, d_here, LANES)]
            even = jnp.concatenate([s[:, : 2 * LANES] for s in spreads], axis=1)
            odd = jnp.concatenate([s[:, 2 * LANES :] for s in spreads], axis=1)
            pltpu.make_async_copy(w_gate.at[l], w_gate.at[l], g_sem.at[l]).wait()
            both = dot(jnp.concatenate([odd, even], axis=0), flat_weight(l))
            fill(u_send, l, both[:tokens])
            fill(z_send, l, both[tokens:])
            fill(q_send, l, raw)
            pl.semaphore_wait(barrier, every - 1)
            send_maps(l)
            for p in range(4):
                send_part(l, p)

        if l == 0:
            for n in range(len(pairs) + 1):
                name = [*pairs, "wout"][n]
                if name not in first:
                    local[name].wait()
            swap = remote(hbm["wout"].at[:, :, theirs], wout.at[:, 1], w_rs, {"tp": jnp.bitwise_xor(tp, 1)})
            swap.start()
            per_layer = seqs * keep + taps_n
            mrow[...] = jnp.zeros_like(mrow)
            for i in range(layers):
                for s in range(seqs):
                    for t in range(keep):
                        pair = cache_m[i, s, t].astype(F32)
                        n = i * per_layer + s * keep + t
                        for which in range(2):
                            mrow[which, n : n + 1, :map_cols] = pair[which : which + 1]
                for t in range(taps_n):
                    pair = tap_m[i, t].astype(F32)
                    n = i * per_layer + seqs * keep + t
                    for which in range(2):
                        mrow[which, n : n + 1, :map_cols] = pair[which : which + 1]
            n_rows = mrow.shape[1]
            r, c = grid(LANES, groups * LANES)
            n = (c & (LANES - 1)) - ng * tp
            chosen = (n >= 0) & (n < ng) & (r == groups * n + over(c, LANES))
            packed = dot(mrow[...].reshape(2 * n_rows, LANES).astype(BF16), ones_where(chosen)).astype(BF16)
            for g in range(groups):
                c_send[g] = packed[:, g * LANES : (g + 1) * LANES]
            for k in peers(n_tp, (6, 7, 4, 5, 2, 3, 1)):
                to = jnp.bitwise_xor(tp, k)
                c = remote(c_send.at[group_of(to)], c_recv.at[k], c_rs, {"tp": to})
                c.start()
                sends.append(c)
            c_recv[0] = c_send[group_of(tp)]
            r, c = grid(LANES, LANES)
            resort = ones_where(r == (over(c, ng) & 1) * map_cols + groups * (c & (ng - 1)) + over(c, pair_cols))
            for i in range(1, layers):
                w_sorted[i] = dot(resort, w_maps[i], 0, 0).astype(BF16)

            slot = lax.broadcasted_iota(jnp.int32, (slots, 1), 0)
            mask = jnp.concatenate([(slot < lens[s]).astype(F32) for s in range(seqs)], axis=0)
            r, c = grid(rows, rows)
            causal = (over(r, slots) == over(c, slots)) & (c <= r)
            tri = ones_where(causal)
            r, c = grid(LANES, hp_cols)
            ex = ones_where(r == over(c, head_size))
            r, c = grid(hp_cols, LANES)
            ext = ones_where(c == over(r, head_size))
            r, c = grid(hp_cols, hp_cols)
            ones = ones_where(over(r, head_size) == over(c, head_size))
            padded[...] = jnp.zeros_like(padded)
            padded_m[...] = jnp.zeros_like(padded_m)
            taps[...] = jnp.zeros_like(taps)
            par[...] = jnp.zeros_like(par)
            extra[...] = jnp.zeros_like(extra)
            for i in range(layers):
                taps[i, :taps_n, :] = tap_u[i].astype(F32)
                par[i, 0:1, :heads] = bias[i : i + 1, :]
                par[i, 1:2, :heads] = rate[i : i + 1, :]
                par[i, 2:3, :heads] = skip[i : i + 1, :]
                for s in range(seqs):
                    extra[i, :heads, s * slots : (s + 1) * slots] = extra_t[i, s]
                    for t in range(keep):
                        n = FRONT - keep + t
                        padded[i, s, n : n + 1, :] = cache_u[i, t].astype(F32)[s : s + 1]
            extra_rows = [extra[i].T[:rows] for i in range(layers)]
            skip_x = [sum(dot(piece, ex) for piece in thirds(par[i]))[2:3] for i in range(layers)]

        def convolve(pad, weights):
            pieces = []
            for s in range(seqs):
                total = pad[l, s, FRONT - keep : FRONT - keep + slots, :] * weights[0:1]
                for t in range(1, taps_n):
                    n = FRONT - keep + t
                    total = total + pad[l, s, n : n + slots, :] * weights[t : t + 1]
                pieces.append(total)
            out = jnp.concatenate(pieces, axis=0)
            return out * jax.nn.sigmoid(out)

        acc = await_part(l, 0)
        tail = acc[:, :LANES]
        squares = tail[:, LANES - 2 : LANES - 1] + tail[:, LANES - 1 : LANES]
        factor = lax.rsqrt(squares / d_model + EPS)
        raw_step = (tail * factor).astype(BF16).astype(F32) + par[l, 0:1, :]
        step = (jnp.maximum(raw_step, 0.0) + jnp.log1p(jnp.exp(-jnp.abs(raw_step)))) * mask
        step = jnp.where(lane < heads, step, 0.0)
        logdec = extra_rows[l] * mask - step * jnp.exp(par[l, 1:2, :])
        logdec = jnp.where(lane < heads, logdec, 0.0)
        parts = dot(tri, jnp.concatenate(thirds(logdec), axis=1))
        sums = parts[:, :LANES] + parts[:, LANES : 2 * LANES] + parts[:, 2 * LANES :]
        sums_t = sums.T
        step_t = step.T
        sums_parts, step_parts = thirds(sums), thirds(step)
        both = dot(jnp.concatenate(sums_parts + step_parts, axis=0), ex)
        sums_x = both[:rows] + both[rows : 2 * rows] + both[2 * rows : 3 * rows]
        step_x = both[3 * rows : 4 * rows] + both[4 * rows : 5 * rows] + both[5 * rows :]
        grow = jnp.exp(sums_x)
        segs = []
        for h in range(heads):
            gap = sums[:, h : h + 1] - sums_t[h : h + 1, :]
            segs.append(jnp.exp(jnp.where(causal, gap, -jnp.inf)) * step_t[h : h + 1, :])

        def filter_inputs():
            proj = (await_part(l, 1) * factor).astype(BF16).astype(F32)
            for s in range(seqs):
                padded[l, s, FRONT : FRONT + slots, :] = proj[s * slots : (s + 1) * slots]
            return convolve(padded, taps[l])

        def unpack_maps():
            landed(m_recv.at[l, 0 : every - 1], m_rs)
            got = m_recv[l].astype(F32).reshape(n_dp, n_tp, 8, LANES)
            got = sum(got[b] for b in range(n_dp))
            cell = over(lane, ng)
            columns = []
            for which in range(2):
                blocks = []
                for q in range(quads):
                    n = 2 * q + which
                    piece = got[0]
                    for t in range(1, n_tp):
                        piece = jnp.where(cell == (n + t) % n_tp, got[t], piece)
                    blocks.append(piece if n == 0 else pltpu.roll(piece, LANES - ng * n, 1))
                columns.append(jnp.concatenate(blocks, axis=0))
            return jnp.concatenate(columns, axis=1)

        def filter_maps(raw):
            proj = (raw * factor).astype(BF16).astype(F32)
            for s in range(seqs):
                padded_m[l, s, FRONT : FRONT + slots, :] = proj[s * slots : (s + 1) * slots]
            n = l * per_layer + seqs * keep
            maps = convolve(padded_m, mrows[n : n + taps_n, :]).astype(BF16)
            b_map, c_map = maps[:, :n_state], maps[:, n_state:]
            carried = jnp.concatenate(
                [
                    dot(c_map[s * slots : (s + 1) * slots], state[l, s].astype(BF16), 1, 1)
                    for s in range(seqs)
                ],
                axis=0,
            )
            return b_map, dot(c_map, b_map, 1, 1), carried * grow

        if l == 0:
            inp = filter_inputs()
            landed(c_recv.at[1:n_tp], c_rs)
            total = c_recv[0].astype(F32)
            for k in range(1, n_tp):
                total = total + c_recv[k].astype(F32)
            mrows[...] = jnp.concatenate([total[:n_rows], total[n_rows:]], axis=1)
            for i in range(layers):
                for s in range(seqs):
                    n = i * per_layer + s * keep
                    padded_m[i, s, FRONT - keep : FRONT, :] = mrows[n : n + keep, :]
            raw = unpack_maps()
            for i in range(1, layers):
                for k in [*[2 * j for j in z_peers], 1]:
                    for which in range(2):
                        fetch(i, k, which).start()
                for which in range(2):
                    w_rows[i, rows_of(tp, which), :] = w_sorted[i, pick_rows(tp, which), :]
            b_map, cross, carried = filter_maps(raw)
        else:
            b_map, cross, carried = filter_maps(acc[:, LANES:])
            inp = filter_inputs()
        inp_b = inp.astype(BF16)
        within = jnp.concatenate(
            [
                dot((cross * segs[h]).astype(BF16), inp_b[:, h * head_size : (h + 1) * head_size])
                for h in range(heads)
            ],
            axis=1,
        )
        inner = within + carried + skip_x[l] * inp
        acc = await_part(l, 2)
        gate = (acc * factor).astype(BF16).astype(F32)
        gate = gate * jax.nn.sigmoid(gate)
        read = inner * gate
        power = read * read
        p_hi = power.astype(BF16)
        p_lo = (power - p_hi.astype(F32)).astype(BF16)
        mean = (dot(p_hi, ones) + dot(p_lo, ones)) / head_size
        headout = (read * lax.rsqrt(mean + EPS) * gain[l : l + 1, :] * mask).astype(BF16)
        h_recv[l, 0, 0] = headout
        own = h_recv.at[l, 0, 0]
        targets = [(1, 0)] + [(i, k) for k in turns for i in (0, 1)]
        for i, k in targets:
            remote(own, h_recv.at[l, i, k], h_rs.at[l, k], at(i, k)).start()

        def push(k):
            value = jnp.concatenate([h_recv[l, 0, k], h_recv[l, 1, k]], axis=1)
            block = jnp.bitwise_xor(dp, k)
            o_send[l, k] = dot(value, wout[l].reshape(2 * hp_cols, half)).astype(BF16)
            for j in z_peers:
                remote(
                    o_send.at[l, k], o_recv.at[l, j, k], o_rs.at[l, k],
                    {"tp": jnp.bitwise_xor(tp, 2 * j)},
                ).start()

        if l == 0:
            swap.wait_recv()
        landed(h_recv.at[l, 1, 0], h_rs.at[l, 0])
        push(0)
        last_x = jnp.concatenate(
            [
                jnp.broadcast_to(sums_x[(s + 1) * slots - 1 : (s + 1) * slots, :], (slots, hp_cols))
                for s in range(seqs)
            ],
            axis=0,
        )
        weighted = (jnp.exp(last_x - sums_x) * step_x * inp).astype(BF16)
        rows_sum = sum(dot(ext, piece, 1, 1) for piece in sums_parts)
        for s in range(seqs):
            span = slice(s * slots, (s + 1) * slots)
            fresh = dot(weighted[span], b_map[span], 0, 0)
            end = (s + 1) * slots - 1
            ssm[l, s] = jnp.exp(rows_sum[:, end : end + 1]) * state[l, s] + fresh
        if l + 1 < layers:
            pltpu.make_async_copy(w_gate.at[l + 1], w_gate.at[l + 1], g_sem.at[l + 1]).wait()
            weight = flat_weight(l + 1)
            r, c = grid(LANES, 2 * LANES)
            for which in range(2):
                picker = ones_where(c == 2 * r + which)
                for n in range(0, d_here, LANES):
                    w_flat[l, which, n : n + LANES] = dot(picker, weight[2 * n : 2 * (n + LANES)]).astype(BF16)
        for k in turns:
            landed(h_recv.at[l, :, k], h_rs.at[l, k])
            push(k)

        r, c = grid(LANES, LANES)
        if l == 0:
            r = (r + LANES - ng * tp) & (LANES - 1)
        unsort = ones_where(
            c == (over(r, ng) & 1) * map_cols + groups * (r & (ng - 1)) + over(r, pair_cols)
        )
        own_maps = dot((await_part(l, 3) * factor).astype(BF16), unsort)
        for s in range(seqs):
            pick = lax.broadcasted_iota(jnp.int32, (8, FRONT + slots), 0)
            spot = lax.broadcasted_iota(jnp.int32, (8, FRONT + slots), 1)
            chooser = ((spot == pick + lens[s] + (FRONT - keep)) & (pick < keep)).astype(BF16)
            kept = dot(chooser, padded[l, s].astype(BF16)).astype(BF16)
            r, c = grid(8, slots)
            later_pick = ones_where((c == r + lens[s] - keep) & (r < keep))
            maps_kept = dot(later_pick, own_maps[s * slots : (s + 1) * slots].astype(BF16))
            for t in range(keep):
                kept_u[l, t, s : s + 1, :] = kept[t : t + 1]
                old = jnp.zeros((1, LANES), F32)
                for n in range(keep):
                    flat = jnp.concatenate(
                        [cache_m[l, s, n].astype(F32)[which : which + 1] for which in range(2)], axis=1
                    )
                    old = jnp.where(t + lens[s] == n, flat, old)
                line = (maps_kept[t : t + 1] + old).astype(BF16)
                for which in range(2):
                    kept_m[l, s, t, which : which + 1, :] = line[:, which * map_cols : (which + 1) * map_cols]

        def gather(k):
            landed(o_recv.at[l, 1:n_z, k], o_rs.at[l, k])
            o_recv[l, 0, k] = o_send[l, k]
            block = jnp.bitwise_xor(dp, k)
            total = o_recv[l, zed, k].astype(F32)
            for z in range(1, n_z):
                total = total + o_recv[l, jnp.bitwise_xor(zed, z), k].astype(F32)
            nb[l, side, block] = total.astype(BF16)
            remote(
                nb.at[l, side, block], nb.at[l, side, block], n_rs.at[l, k], at(1, 0)
            ).start()

        if l == 0:
            for i in range(1, layers):
                fetched(i, 1)
                for j in z_peers:
                    for which in range(2):
                        relay(i, j, which).start()
        def receive(k):
            landed(nb.at[l, 1 - side, jnp.bitwise_xor(dp, k)], n_rs.at[l, k])
            block = jnp.bitwise_xor(dp, k)
            span = pl.ds(pl.multiple_of(block * rows, rows), rows)
            st = stream[span, :] + jnp.concatenate([nb[l, h, block].astype(F32) for h in range(2)], axis=1)
            stream[span, :] = st
            n = l + 1
            if n == layers:
                return
            squares = jnp.sum(st * st, axis=1, keepdims=True)
            normed = (st * scale[n : n + 1, :]).astype(BF16)
            tail = dot(normed, w_rows[n], 1, 1)
            tail = jnp.concatenate([with_squares(tail[:, :LANES], squares), tail[:, LANES:]], axis=1)
            t_send[n, block] = tail.astype(BF16)
            if k:
                part(n, 0, k).start()
            u_send[n, block] = dot(normed, w_flat[l, 1]).astype(BF16)
            if k:
                part(n, 1, k).start()
            z_send[n, block] = dot(normed, w_flat[l, 0]).astype(BF16)
            if k:
                part(n, 2, k).start()
            q_send[n, block] = dot(normed, w_sorted[n], 1, 1).astype(BF16)
            if k:
                part(n, 3, k).start()

        order = [0, *turns]
        gather(order[0])
        for n in range(1, len(order)):
            gather(order[n])
            if n == 1 and l + 1 < layers:
                fetched(l + 1, 0)
            receive(order[n - 1])
        receive(order[-1])

    for c in sends:
        c.wait_send()
    swap.wait_send()
    for l in range(layers):
        if l == 0:
            for i, j in others:
                remote(m_send.at[l, 0, 0], m_recv.at[l, 0], m_rs, at(i, j)).wait_send()
        else:
            for which in range(2):
                for k in [*[2 * j for j in z_peers], 1]:
                    fetch(l, k, which).wait_send()
                for j in z_peers:
                    relay(l, j, which).wait_send()
        for k in dp_peers:
            for p in range(4):
                part(l, p, k).wait_send()
        for i, k in [(1, 0)] + [(i, k) for k in turns for i in (0, 1)]:
            remote(
                h_recv.at[l, 0, 0], h_recv.at[l, i, k], h_rs.at[l, k], at(i, k)
            ).wait_send()
        for k in range(n_dp):
            for j in z_peers:
                remote(
                    o_send.at[l, k], o_recv.at[l, j, k], o_rs.at[l, k], at(2 * j, 0)
                ).wait_send()
            remote(nb.at[l, 0, 0], nb.at[l, 0, 0], n_rs.at[l, k], at(1, 0)).wait_send()


def finish(stream, kept_u, kept_m, ssm, stream_out, kept_u_out, kept_m_out, ssm_out, sems):
    pairs = ((ssm, ssm_out), (stream, stream_out), (kept_u, kept_u_out), (kept_m, kept_m_out))
    copies = [pltpu.make_async_copy(a, b, sems.at[i]) for i, (a, b) in enumerate(pairs)]
    for c in copies:
        c.start()
    for c in copies:
        c.wait()


def fits(n_tp, n_dp, heads, hp_cols, map_cols, n_state, rows, d_here, keep):
    groups = map_cols * n_tp // n_state
    powers = all(n & (n - 1) == 0 for n in (n_tp, n_dp, groups, map_cols // groups))
    return (
        powers and n_tp > 1 and n_dp > 1 and n_tp * n_dp <= 64 and n_tp % groups == 0 and map_cols % groups == 0
        and hp_cols % LANES == 0 and 2 * map_cols == LANES and n_state == LANES
        and rows * 2 * (map_cols // groups) == 8 * LANES and d_here % (2 * LANES) == 0
        and keep <= FRONT and heads <= LANES - 2
    )


def body(n_tp, n_dp, *args):
    (
        tokens, lengths, input_norm_scale, gate_input_weight, maps_weight, step_weight,
        input_tap_weight, map_tap_weight, step_size_bias, decay_rate_logarithm, direct_path_weight,
        head_norm_scale, output_weight, convolution_input_cache, convolution_map_cache,
        recurrent_state, extra_log_decay,
    ) = args
    layers, seqs, slots, heads = extra_log_decay.shape
    head_size, n_state = recurrent_state.shape[3:]
    hp_cols = heads * head_size
    map_cols = maps_weight.shape[3]
    rows = seqs * slots
    d_here = tokens.shape[1]
    keep = convolution_input_cache.shape[2]
    if not fits(n_tp, n_dp, heads, hp_cols, map_cols, n_state, rows, d_here, keep):
        return general_body(n_tp, n_dp, *args)
    groups = map_cols * n_tp // n_state
    n_z = n_tp // 2
    taps_n = keep + 1
    n_rows = -(-layers * (seqs * keep + taps_n) // 8) * 8

    state = recurrent_state.reshape(layers, seqs, hp_cols, n_state)
    operands = [
        lengths, tokens, input_norm_scale, gate_input_weight,
        jnp.transpose(maps_weight, (0, 2, 3, 1)).reshape(layers, 2 * map_cols, d_here),
        jnp.transpose(step_weight, (0, 2, 1)),
        input_tap_weight, map_tap_weight, step_size_bias, decay_rate_logarithm, direct_path_weight, head_norm_scale,
        jnp.transpose(convolution_input_cache, (0, 2, 1, 3)), convolution_map_cache,
        jnp.transpose(extra_log_decay, (0, 1, 3, 2)), state, output_weight,
    ]
    vmem = pl.BlockSpec(memory_space=pltpu.VMEM)
    hbm = pl.BlockSpec(memory_space=pltpu.HBM)
    sems = lambda *n: pltpu.SemaphoreType.DMA((layers, *n))
    held = [pltpu.VMEM(a.shape, a.dtype) for a in operands[1:-1]]
    held[2] = pltpu.VMEM((layers, hp_cols // LANES, d_here, 2, LANES), BF16)
    results = (
        jax.ShapeDtypeStruct(tokens.shape, F32),
        jax.ShapeDtypeStruct((layers, keep, seqs, hp_cols), BF16),
        jax.ShapeDtypeStruct((layers, seqs, keep, 2, map_cols), BF16),
        jax.ShapeDtypeStruct(state.shape, F32),
    )
    made = pl.pallas_call(
        functools.partial(
            kernel, n_tp, n_dp, d_here * n_dp, groups,
            (layers, seqs, slots, heads, head_size, n_state, hp_cols, map_cols),
        ),
        out_shape=results,
        in_specs=[hbm] * len(operands),
        out_specs=(vmem,) * len(results),
        scratch_shapes=[
            pltpu.SMEM(lengths.shape, jnp.int32),
            *held,
            pltpu.VMEM((layers, 2, hp_cols, d_here // 2), BF16),
            pltpu.SemaphoreType.DMA((len(operands),)),
            sems(),
            *[
                pltpu.VMEM((layers, n, rows, width), BF16)
                for width in (LANES + 2 * n_state, hp_cols, hp_cols, LANES)
                for n in (n_dp, n_dp - 1)
            ],
            pltpu.VMEM((layers, groups, n_dp, 8, LANES), BF16),
            pltpu.VMEM((layers, n_dp * n_tp, 8, LANES), BF16),
            pltpu.VMEM((groups, 2 * n_rows, LANES), BF16),
            pltpu.VMEM((n_tp, 2 * n_rows, LANES), BF16),
            pltpu.VMEM((layers, 2, n_dp, rows, hp_cols), BF16),
            pltpu.VMEM((layers, n_dp, rows, d_here // 2), BF16),
            pltpu.VMEM((layers, n_z, n_dp, rows, d_here // 2), BF16),
            pltpu.VMEM((layers, 2, n_dp, rows, d_here // 2), BF16),
            pltpu.VMEM((layers, seqs, FRONT + slots, hp_cols), F32),
            pltpu.VMEM((layers, seqs, FRONT + slots, 2 * n_state), F32),
            pltpu.VMEM((2, n_rows, LANES), F32),
            pltpu.VMEM((n_rows, 2 * n_state), F32),
            pltpu.VMEM((layers, LANES + 2 * n_state, d_here), BF16),
            pltpu.VMEM((layers, LANES, d_here), BF16),
            pltpu.VMEM((max(layers - 1, 1), 2, d_here, hp_cols), BF16),
            pltpu.VMEM((layers, 8, hp_cols), F32),
            pltpu.VMEM((layers, 8, LANES), F32),
            pltpu.VMEM((layers, LANES, LANES), F32),
            pltpu.SemaphoreType.DMA,
            sems(4),
            pltpu.SemaphoreType.DMA,
            pltpu.SemaphoreType.DMA,
            sems(n_dp),
            sems(n_dp),
            sems(n_dp),
            pltpu.SemaphoreType.DMA,
            pltpu.SemaphoreType.DMA((2 * max(layers - 1, 1),)),
        ],
        compiler_params=pltpu.CompilerParams(
            collective_id=0, has_side_effects=True, vmem_limit_bytes=32 * 2**20
        ),
        name="mixer",
    )(*[pltpu.with_memory_space_constraint(a, pltpu.HBM) for a in operands])
    stream, conv_in, conv_maps, ssm = pl.pallas_call(
        finish,
        out_shape=results,
        in_specs=[vmem] * len(results),
        out_specs=(hbm,) * len(results),
        scratch_shapes=[pltpu.SemaphoreType.DMA((len(results),))],
        compiler_params=pltpu.CompilerParams(vmem_limit_bytes=2**20),
        name="finish",
    )(*made)
    return stream, jnp.transpose(conv_in, (0, 2, 1, 3)), conv_maps, ssm.reshape(recurrent_state.shape)


def solution(mesh):
    placed = (
        P(None, "dp"),
        P("dp"),
        P(None, "dp"),
        P(None, "dp", None, "tp"),
        P(None, "dp", None, "tp"),
        P(None, "dp", "tp"),
        P(None, None, "tp"),
        P(None, None, None, "tp"),
        P(None, "tp"),
        P(None, "tp"),
        P(None, "tp"),
        P(None, "tp"),
        P(None, "tp", "dp"),
        P(None, "dp", None, "tp"),
        P(None, "dp", None, None, "tp"),
        P(None, "dp", "tp", None, None),
        P(None, "dp", None, "tp"),
    )
    return jax.shard_map(
        functools.partial(body, mesh.shape["tp"], mesh.shape["dp"]),
        mesh=mesh,
        in_specs=placed,
        out_specs=(
            P(None, "dp"),
            P(None, "dp", None, "tp"),
            P(None, "dp", None, None, "tp"),
            P(None, "dp", "tp", None, None),
        ),
        check_vma=False,
    )
```

```python
import functools

import jax
import jax.numpy as jnp
from jax import lax
from jax.experimental import pallas as pl
from jax.experimental.pallas import tpu as pltpu
from jax.sharding import PartitionSpec as P

EPS = 1e-06
LANES = 128
FRONT = 8
F32, BF16 = jnp.float32, jnp.bfloat16


def up(n):
    return -(-n // LANES) * LANES


def dot(a, b, ca=1, cb=0):
    return lax.dot_general(a, b, (((ca,), (cb,)), ((), ())), preferred_element_type=F32)


def thirds(a):
    high = a.astype(BF16)
    rest = a - high.astype(F32)
    middle = rest.astype(BF16)
    return high, middle, (rest - middle.astype(F32)).astype(BF16)


def grid(n_rows, n_cols):
    return (
        lax.broadcasted_iota(jnp.int32, (n_rows, n_cols), 0),
        lax.broadcasted_iota(jnp.int32, (n_rows, n_cols), 1),
    )


def over(a, n):
    return lax.shift_right_logical(a, jnp.full_like(a, n.bit_length() - 1))


def ones_where(cond):
    return jnp.where(cond, 1.0, 0.0).astype(BF16)


def far_first(k, me, n):
    upper = me // (n // 2)
    mirrored = n - 1 - me
    return upper * (k + (k - me + n) // n) + (1 - upper) * (n - 1 - k - (k - mirrored + n) // n)


def general_kernel(
    n_tp, n_dp, d_model, heads, groups, slots, seqs, hp_cols, map_cols,
    lens, x, scale, w_pair, w_maps, w_step, tap_u, tap_m, bias, rate, skip, gain, cache_u, cache_m, extra_t,
    state_hbm, wout_hbm,
    stream, kept, ssm,
    a_send, a_recv, m_send, m_recv, h_send, h_recv, o_send, o_recv, n_send, n_recv, padded, step_w, state, wout, taps, par, extra,
    a_ss, a_rs, m_ss, m_rs, h_ss, h_rs, o_ss, o_rs, n_ss, n_rs, s_sem, w_sem,
):
    tp, dp = lax.axis_index("tp"), lax.axis_index("dp")
    layers = w_pair.shape[0]
    rows = seqs * slots
    taps_n = tap_u.shape[1]
    keep = taps_n - 1
    zc = up(hp_cols)
    ng = map_cols // groups
    n_state = state.shape[-1]
    cut = stream.shape[0] // n_tp
    per = rows // cut
    head_size = hp_cols // heads

    state_copy = pltpu.make_async_copy(state_hbm, state, s_sem)
    wout_copy = pltpu.make_async_copy(wout_hbm, wout, w_sem)
    state_copy.start()
    wout_copy.start()
    barrier = pltpu.get_barrier_semaphore()
    for k in range(1, n_dp):
        pl.semaphore_signal(barrier, inc=1, device_id={"dp": lax.rem(dp + k, n_dp)})
    for k in range(1, n_tp):
        pl.semaphore_signal(barrier, inc=1, device_id={"tp": lax.rem(tp + k, n_tp)})

    stream[...] = x[...].astype(F32)
    slot = lax.broadcasted_iota(jnp.int32, (slots, 1), 0)
    mask = jnp.concatenate([(slot < lens[s]).astype(F32) for s in range(seqs)], axis=0)
    lane = lax.broadcasted_iota(jnp.int32, (1, LANES), 1)
    r, c = grid(rows, rows)
    causal = (over(r, slots) == over(c, slots)) & (c <= r)
    tri = ones_where(causal)
    r, c = grid(2 * map_cols, up(2 * map_cols))
    which = over(r, ng) & 1
    sel = ones_where(c == which * map_cols + groups * (r & (ng - 1)) + over(r, 2 * ng))
    r, c = grid(n_tp * 2 * ng, 2 * n_state)
    sel2 = ones_where(c == (over(r, ng) & 1) * n_state + over(r, 2 * ng) * ng + (r & (ng - 1)))
    r, c = grid(LANES, hp_cols)
    ex = ones_where(r == over(c, head_size))
    r, c = grid(hp_cols, LANES)
    ext = ones_where(c == over(r, head_size))
    r, c = grid(hp_cols, hp_cols)
    ones = ones_where(over(r, head_size) == over(c, head_size))
    r, c = grid(LANES, 2 * LANES)
    spread = ones_where(c == 2 * r)
    padded[...] = jnp.zeros_like(padded)
    step_w[...] = jnp.zeros_like(step_w)
    taps[...] = jnp.zeros_like(taps)
    par[...] = jnp.zeros_like(par)
    extra[...] = jnp.zeros_like(extra)
    for l in range(layers):
        step_w[l, :heads, :] = w_step[l]
        taps[l, :taps_n, :hp_cols] = tap_u[l].astype(F32)
        for t in range(taps_n):
            pair = tap_m[l, t].astype(F32)
            for which in range(2):
                at = zc + which * map_cols
                taps[l, t : t + 1, at : at + map_cols] = pair[which : which + 1]
        par[l, 0:1, :heads] = bias[l : l + 1, :]
        par[l, 1:2, :heads] = rate[l : l + 1, :]
        par[l, 2:3, :heads] = skip[l : l + 1, :]
        for s in range(seqs):
            extra[l, :heads, s * slots : (s + 1) * slots] = extra_t[l, s]
    extra_rows = [extra[l].T[:rows] for l in range(layers)]
    skip_x = [sum(dot(piece, ex) for piece in thirds(par[l]))[2:3] for l in range(layers)]
    sends = []

    def copy(src, dst, ss, rs, where):
        return pltpu.make_async_remote_copy(
            src_ref=src, dst_ref=dst, send_sem=ss, recv_sem=rs, device_id=where
        )

    for l in range(layers):
        st = stream[...]
        squares = jnp.sum(st * st, axis=1, keepdims=True)
        normed = (st * scale[l : l + 1, :]).astype(BF16)
        even = jnp.concatenate(
            [dot(normed[:, i : i + LANES], spread) for i in range(0, normed.shape[1], LANES)], axis=1
        )
        odd = pltpu.roll(even, 1, 1)
        pair = dot(jnp.concatenate([even.astype(BF16), odd.astype(BF16)], axis=0), w_pair[l])
        tokens = st.shape[0]
        tail = dot(normed, step_w[l], 1, 1)
        high = squares.astype(BF16).astype(F32)
        tail = jnp.where(lane == LANES - 2, high, jnp.where(lane == LANES - 1, squares - high, tail))
        part = jnp.concatenate(
            [pair[:tokens], pair[tokens:], dot(normed, w_maps[l], 1, 1), tail], axis=1
        ).astype(BF16)
        for b in range(n_dp):
            a_send[l, b] = part[b * rows : (b + 1) * rows]
        if l == 0:
            pl.semaphore_wait(barrier, n_dp - 1 + n_tp - 1)
        flights = []
        for k in range(1, n_dp):
            to = lax.rem(dp + k, n_dp)
            c = copy(a_send.at[l, to], a_recv.at[l, k - 1], a_ss.at[l, k - 1], a_rs.at[l, k - 1], {"dp": to})
            c.start()
            flights.append(c)
        sends += flights
        acc = a_send[l, dp].astype(F32)
        for k, c in enumerate(flights):
            c.wait_recv()
            acc = acc + a_recv[l, k].astype(F32)
        tail = acc[:, acc.shape[1] - LANES :]
        squares = tail[:, LANES - 2 : LANES - 1] + tail[:, LANES - 1 : LANES]
        factor = lax.rsqrt(squares / d_model + EPS)
        proj = (acc * factor).astype(BF16).astype(F32)

        conv_w = taps.shape[2]
        pieces = []
        for s in range(seqs):
            for t in range(keep):
                at = FRONT - keep + t
                padded[s, at : at + 1, :hp_cols] = cache_u[l, t].astype(F32)[s : s + 1]
                pair = cache_m[l, s, t].astype(F32)
                for which in range(2):
                    col = zc + which * map_cols
                    padded[s, at : at + 1, col : col + map_cols] = pair[which : which + 1]
            padded[s, FRONT : FRONT + slots, :] = proj[s * slots : (s + 1) * slots, zc : zc + conv_w]
            total = padded[s, FRONT - keep : FRONT - keep + slots, :] * taps[l, 0:1, :]
            for t in range(1, taps_n):
                at = FRONT - keep + t
                total = total + padded[s, at : at + slots, :] * taps[l, t : t + 1, :]
            pieces.append(total)
        filtered = jnp.concatenate(pieces, axis=0)
        filtered = filtered * jax.nn.sigmoid(filtered)
        maps = filtered[:, conv_w - up(2 * map_cols) :].astype(BF16)
        sorted_maps = dot(sel, maps, 1, 1)
        for g in range(groups):
            m_send[l, g] = sorted_maps[g * 2 * ng : (g + 1) * 2 * ng, :].astype(BF16)

        def group_of(rank):
            return rank * heads // (heads * n_tp // groups)

        flights = []
        for k in range(n_tp - 1):
            to = far_first(k, tp, n_tp)
            c = copy(m_send.at[l, group_of(to)], m_recv.at[l, tp], m_ss.at[l, k], m_rs.at[l, tp], {"tp": to})
            c.start()
            sends.append(c)
        m_recv[l, tp] = m_send[l, group_of(tp)]

        for s in range(seqs):
            pick = lax.broadcasted_iota(jnp.int32, (8, FRONT + slots), 0)
            place = lax.broadcasted_iota(jnp.int32, (8, FRONT + slots), 1)
            chooser = ((place == pick + lens[s] + (FRONT - keep)) & (pick < keep)).astype(BF16)
            kept[l, s] = dot(chooser, padded[s].astype(BF16)).astype(BF16)
        raw = proj[:, proj.shape[1] - LANES :] + par[l, 0:1, :]
        step = (jnp.maximum(raw, 0.0) + jnp.log1p(jnp.exp(-jnp.abs(raw)))) * mask
        step = jnp.where(lane < heads, step, 0.0)
        logdec = extra_rows[l] * mask - step * jnp.exp(par[l, 1:2, :])
        logdec = jnp.where(lane < heads, logdec, 0.0)
        parts = dot(tri, jnp.concatenate(thirds(logdec), axis=1))
        sums = parts[:, :LANES] + parts[:, LANES : 2 * LANES] + parts[:, 2 * LANES :]
        sums_t = sums.T
        step_t = step.T
        sums_parts, step_parts = thirds(sums), thirds(step)
        both = dot(jnp.concatenate(sums_parts + step_parts, axis=0), ex)
        sums_x = both[:rows] + both[rows : 2 * rows] + both[2 * rows : 3 * rows]
        step_x = both[3 * rows : 4 * rows] + both[4 * rows : 5 * rows] + both[5 * rows :]
        inp = filtered[:, :hp_cols]
        gate = proj[:, :hp_cols]
        last_x = jnp.concatenate(
            [
                jnp.broadcast_to(sums_x[(s + 1) * slots - 1 : (s + 1) * slots, :], (slots, hp_cols))
                for s in range(seqs)
            ],
            axis=0,
        )
        weighted = (jnp.exp(last_x - sums_x) * step_x * inp).astype(BF16)
        inp_b = inp.astype(BF16)
        grow = jnp.exp(sums_x)
        direct = skip_x[l] * inp
        gate = gate * jax.nn.sigmoid(gate)
        rows_sum = sum(dot(ext, piece, 1, 1) for piece in sums_parts)
        segs = []
        for h in range(heads):
            gap = sums[:, h : h + 1] - sums_t[h : h + 1, :]
            segs.append(jnp.exp(jnp.where(causal, gap, -jnp.inf)) * step_t[h : h + 1, :])

        if l == 0:
            state_copy.wait()
            wout_copy.wait()
        for k in range(1, n_tp):
            src = lax.rem(tp + n_tp - k, n_tp)
            copy(m_send.at[l, 0], m_recv.at[l, src], m_ss.at[l, 0], m_rs.at[l, src], {"tp": src}).wait_recv()
        got = m_recv[l].astype(F32).reshape(n_tp * 2 * ng, rows)
        both_maps = dot(got.T.astype(BF16), sel2).astype(BF16)
        b_map, c_map = both_maps[:, :n_state], both_maps[:, n_state:]
        cross = dot(c_map, b_map, 1, 1)
        within = jnp.concatenate(
            [
                dot((cross * segs[h]).astype(BF16), inp_b[:, h * head_size : (h + 1) * head_size])
                for h in range(heads)
            ],
            axis=1,
        )
        carried = jnp.concatenate(
            [
                dot(c_map[s * slots : (s + 1) * slots], state[l, s].astype(BF16), 1, 1)
                for s in range(seqs)
            ],
            axis=0,
        )
        read = (within + carried * grow + direct) * gate
        power = read * read
        p_hi = power.astype(BF16)
        p_lo = (power - p_hi.astype(F32)).astype(BF16)
        mean = (dot(p_hi, ones) + dot(p_lo, ones)) / head_size
        headout = (read * lax.rsqrt(mean + EPS) * gain[l : l + 1, :] * mask).astype(BF16)
        h_send[l] = headout
        flights = []
        for k in range(1, n_dp):
            to = lax.rem(dp + k, n_dp)
            c = copy(h_send.at[l], h_recv.at[l, k - 1], h_ss.at[l, k - 1], h_rs.at[l, k - 1], {"dp": to})
            c.start()
            flights.append(c)
        sends += flights

        def push(value, block):
            out = dot(value, wout[l]).astype(BF16)
            for i in range(per):
                to = block * per + i
                o_send[l, to] = out[i * cut : (i + 1) * cut]

                @pl.when(to != tp)
                def _():
                    copy(o_send.at[l, to], o_recv.at[l, tp], o_ss.at[l, to], o_rs.at[l, tp], {"tp": to}).start()

        push(headout, dp)
        for s in range(seqs):
            at = slice(s * slots, (s + 1) * slots)
            fresh = dot(weighted[at], b_map[at], 0, 0)
            end = (s + 1) * slots - 1
            ssm[l, s] = jnp.exp(rows_sum[:, end : end + 1]) * state[l, s] + fresh
        for k, c in enumerate(flights):
            c.wait_recv()
            push(h_recv[l, k], lax.rem(dp + n_dp - k - 1, n_dp))
        total = o_send[l, tp].astype(F32)
        for k in range(1, n_tp):
            src = lax.rem(tp + n_tp - k, n_tp)
            copy(o_send.at[l, src], o_recv.at[l, src], o_ss.at[l, src], o_rs.at[l, src], {"tp": src}).wait_recv()
            total = total + o_recv[l, src].astype(F32)
        fresh = total.astype(BF16)
        n_send[l] = fresh
        n_recv[l, tp] = fresh
        for k in range(n_tp - 1):
            to = far_first(k, tp, n_tp)
            c = copy(n_send.at[l], n_recv.at[l, tp], n_ss.at[l, k], n_rs.at[l, tp], {"tp": to})
            c.start()
            sends.append(c)
        for k in range(1, n_tp):
            src = lax.rem(tp + n_tp - k, n_tp)
            copy(n_send.at[l], n_recv.at[l, src], n_ss.at[l, 0], n_rs.at[l, src], {"tp": src}).wait_recv()
        stream[...] += n_recv[l].astype(F32).reshape(stream.shape)

    for c in sends:
        c.wait_send()
    for l in range(layers):
        for k in range(1, n_tp):
            to = lax.rem(tp + k, n_tp)
            copy(o_send.at[l, to], o_recv.at[l, tp], o_ss.at[l, to], o_rs.at[l, tp], {"tp": to}).wait_send()


def general_body(
    n_tp, n_dp,
    tokens, lengths, input_norm_scale, gate_input_weight, maps_weight, step_weight,
    input_tap_weight, map_tap_weight, step_size_bias, decay_rate_logarithm, direct_path_weight,
    head_norm_scale, output_weight, convolution_input_cache, convolution_map_cache,
    recurrent_state, extra_log_decay,
):
    layers, seqs, slots, heads = extra_log_decay.shape
    head_size, n_state = recurrent_state.shape[3:]
    hp_cols = heads * head_size
    map_cols = maps_weight.shape[3]
    groups = map_cols * n_tp // n_state
    ng = map_cols // groups
    rows = seqs * slots
    d_here = tokens.shape[1]
    keep = convolution_input_cache.shape[2]

    def wide(a):
        pad = up(a.shape[-1]) - a.shape[-1]
        return a if pad == 0 else jnp.pad(a, [(0, 0)] * (a.ndim - 1) + [(0, pad)])

    w_pair = wide(gate_input_weight.reshape(layers, 2 * d_here, hp_cols))
    w_maps = jnp.transpose(maps_weight, (0, 2, 3, 1)).reshape(layers, 2 * map_cols, d_here)
    if up(2 * map_cols) > 2 * map_cols:
        w_maps = jnp.pad(w_maps, ((0, 0), (0, up(2 * map_cols) - 2 * map_cols), (0, 0)))
    w_step = jnp.transpose(step_weight, (0, 2, 1))
    cache_u = jnp.transpose(convolution_input_cache, (0, 2, 1, 3))
    extra_t = jnp.transpose(extra_log_decay, (0, 1, 3, 2))
    state = recurrent_state.reshape(layers, seqs, hp_cols, n_state)

    vmem = pl.BlockSpec(memory_space=pltpu.VMEM)
    wide_cols = 2 * up(hp_cols) + up(2 * map_cols) + LANES
    anywhere = pl.BlockSpec(memory_space=pl.ANY)
    conv_w = up(hp_cols) + up(2 * map_cols)
    cut = tokens.shape[0] // n_tp
    sems = lambda n: pltpu.SemaphoreType.DMA((layers, n))
    args = [tokens, input_norm_scale, w_pair, w_maps, w_step, input_tap_weight,
        map_tap_weight, step_size_bias, decay_rate_logarithm, direct_path_weight, head_norm_scale,
        cache_u, convolution_map_cache, extra_t]
    stream, kept, ssm = pl.pallas_call(
        functools.partial(
            general_kernel, n_tp, n_dp, d_here * n_dp, heads, groups, slots, seqs, hp_cols, map_cols
        ),
        out_shape=(
            jax.ShapeDtypeStruct(tokens.shape, F32),
            jax.ShapeDtypeStruct((layers, seqs, 8, conv_w), BF16),
            jax.ShapeDtypeStruct(state.shape, F32),
        ),
        in_specs=[pl.BlockSpec(memory_space=pltpu.SMEM)] + [vmem] * len(args) + [anywhere] * 2,
        out_specs=(vmem, vmem, vmem),
        scratch_shapes=[
            pltpu.VMEM((layers, n_dp, rows, wide_cols), BF16),
            pltpu.VMEM((layers, n_dp - 1, rows, wide_cols), BF16),
            pltpu.VMEM((layers, groups, 2 * ng, rows), BF16),
            pltpu.VMEM((layers, n_tp, 2 * ng, rows), BF16),
            pltpu.VMEM((layers, rows, hp_cols), BF16),
            pltpu.VMEM((layers, n_dp - 1, rows, hp_cols), BF16),
            pltpu.VMEM((layers, n_tp, cut, d_here), BF16),
            pltpu.VMEM((layers, n_tp, cut, d_here), BF16),
            pltpu.VMEM((layers, cut, d_here), BF16),
            pltpu.VMEM((layers, n_tp, cut, d_here), BF16),
            pltpu.VMEM((seqs, FRONT + slots, conv_w), F32),
            pltpu.VMEM((layers, LANES, d_here), BF16),
            pltpu.VMEM(state.shape, F32),
            pltpu.VMEM(output_weight.shape, BF16),
            pltpu.VMEM((layers, 8, conv_w), F32),
            pltpu.VMEM((layers, 8, LANES), F32),
            pltpu.VMEM((layers, LANES, LANES), F32),
            sems(n_dp - 1), sems(n_dp - 1), sems(n_tp - 1), sems(n_tp), sems(n_dp - 1),
            sems(n_dp - 1), sems(n_tp), sems(n_tp), sems(n_tp - 1), sems(n_tp),
            pltpu.SemaphoreType.DMA, pltpu.SemaphoreType.DMA,
        ],
        compiler_params=pltpu.CompilerParams(
            collective_id=0, has_side_effects=True, vmem_limit_bytes=48 * 2**20
        ),
        name="mixer",
    )(lengths, *args, state, output_weight)
    conv_in = kept[:, :, :keep, :hp_cols]
    start = conv_w - up(2 * map_cols)
    conv_maps = kept[:, :, :keep, start : start + 2 * map_cols].reshape(
        layers, seqs, keep, 2, map_cols
    )
    return stream, conv_in, conv_maps, ssm.reshape(recurrent_state.shape)


def peers(n, order):
    return [k for k in order if 0 < k < n] + [k for k in range(1, n) if k not in order]


def kernel(
    n_tp, n_dp, d_model, groups, shapes,
    *refs,
):
    names = (
        "lens", "x", "scale", "gate", "w_maps", "w_step", "tap_u", "tap_m", "bias", "rate", "skip", "gain",
        "cache_u", "cache_m", "extra_t", "state", "wout",
    )
    hbm = dict(zip(names, refs[: len(names)]))
    (
        stream, kept_u, kept_m, ssm,
        lens, x, scale, w_gate, w_maps, w_step, tap_u, tap_m, bias, rate, skip, gain, cache_u, cache_m, extra_t, state,
        wout, g_sem,
        t_send, t_recv, u_send, u_recv, z_send, z_recv, q_send, q_recv, m_send, m_recv, c_send, c_recv, h_recv, o_send, o_recv, nb,
        padded, padded_m, mrow, mrows, w_rows, w_sorted, w_flat, w_turned, taps, par, extra,
        out_sem, a_rs, m_rs, c_rs, h_rs, o_rs, n_rs, w_rs, f_rs,
    ) = refs[len(names) :]
    layers, seqs, slots, heads, head_size, n_state, hp_cols, map_cols = shapes
    tp, dp = lax.axis_index("tp"), lax.axis_index("dp")
    rows = seqs * slots
    taps_n = tap_u.shape[1]
    keep = taps_n - 1
    ng = map_cols // groups
    pair_cols = 2 * ng
    quads = LANES // pair_cols
    d_here = x.shape[1]
    half = d_here // 2
    tokens = x.shape[0]
    side = lax.rem(tp, 2)
    zed = lax.div(tp, 2)
    n_z = n_tp // 2
    every = n_tp * n_dp
    me = dp * n_tp + tp
    dp_peers = peers(n_dp, (3, 1, 2))
    turns = peers(n_dp, (1, 2, 3))
    z_peers = peers(n_z, (3, 2, 1))

    def remote(src, dst, arrived, where):
        return pltpu.make_async_remote_copy(
            src_ref=src, dst_ref=dst, send_sem=out_sem, recv_sem=arrived, device_id=where
        )

    def landed(block, arrived):
        remote(block, block, arrived, {"tp": jnp.bitwise_xor(tp, 1)}).wait_recv()

    barrier = pltpu.get_barrier_semaphore()
    others = [
        (i, j) for i in [*peers(n_tp, (6, 7, 4, 5, 2, 3, 1)), 0] for j in [*dp_peers, 0] if i or j
    ]

    def at(i, j):
        return {"tp": jnp.bitwise_xor(tp, i), "dp": jnp.bitwise_xor(dp, j)}

    for i, j in others:
        pl.semaphore_signal(barrier, inc=1, device_id=at(i, j))

    spare = [
        *[o_rs.at[layers - 1, k] for k in range(n_dp)], *[h_rs.at[layers - 1, k] for k in range(n_dp)],
        *[n_rs.at[layers - 1, k] for k in range(n_dp)], *[a_rs.at[layers - 1, p] for p in range(4)],
        f_rs.at[0], w_rs,
    ]
    local = {}
    pairs = dict(
        x=x, scale=scale, w_maps=w_maps, w_step=w_step, lens=lens, tap_u=tap_u, tap_m=tap_m, bias=bias, rate=rate,
        skip=skip, gain=gain, cache_u=cache_u, cache_m=cache_m, extra_t=extra_t, state=state,
    )
    for n, name in enumerate(pairs):
        local[name] = pltpu.make_async_copy(hbm[name], pairs[name], spare[n])
    mine = pl.ds(pl.multiple_of(side * half, LANES), half)
    theirs = pl.ds(pl.multiple_of((1 - side) * half, LANES), half)
    local["wout"] = pltpu.make_async_copy(hbm["wout"].at[:, :, mine], wout.at[:, 0], spare[len(pairs)])
    gate_copies = [
        [
            pltpu.make_async_copy(
                hbm["gate"].at[l, :, :, i : i + LANES], w_gate.at[l, i // LANES], g_sem.at[l]
            )
            for i in range(0, hp_cols, LANES)
        ]
        for l in range(layers)
    ]
    first = ("x", "scale", "w_maps", "w_step")
    for name in first:
        local[name].start()
    for c in gate_copies[0]:
        c.start()
    for name in local:
        if name not in first:
            local[name].start()
    for l in range(1, layers):
        for c in gate_copies[l]:
            c.start()

    lane = lax.broadcasted_iota(jnp.int32, (1, LANES), 1)
    r, c = grid(LANES, 4 * LANES)
    spread = ones_where(c == jnp.where(c < 2 * LANES, 2 * r, 2 * LANES + 2 * r + 1))
    r, c = grid(LANES, LANES)
    place = (c + LANES - ng * tp) & (LANES - 1)
    wanted = (over(place, ng) & 1) * map_cols + groups * (place & (ng - 1)) + over(place, pair_cols)
    sorter = ones_where(r == wanted)
    home = over((lane + LANES - ng * tp) & (LANES - 1), pair_cols)
    for l in range(layers):
        w_rows[l, :LANES] = jnp.zeros_like(w_rows[l, :LANES])
    gate_rows = w_gate.reshape(layers, hp_cols // LANES, 2 * d_here, LANES)

    def group_of(rank):
        return rank * groups // n_tp

    def with_squares(tail, squares):
        high = squares.astype(BF16).astype(F32)
        return jnp.where(lane == LANES - 2, high, jnp.where(lane == LANES - 1, squares - high, tail))

    def fill(buffer, l, value):
        for b in range(n_dp):
            buffer[l, b, :, : value.shape[1]] = value[b * rows : (b + 1) * rows].astype(BF16)

    def pack_maps(l, raw):
        turned = [raw if k == 0 else pltpu.roll(raw, k * pair_cols, 1) for k in range(quads)]
        turned = [t.reshape(n_dp, quads, 8, LANES) for t in turned]
        for g in range(groups):
            piece = turned[(0 - g) % quads][:, 0]
            for q in range(1, quads):
                piece = jnp.where((home == q)[None], turned[(q - g) % quads][:, q], piece)
            m_send[l, g] = piece.astype(BF16)

    def send_maps(l):
        for i, j in others:
            to = at(i, j)
            remote(
                m_send.at[l, group_of(to["tp"]), to["dp"]], m_recv.at[l, me], m_rs, to
            ).start()
        m_recv[l, me] = m_send[l, group_of(tp), dp]

    def rows_of(rank, which):
        return pl.ds(pl.multiple_of(LANES + which * n_state + ng * rank, ng), ng)

    def pick_rows(rank, which):
        return pl.ds(pl.multiple_of(pair_cols * group_of(rank) + which * ng, ng), ng)

    def fetch(i, k, which):
        to = jnp.bitwise_xor(tp, k)
        n = 2 * (i - 1) + (k == 1)
        return remote(
            w_sorted.at[i, pick_rows(to, which)], w_rows.at[i, rows_of(tp, which)], f_rs.at[n], {"tp": to}
        )

    def relay(i, j, which):
        n = 2 * (i - 1) + 1
        block = w_rows.at[i, rows_of(jnp.bitwise_xor(tp, 2 * j), which)]
        return remote(block, block, f_rs.at[n], at(1, 0))

    def fetched(i, far):
        n = 2 * (i - 1) + 1 - far
        landed(w_rows.at[i, pl.ds(LANES, 2 * ng * (n_z - 1 if far else n_z))], f_rs.at[n])

    parts_of = ((t_send, t_recv), (u_send, u_recv), (z_send, z_recv), (q_send, q_recv))

    def part(l, p, k):
        send, recv = parts_of[p]
        to = jnp.bitwise_xor(dp, k)
        src, dst = send.at[l, to], recv.at[l, k - 1]
        if p == 0 and l == 0:
            src, dst = src.at[:, :LANES], dst.at[:, :LANES]
        return remote(src, dst, a_rs.at[l, p], {"dp": to})

    def send_part(l, p):
        for k in dp_peers:
            part(l, p, k).start()

    def await_part(l, p):
        send, recv = parts_of[p]
        width = LANES if p == 0 and l == 0 else send.shape[-1]
        landed(recv.at[l, :, :, :width], a_rs.at[l, p])
        acc = send[l, dp, :, :width].astype(F32)
        for k in range(1, n_dp):
            acc = acc + recv[l, k - 1, :, :width].astype(F32)
        return acc

    def flat_weight(l):
        return jnp.concatenate([gate_rows[l, i] for i in range(hp_cols // LANES)], axis=1)

    sends = []
    for name in first:
        local[name].wait()
    for l in range(layers):
        w_rows[l, :heads, :] = w_step[l]
    w_sorted[0] = dot(sorter, w_maps[0], 0, 0).astype(BF16)
    stream[...] = x[...].astype(F32)

    for l in range(layers):
        if l == 0:
            st = stream[...]
            squares = jnp.sum(st * st, axis=1, keepdims=True)
            normed = (st * scale[l : l + 1, :]).astype(BF16)
            raw = dot(normed, w_sorted[l], 1, 1)
            pack_maps(l, raw)
            fill(t_send, l, with_squares(dot(normed, w_rows[l, :LANES], 1, 1), squares))
            spreads = [dot(normed[:, i : i + LANES], spread).astype(BF16) for i in range(0, d_here, LANES)]
            even = jnp.concatenate([s[:, : 2 * LANES] for s in spreads], axis=1)
            odd = jnp.concatenate([s[:, 2 * LANES :] for s in spreads], axis=1)
            pltpu.make_async_copy(w_gate.at[l], w_gate.at[l], g_sem.at[l]).wait()
            both = dot(jnp.concatenate([odd, even], axis=0), flat_weight(l))
            fill(u_send, l, both[:tokens])
            fill(z_send, l, both[tokens:])
            fill(q_send, l, raw)
            pl.semaphore_wait(barrier, every - 1)
            send_maps(l)
            for p in range(4):
                send_part(l, p)

        if l == 0:
            for n in range(len(pairs) + 1):
                name = [*pairs, "wout"][n]
                if name not in first:
                    local[name].wait()
            swap = remote(hbm["wout"].at[:, :, theirs], wout.at[:, 1], w_rs, {"tp": jnp.bitwise_xor(tp, 1)})
            swap.start()
            per_layer = seqs * keep + taps_n
            mrow[...] = jnp.zeros_like(mrow)
            for i in range(layers):
                for s in range(seqs):
                    for t in range(keep):
                        pair = cache_m[i, s, t].astype(F32)
                        n = i * per_layer + s * keep + t
                        for which in range(2):
                            mrow[which, n : n + 1, :map_cols] = pair[which : which + 1]
                for t in range(taps_n):
                    pair = tap_m[i, t].astype(F32)
                    n = i * per_layer + seqs * keep + t
                    for which in range(2):
                        mrow[which, n : n + 1, :map_cols] = pair[which : which + 1]
            n_rows = mrow.shape[1]
            r, c = grid(LANES, groups * LANES)
            n = (c & (LANES - 1)) - ng * tp
            chosen = (n >= 0) & (n < ng) & (r == groups * n + over(c, LANES))
            packed = dot(mrow[...].reshape(2 * n_rows, LANES).astype(BF16), ones_where(chosen)).astype(BF16)
            for g in range(groups):
                c_send[g] = packed[:, g * LANES : (g + 1) * LANES]
            for k in peers(n_tp, (6, 7, 4, 5, 2, 3, 1)):
                to = jnp.bitwise_xor(tp, k)
                c = remote(c_send.at[group_of(to)], c_recv.at[k], c_rs, {"tp": to})
                c.start()
                sends.append(c)
            c_recv[0] = c_send[group_of(tp)]
            r, c = grid(LANES, LANES)
            resort = ones_where(r == (over(c, ng) & 1) * map_cols + groups * (c & (ng - 1)) + over(c, pair_cols))
            for i in range(1, layers):
                w_sorted[i] = dot(resort, w_maps[i], 0, 0).astype(BF16)

            slot = lax.broadcasted_iota(jnp.int32, (slots, 1), 0)
            mask = jnp.concatenate([(slot < lens[s]).astype(F32) for s in range(seqs)], axis=0)
            r, c = grid(rows, rows)
            causal = (over(r, slots) == over(c, slots)) & (c <= r)
            within_sequence = lax.broadcasted_iota(jnp.int32, (rows, LANES), 0) & (slots - 1)
            r, c = grid(LANES, hp_cols)
            ex = ones_where(r == over(c, head_size))
            r, c = grid(hp_cols, LANES)
            ext = ones_where(c == over(r, head_size))
            r, c = grid(hp_cols, hp_cols)
            ones = ones_where(over(r, head_size) == over(c, head_size))
            padded[...] = jnp.zeros_like(padded)
            padded_m[...] = jnp.zeros_like(padded_m)
            taps[...] = jnp.zeros_like(taps)
            par[...] = jnp.zeros_like(par)
            extra[...] = jnp.zeros_like(extra)
            for i in range(layers):
                taps[i, :taps_n, :] = tap_u[i].astype(F32)
                par[i, 0:1, :heads] = bias[i : i + 1, :]
                par[i, 1:2, :heads] = rate[i : i + 1, :]
                par[i, 2:3, :heads] = skip[i : i + 1, :]
                for s in range(seqs):
                    extra[i, :heads, s * slots : (s + 1) * slots] = extra_t[i, s]
                    for t in range(keep):
                        n = FRONT - keep + t
                        padded[i, s, n : n + 1, :] = cache_u[i, t].astype(F32)[s : s + 1]
            extra_rows = [extra[i].T[:rows] for i in range(layers)]
            skip_x = [sum(dot(piece, ex) for piece in thirds(par[i]))[2:3] for i in range(layers)]

        def convolve(pad, weights):
            pieces = []
            for s in range(seqs):
                total = pad[l, s, FRONT - keep : FRONT - keep + slots, :] * weights[0:1]
                for t in range(1, taps_n):
                    n = FRONT - keep + t
                    total = total + pad[l, s, n : n + slots, :] * weights[t : t + 1]
                pieces.append(total)
            out = jnp.concatenate(pieces, axis=0)
            return out * jax.nn.sigmoid(out)

        acc = await_part(l, 0)
        tail = acc[:, :LANES]
        squares = tail[:, LANES - 2 : LANES - 1] + tail[:, LANES - 1 : LANES]
        factor = lax.rsqrt(squares / d_model + EPS)
        raw_step = (tail * factor).astype(BF16).astype(F32) + par[l, 0:1, :]
        step = (jnp.maximum(raw_step, 0.0) + jnp.log1p(jnp.exp(-jnp.abs(raw_step)))) * mask
        step = jnp.where(lane < heads, step, 0.0)
        logdec = extra_rows[l] * mask - step * jnp.exp(par[l, 1:2, :])
        logdec = jnp.where(lane < heads, logdec, 0.0)
        sums = logdec
        for n in [2**i for i in range(slots.bit_length()) if 2**i < slots]:
            sums = sums + jnp.where(within_sequence >= n, pltpu.roll(sums, n, 0), 0.0)
        sums_t = sums.T
        step_t = step.T
        sums_parts, step_parts = thirds(sums), thirds(step)
        both = dot(jnp.concatenate(sums_parts + step_parts, axis=0), ex)
        sums_x = both[:rows] + both[rows : 2 * rows] + both[2 * rows : 3 * rows]
        step_x = both[3 * rows : 4 * rows] + both[4 * rows : 5 * rows] + both[5 * rows :]
        grow = jnp.exp(sums_x)
        segs = []
        for h in range(heads):
            gap = sums[:, h : h + 1] - sums_t[h : h + 1, :]
            segs.append(jnp.exp(jnp.where(causal, gap, -jnp.inf)) * step_t[h : h + 1, :])

        def filter_inputs(acc):
            proj = (acc * factor).astype(BF16).astype(F32)
            for s in range(seqs):
                padded[l, s, FRONT : FRONT + slots, :] = proj[s * slots : (s + 1) * slots]
            return convolve(padded, taps[l])

        def unpack_maps():
            landed(m_recv.at[l, 0 : every - 1], m_rs)
            got = m_recv[l].astype(F32).reshape(n_dp, n_tp, 8, LANES)
            got = sum(got[b] for b in range(n_dp))
            cell = over(lane, ng)
            columns = []
            for which in range(2):
                blocks = []
                for q in range(quads):
                    n = 2 * q + which
                    piece = got[0]
                    for t in range(1, n_tp):
                        piece = jnp.where(cell == (n + t) % n_tp, got[t], piece)
                    blocks.append(piece if n == 0 else pltpu.roll(piece, LANES - ng * n, 1))
                columns.append(jnp.concatenate(blocks, axis=0))
            return jnp.concatenate(columns, axis=1)

        def filter_maps(raw):
            proj = (raw * factor).astype(BF16).astype(F32)
            for s in range(seqs):
                padded_m[l, s, FRONT : FRONT + slots, :] = proj[s * slots : (s + 1) * slots]
            n = l * per_layer + seqs * keep
            maps = convolve(padded_m, mrows[n : n + taps_n, :]).astype(BF16)
            b_map, c_map = maps[:, :n_state], maps[:, n_state:]
            carried = jnp.concatenate(
                [
                    dot(c_map[s * slots : (s + 1) * slots], state[l, s].astype(BF16), 1, 1)
                    for s in range(seqs)
                ],
                axis=0,
            )
            return b_map, dot(c_map, b_map, 1, 1), carried * grow

        def gate_of(acc):
            gate = (acc * factor).astype(BF16).astype(F32)
            return gate * jax.nn.sigmoid(gate)

        if l == 0:
            inp = filter_inputs(await_part(l, 1))
            gate = gate_of(await_part(l, 2))
            landed(c_recv.at[1:n_tp], c_rs)
            total = c_recv[0].astype(F32)
            for k in range(1, n_tp):
                total = total + c_recv[k].astype(F32)
            mrows[...] = jnp.concatenate([total[:n_rows], total[n_rows:]], axis=1)
            for i in range(layers):
                for s in range(seqs):
                    n = i * per_layer + s * keep
                    padded_m[i, s, FRONT - keep : FRONT, :] = mrows[n : n + keep, :]
            maps_in = unpack_maps()
            for i in range(1, layers):
                for k in [*[2 * j for j in z_peers], 1]:
                    for which in range(2):
                        fetch(i, k, which).start()
                for which in range(2):
                    w_rows[i, rows_of(tp, which), :] = w_sorted[i, pick_rows(tp, which), :]
            b_map, cross, carried = filter_maps(maps_in)
        else:
            b_map, cross, carried = filter_maps(acc[:, LANES:])
            inp = filter_inputs(await_part(l, 1))
        inp_b = inp.astype(BF16)
        within = jnp.concatenate(
            [
                dot((cross * segs[h]).astype(BF16), inp_b[:, h * head_size : (h + 1) * head_size])
                for h in range(heads)
            ],
            axis=1,
        )
        inner = within + carried + skip_x[l] * inp
        if l > 0:
            gate = gate_of(await_part(l, 2))
        read = inner * gate
        power = read * read
        p_hi = power.astype(BF16)
        p_lo = (power - p_hi.astype(F32)).astype(BF16)
        mean = (dot(p_hi, ones) + dot(p_lo, ones)) / head_size
        headout = (read * lax.rsqrt(mean + EPS) * gain[l : l + 1, :] * mask).astype(BF16)
        h_recv[l, 0, 0] = headout
        own = h_recv.at[l, 0, 0]
        targets = [(1, 0)] + [(i, k) for k in turns for i in (0, 1)]
        for i, k in targets:
            remote(own, h_recv.at[l, i, k], h_rs.at[l, k], at(i, k)).start()

        def push(k):
            value = jnp.concatenate([h_recv[l, 0, k], h_recv[l, 1, k]], axis=1)
            block = jnp.bitwise_xor(dp, k)
            o_send[l, k] = dot(value, wout[l].reshape(2 * hp_cols, half)).astype(BF16)
            for j in z_peers:
                remote(
                    o_send.at[l, k], o_recv.at[l, j, k], o_rs.at[l, k],
                    {"tp": jnp.bitwise_xor(tp, 2 * j)},
                ).start()

        if l == 0:
            swap.wait_recv()
        landed(h_recv.at[l, 1, 0], h_rs.at[l, 0])
        push(0)
        last_x = jnp.concatenate(
            [
                jnp.broadcast_to(sums_x[(s + 1) * slots - 1 : (s + 1) * slots, :], (slots, hp_cols))
                for s in range(seqs)
            ],
            axis=0,
        )
        weighted = (jnp.exp(last_x - sums_x) * step_x * inp).astype(BF16)
        rows_sum = sum(dot(ext, piece, 1, 1) for piece in sums_parts)
        for s in range(seqs):
            span = slice(s * slots, (s + 1) * slots)
            fresh = dot(weighted[span], b_map[span], 0, 0)
            end = (s + 1) * slots - 1
            ssm[l, s] = jnp.exp(rows_sum[:, end : end + 1]) * state[l, s] + fresh
        if l + 1 < layers:
            pltpu.make_async_copy(w_gate.at[l + 1], w_gate.at[l + 1], g_sem.at[l + 1]).wait()
            weight = flat_weight(l + 1)
            r, c = grid(LANES, 2 * LANES)
            for which in range(2):
                picker = ones_where(c == 2 * r + which)
                for n in range(0, d_here, LANES):
                    w_flat[l, which, n : n + LANES] = dot(picker, weight[2 * n : 2 * (n + LANES)]).astype(BF16)
        for k in turns:
            landed(h_recv.at[l, :, k], h_rs.at[l, k])
            push(k)

        r, c = grid(LANES, LANES)
        if l == 0:
            r = (r + LANES - ng * tp) & (LANES - 1)
        unsort = ones_where(
            c == (over(r, ng) & 1) * map_cols + groups * (r & (ng - 1)) + over(r, pair_cols)
        )
        own_maps = dot((await_part(l, 3) * factor).astype(BF16), unsort)
        for s in range(seqs):
            pick = lax.broadcasted_iota(jnp.int32, (8, FRONT + slots), 0)
            spot = lax.broadcasted_iota(jnp.int32, (8, FRONT + slots), 1)
            chooser = ((spot == pick + lens[s] + (FRONT - keep)) & (pick < keep)).astype(BF16)
            kept = dot(chooser, padded[l, s].astype(BF16)).astype(BF16)
            r, c = grid(8, slots)
            later_pick = ones_where((c == r + lens[s] - keep) & (r < keep))
            maps_kept = dot(later_pick, own_maps[s * slots : (s + 1) * slots].astype(BF16))
            for t in range(keep):
                kept_u[l, t, s : s + 1, :] = kept[t : t + 1]
                old = jnp.zeros((1, LANES), F32)
                for n in range(keep):
                    flat = jnp.concatenate(
                        [cache_m[l, s, n].astype(F32)[which : which + 1] for which in range(2)], axis=1
                    )
                    old = jnp.where(t + lens[s] == n, flat, old)
                line = (maps_kept[t : t + 1] + old).astype(BF16)
                for which in range(2):
                    kept_m[l, s, t, which : which + 1, :] = line[:, which * map_cols : (which + 1) * map_cols]

        def gather(k):
            landed(o_recv.at[l, 1:n_z, k], o_rs.at[l, k])
            o_recv[l, 0, k] = o_send[l, k]
            block = jnp.bitwise_xor(dp, k)
            total = o_recv[l, zed, k].astype(F32)
            for z in range(1, n_z):
                total = total + o_recv[l, jnp.bitwise_xor(zed, z), k].astype(F32)
            nb[l, side, block] = total.astype(BF16)
            remote(
                nb.at[l, side, block], nb.at[l, side, block], n_rs.at[l, k], at(1, 0)
            ).start()

        if l == 0:
            for i in range(1, layers):
                fetched(i, 1)
                for j in z_peers:
                    for which in range(2):
                        relay(i, j, which).start()
        def receive(k):
            landed(nb.at[l, 1 - side, jnp.bitwise_xor(dp, k)], n_rs.at[l, k])
            block = jnp.bitwise_xor(dp, k)
            span = pl.ds(pl.multiple_of(block * rows, rows), rows)
            st = stream[span, :] + jnp.concatenate([nb[l, h, block].astype(F32) for h in range(2)], axis=1)
            stream[span, :] = st
            n = l + 1
            if n == layers:
                return
            squares = jnp.sum(st * st, axis=1, keepdims=True)
            normed = (st * scale[n : n + 1, :]).astype(BF16)
            tail = dot(normed, w_turned[l, :, : w_rows.shape[1]])
            tail = jnp.concatenate([with_squares(tail[:, :LANES], squares), tail[:, LANES:]], axis=1)
            t_send[n, block] = tail.astype(BF16)
            if k:
                part(n, 0, k).start()
            u_send[n, block] = dot(normed, w_flat[l, 1]).astype(BF16)
            if k:
                part(n, 1, k).start()
            z_send[n, block] = dot(normed, w_flat[l, 0]).astype(BF16)
            if k:
                part(n, 2, k).start()
            q_send[n, block] = dot(normed, w_turned[l, :, w_rows.shape[1] :]).astype(BF16)
            if k:
                part(n, 3, k).start()

        order = [0, *turns]
        gather(order[0])
        if l + 1 < layers:
            fetched(l + 1, 0)
            w_turned[l, :, : w_rows.shape[1]] = w_rows[l + 1].T
            w_turned[l, :, w_rows.shape[1] :] = w_sorted[l + 1].T
        receive(order[0])
        gather(order[1])
        for n in range(2, len(order)):
            gather(order[n])
            receive(order[n - 1])
        receive(order[-1])

    for c in sends:
        c.wait_send()
    swap.wait_send()
    for l in range(layers):
        if l == 0:
            for i, j in others:
                remote(m_send.at[l, 0, 0], m_recv.at[l, 0], m_rs, at(i, j)).wait_send()
        else:
            for which in range(2):
                for k in [*[2 * j for j in z_peers], 1]:
                    fetch(l, k, which).wait_send()
                for j in z_peers:
                    relay(l, j, which).wait_send()
        for k in dp_peers:
            for p in range(4):
                part(l, p, k).wait_send()
        for i, k in [(1, 0)] + [(i, k) for k in turns for i in (0, 1)]:
            remote(
                h_recv.at[l, 0, 0], h_recv.at[l, i, k], h_rs.at[l, k], at(i, k)
            ).wait_send()
        for k in range(n_dp):
            for j in z_peers:
                remote(
                    o_send.at[l, k], o_recv.at[l, j, k], o_rs.at[l, k], at(2 * j, 0)
                ).wait_send()
            remote(nb.at[l, 0, 0], nb.at[l, 0, 0], n_rs.at[l, k], at(1, 0)).wait_send()


def finish(stream, kept_u, kept_m, ssm, stream_out, kept_u_out, kept_m_out, ssm_out, sems):
    pairs = ((ssm, ssm_out), (stream, stream_out), (kept_u, kept_u_out), (kept_m, kept_m_out))
    step = stream.shape[0] // 4
    for i, j in [(i, j) for i in range(ssm.shape[0]) for j in range(ssm.shape[1])]:
        pltpu.make_async_copy(ssm.at[i, j], ssm_out.at[i, j], sems.at[0]).start()
    for i in range(0, stream.shape[0], step):
        pltpu.make_async_copy(stream.at[i : i + step], stream_out.at[i : i + step], sems.at[1]).start()
    for i in (2, 3):
        pltpu.make_async_copy(*pairs[i], sems.at[i]).start()
    for i, pair in enumerate(pairs):
        pltpu.make_async_copy(*pair, sems.at[i]).wait()


def fits(layers, n_tp, n_dp, heads, hp_cols, map_cols, n_state, rows, d_here, keep):
    groups = map_cols * n_tp // n_state
    powers = all(n & (n - 1) == 0 for n in (n_tp, n_dp, groups, map_cols // groups))
    return (
        powers and layers > 1 and n_tp > 2 and n_dp > 2 and n_tp * n_dp <= 64 and n_tp % groups == 0 and map_cols % groups == 0
        and hp_cols % LANES == 0 and 2 * map_cols == LANES and n_state == LANES
        and rows * 2 * (map_cols // groups) == 8 * LANES and d_here % (2 * LANES) == 0
        and keep <= FRONT and heads <= LANES - 2
    )


def body(n_tp, n_dp, *args):
    (
        tokens, lengths, input_norm_scale, gate_input_weight, maps_weight, step_weight,
        input_tap_weight, map_tap_weight, step_size_bias, decay_rate_logarithm, direct_path_weight,
        head_norm_scale, output_weight, convolution_input_cache, convolution_map_cache,
        recurrent_state, extra_log_decay,
    ) = args
    layers, seqs, slots, heads = extra_log_decay.shape
    head_size, n_state = recurrent_state.shape[3:]
    hp_cols = heads * head_size
    map_cols = maps_weight.shape[3]
    rows = seqs * slots
    d_here = tokens.shape[1]
    keep = convolution_input_cache.shape[2]
    if not fits(layers, n_tp, n_dp, heads, hp_cols, map_cols, n_state, rows, d_here, keep):
        return general_body(n_tp, n_dp, *args)
    groups = map_cols * n_tp // n_state
    n_z = n_tp // 2
    taps_n = keep + 1
    n_rows = -(-layers * (seqs * keep + taps_n) // 8) * 8

    state = recurrent_state.reshape(layers, seqs, hp_cols, n_state)
    operands = [
        lengths, tokens, input_norm_scale, gate_input_weight,
        jnp.transpose(maps_weight, (0, 2, 3, 1)).reshape(layers, 2 * map_cols, d_here),
        jnp.transpose(step_weight, (0, 2, 1)),
        input_tap_weight, map_tap_weight, step_size_bias, decay_rate_logarithm, direct_path_weight, head_norm_scale,
        jnp.transpose(convolution_input_cache, (0, 2, 1, 3)), convolution_map_cache,
        jnp.transpose(extra_log_decay, (0, 1, 3, 2)), state, output_weight,
    ]
    vmem = pl.BlockSpec(memory_space=pltpu.VMEM)
    hbm = pl.BlockSpec(memory_space=pltpu.HBM)
    sems = lambda *n: pltpu.SemaphoreType.DMA((layers, *n))
    held = [pltpu.VMEM(a.shape, a.dtype) for a in operands[1:-1]]
    held[2] = pltpu.VMEM((layers, hp_cols // LANES, d_here, 2, LANES), BF16)
    results = (
        jax.ShapeDtypeStruct(tokens.shape, F32),
        jax.ShapeDtypeStruct((layers, keep, seqs, hp_cols), BF16),
        jax.ShapeDtypeStruct((layers, seqs, keep, 2, map_cols), BF16),
        jax.ShapeDtypeStruct(state.shape, F32),
    )
    made = pl.pallas_call(
        functools.partial(
            kernel, n_tp, n_dp, d_here * n_dp, groups,
            (layers, seqs, slots, heads, head_size, n_state, hp_cols, map_cols),
        ),
        out_shape=results,
        in_specs=[hbm] * len(operands),
        out_specs=(vmem,) * len(results),
        scratch_shapes=[
            pltpu.SMEM(lengths.shape, jnp.int32),
            *held,
            pltpu.VMEM((layers, 2, hp_cols, d_here // 2), BF16),
            sems(),
            *[
                pltpu.VMEM((layers, n, rows, width), BF16)
                for width in (LANES + 2 * n_state, hp_cols, hp_cols, LANES)
                for n in (n_dp, n_dp - 1)
            ],
            pltpu.VMEM((layers, groups, n_dp, 8, LANES), BF16),
            pltpu.VMEM((layers, n_dp * n_tp, 8, LANES), BF16),
            pltpu.VMEM((groups, 2 * n_rows, LANES), BF16),
            pltpu.VMEM((n_tp, 2 * n_rows, LANES), BF16),
            pltpu.VMEM((layers, 2, n_dp, rows, hp_cols), BF16),
            pltpu.VMEM((layers, n_dp, rows, d_here // 2), BF16),
            pltpu.VMEM((layers, n_z, n_dp, rows, d_here // 2), BF16),
            pltpu.VMEM((layers, 2, n_dp, rows, d_here // 2), BF16),
            pltpu.VMEM((layers, seqs, FRONT + slots, hp_cols), F32),
            pltpu.VMEM((layers, seqs, FRONT + slots, 2 * n_state), F32),
            pltpu.VMEM((2, n_rows, LANES), F32),
            pltpu.VMEM((n_rows, 2 * n_state), F32),
            pltpu.VMEM((layers, LANES + 2 * n_state, d_here), BF16),
            pltpu.VMEM((layers, LANES, d_here), BF16),
            pltpu.VMEM((layers - 1, 2, d_here, hp_cols), BF16),
            pltpu.VMEM((layers - 1, d_here, 2 * LANES + 2 * n_state), BF16),
            pltpu.VMEM((layers, 8, hp_cols), F32),
            pltpu.VMEM((layers, 8, LANES), F32),
            pltpu.VMEM((layers, LANES, LANES), F32),
            pltpu.SemaphoreType.DMA,
            sems(4),
            pltpu.SemaphoreType.DMA,
            pltpu.SemaphoreType.DMA,
            sems(n_dp),
            sems(n_dp),
            sems(n_dp),
            pltpu.SemaphoreType.DMA,
            pltpu.SemaphoreType.DMA((2 * (layers - 1),)),
        ],
        compiler_params=pltpu.CompilerParams(
            collective_id=0, has_side_effects=True, vmem_limit_bytes=32 * 2**20
        ),
        name="mixer",
    )(*[pltpu.with_memory_space_constraint(a, pltpu.HBM) for a in operands])
    stream, conv_in, conv_maps, ssm = pl.pallas_call(
        finish,
        out_shape=results,
        in_specs=[vmem] * len(results),
        out_specs=(hbm,) * len(results),
        scratch_shapes=[pltpu.SemaphoreType.DMA((len(results),))],
        compiler_params=pltpu.CompilerParams(vmem_limit_bytes=2**20),
        name="finish",
    )(*made)
    return stream, jnp.transpose(conv_in, (0, 2, 1, 3)), conv_maps, ssm.reshape(recurrent_state.shape)


def solution(mesh):
    placed = (
        P(None, "dp"),
        P("dp"),
        P(None, "dp"),
        P(None, "dp", None, "tp"),
        P(None, "dp", None, "tp"),
        P(None, "dp", "tp"),
        P(None, None, "tp"),
        P(None, None, None, "tp"),
        P(None, "tp"),
        P(None, "tp"),
        P(None, "tp"),
        P(None, "tp"),
        P(None, "tp", "dp"),
        P(None, "dp", None, "tp"),
        P(None, "dp", None, None, "tp"),
        P(None, "dp", "tp", None, None),
        P(None, "dp", None, "tp"),
    )
    return jax.shard_map(
        functools.partial(body, mesh.shape["tp"], mesh.shape["dp"]),
        mesh=mesh,
        in_specs=placed,
        out_specs=(
            P(None, "dp"),
            P(None, "dp", None, "tp"),
            P(None, "dp", None, None, "tp"),
            P(None, "dp", "tp", None, None),
        ),
        check_vma=False,
    )
```

```python
import functools

import jax
import jax.numpy as jnp
from jax import lax
from jax.experimental import pallas as pl
from jax.experimental.pallas import tpu as pltpu
from jax.sharding import PartitionSpec as P

EPS = 1e-06
LANES = 128
FRONT = 8
F32, BF16 = jnp.float32, jnp.bfloat16


def up(n):
    return -(-n // LANES) * LANES


def dot(a, b, ca=1, cb=0):
    return lax.dot_general(a, b, (((ca,), (cb,)), ((), ())), preferred_element_type=F32)


def thirds(a):
    high = a.astype(BF16)
    rest = a - high.astype(F32)
    middle = rest.astype(BF16)
    return high, middle, (rest - middle.astype(F32)).astype(BF16)


def grid(n_rows, n_cols):
    return (
        lax.broadcasted_iota(jnp.int32, (n_rows, n_cols), 0),
        lax.broadcasted_iota(jnp.int32, (n_rows, n_cols), 1),
    )


def over(a, n):
    return lax.shift_right_logical(a, jnp.full_like(a, n.bit_length() - 1))


def ones_where(cond):
    return jnp.where(cond, 1.0, 0.0).astype(BF16)


def far_first(k, me, n):
    upper = me // (n // 2)
    mirrored = n - 1 - me
    return upper * (k + (k - me + n) // n) + (1 - upper) * (n - 1 - k - (k - mirrored + n) // n)


def general_kernel(
    n_tp, n_dp, d_model, heads, groups, slots, seqs, hp_cols, map_cols,
    lens, x, scale, w_pair, w_maps, w_step, tap_u, tap_m, bias, rate, skip, gain, cache_u, cache_m, extra_t,
    state_hbm, wout_hbm,
    stream, kept, ssm,
    a_send, a_recv, m_send, m_recv, h_send, h_recv, o_send, o_recv, n_send, n_recv, padded, step_w, state, wout, taps, par, extra,
    a_ss, a_rs, m_ss, m_rs, h_ss, h_rs, o_ss, o_rs, n_ss, n_rs, s_sem, w_sem,
):
    tp, dp = lax.axis_index("tp"), lax.axis_index("dp")
    layers = w_pair.shape[0]
    rows = seqs * slots
    taps_n = tap_u.shape[1]
    keep = taps_n - 1
    zc = up(hp_cols)
    ng = map_cols // groups
    n_state = state.shape[-1]
    cut = stream.shape[0] // n_tp
    per = rows // cut
    head_size = hp_cols // heads

    state_copy = pltpu.make_async_copy(state_hbm, state, s_sem)
    wout_copy = pltpu.make_async_copy(wout_hbm, wout, w_sem)
    state_copy.start()
    wout_copy.start()
    barrier = pltpu.get_barrier_semaphore()
    for k in range(1, n_dp):
        pl.semaphore_signal(barrier, inc=1, device_id={"dp": lax.rem(dp + k, n_dp)})
    for k in range(1, n_tp):
        pl.semaphore_signal(barrier, inc=1, device_id={"tp": lax.rem(tp + k, n_tp)})

    stream[...] = x[...].astype(F32)
    slot = lax.broadcasted_iota(jnp.int32, (slots, 1), 0)
    mask = jnp.concatenate([(slot < lens[s]).astype(F32) for s in range(seqs)], axis=0)
    lane = lax.broadcasted_iota(jnp.int32, (1, LANES), 1)
    r, c = grid(rows, rows)
    causal = (over(r, slots) == over(c, slots)) & (c <= r)
    tri = ones_where(causal)
    r, c = grid(2 * map_cols, up(2 * map_cols))
    which = over(r, ng) & 1
    sel = ones_where(c == which * map_cols + groups * (r & (ng - 1)) + over(r, 2 * ng))
    r, c = grid(n_tp * 2 * ng, 2 * n_state)
    sel2 = ones_where(c == (over(r, ng) & 1) * n_state + over(r, 2 * ng) * ng + (r & (ng - 1)))
    r, c = grid(LANES, hp_cols)
    ex = ones_where(r == over(c, head_size))
    r, c = grid(hp_cols, LANES)
    ext = ones_where(c == over(r, head_size))
    r, c = grid(hp_cols, hp_cols)
    ones = ones_where(over(r, head_size) == over(c, head_size))
    r, c = grid(LANES, 2 * LANES)
    spread = ones_where(c == 2 * r)
    padded[...] = jnp.zeros_like(padded)
    step_w[...] = jnp.zeros_like(step_w)
    taps[...] = jnp.zeros_like(taps)
    par[...] = jnp.zeros_like(par)
    extra[...] = jnp.zeros_like(extra)
    for l in range(layers):
        step_w[l, :heads, :] = w_step[l]
        taps[l, :taps_n, :hp_cols] = tap_u[l].astype(F32)
        for t in range(taps_n):
            pair = tap_m[l, t].astype(F32)
            for which in range(2):
                at = zc + which * map_cols
                taps[l, t : t + 1, at : at + map_cols] = pair[which : which + 1]
        par[l, 0:1, :heads] = bias[l : l + 1, :]
        par[l, 1:2, :heads] = rate[l : l + 1, :]
        par[l, 2:3, :heads] = skip[l : l + 1, :]
        for s in range(seqs):
            extra[l, :heads, s * slots : (s + 1) * slots] = extra_t[l, s]
    extra_rows = [extra[l].T[:rows] for l in range(layers)]
    skip_x = [sum(dot(piece, ex) for piece in thirds(par[l]))[2:3] for l in range(layers)]
    sends = []

    def copy(src, dst, ss, rs, where):
        return pltpu.make_async_remote_copy(
            src_ref=src, dst_ref=dst, send_sem=ss, recv_sem=rs, device_id=where
        )

    for l in range(layers):
        st = stream[...]
        squares = jnp.sum(st * st, axis=1, keepdims=True)
        normed = (st * scale[l : l + 1, :]).astype(BF16)
        even = jnp.concatenate(
            [dot(normed[:, i : i + LANES], spread) for i in range(0, normed.shape[1], LANES)], axis=1
        )
        odd = pltpu.roll(even, 1, 1)
        pair = dot(jnp.concatenate([even.astype(BF16), odd.astype(BF16)], axis=0), w_pair[l])
        tokens = st.shape[0]
        tail = dot(normed, step_w[l], 1, 1)
        high = squares.astype(BF16).astype(F32)
        tail = jnp.where(lane == LANES - 2, high, jnp.where(lane == LANES - 1, squares - high, tail))
        part = jnp.concatenate(
            [pair[:tokens], pair[tokens:], dot(normed, w_maps[l], 1, 1), tail], axis=1
        ).astype(BF16)
        for b in range(n_dp):
            a_send[l, b] = part[b * rows : (b + 1) * rows]
        if l == 0:
            pl.semaphore_wait(barrier, n_dp - 1 + n_tp - 1)
        flights = []
        for k in range(1, n_dp):
            to = lax.rem(dp + k, n_dp)
            c = copy(a_send.at[l, to], a_recv.at[l, k - 1], a_ss.at[l, k - 1], a_rs.at[l, k - 1], {"dp": to})
            c.start()
            flights.append(c)
        sends += flights
        acc = a_send[l, dp].astype(F32)
        for k, c in enumerate(flights):
            c.wait_recv()
            acc = acc + a_recv[l, k].astype(F32)
        tail = acc[:, acc.shape[1] - LANES :]
        squares = tail[:, LANES - 2 : LANES - 1] + tail[:, LANES - 1 : LANES]
        factor = lax.rsqrt(squares / d_model + EPS)
        proj = (acc * factor).astype(BF16).astype(F32)

        conv_w = taps.shape[2]
        pieces = []
        for s in range(seqs):
            for t in range(keep):
                at = FRONT - keep + t
                padded[s, at : at + 1, :hp_cols] = cache_u[l, t].astype(F32)[s : s + 1]
                pair = cache_m[l, s, t].astype(F32)
                for which in range(2):
                    col = zc + which * map_cols
                    padded[s, at : at + 1, col : col + map_cols] = pair[which : which + 1]
            padded[s, FRONT : FRONT + slots, :] = proj[s * slots : (s + 1) * slots, zc : zc + conv_w]
            total = padded[s, FRONT - keep : FRONT - keep + slots, :] * taps[l, 0:1, :]
            for t in range(1, taps_n):
                at = FRONT - keep + t
                total = total + padded[s, at : at + slots, :] * taps[l, t : t + 1, :]
            pieces.append(total)
        filtered = jnp.concatenate(pieces, axis=0)
        filtered = filtered * jax.nn.sigmoid(filtered)
        maps = filtered[:, conv_w - up(2 * map_cols) :].astype(BF16)
        sorted_maps = dot(sel, maps, 1, 1)
        for g in range(groups):
            m_send[l, g] = sorted_maps[g * 2 * ng : (g + 1) * 2 * ng, :].astype(BF16)

        def group_of(rank):
            return rank * heads // (heads * n_tp // groups)

        flights = []
        for k in range(n_tp - 1):
            to = far_first(k, tp, n_tp)
            c = copy(m_send.at[l, group_of(to)], m_recv.at[l, tp], m_ss.at[l, k], m_rs.at[l, tp], {"tp": to})
            c.start()
            sends.append(c)
        m_recv[l, tp] = m_send[l, group_of(tp)]

        for s in range(seqs):
            pick = lax.broadcasted_iota(jnp.int32, (8, FRONT + slots), 0)
            place = lax.broadcasted_iota(jnp.int32, (8, FRONT + slots), 1)
            chooser = ((place == pick + lens[s] + (FRONT - keep)) & (pick < keep)).astype(BF16)
            kept[l, s] = dot(chooser, padded[s].astype(BF16)).astype(BF16)
        raw = proj[:, proj.shape[1] - LANES :] + par[l, 0:1, :]
        step = (jnp.maximum(raw, 0.0) + jnp.log1p(jnp.exp(-jnp.abs(raw)))) * mask
        step = jnp.where(lane < heads, step, 0.0)
        logdec = extra_rows[l] * mask - step * jnp.exp(par[l, 1:2, :])
        logdec = jnp.where(lane < heads, logdec, 0.0)
        parts = dot(tri, jnp.concatenate(thirds(logdec), axis=1))
        sums = parts[:, :LANES] + parts[:, LANES : 2 * LANES] + parts[:, 2 * LANES :]
        sums_t = sums.T
        step_t = step.T
        sums_parts, step_parts = thirds(sums), thirds(step)
        both = dot(jnp.concatenate(sums_parts + step_parts, axis=0), ex)
        sums_x = both[:rows] + both[rows : 2 * rows] + both[2 * rows : 3 * rows]
        step_x = both[3 * rows : 4 * rows] + both[4 * rows : 5 * rows] + both[5 * rows :]
        inp = filtered[:, :hp_cols]
        gate = proj[:, :hp_cols]
        last_x = jnp.concatenate(
            [
                jnp.broadcast_to(sums_x[(s + 1) * slots - 1 : (s + 1) * slots, :], (slots, hp_cols))
                for s in range(seqs)
            ],
            axis=0,
        )
        weighted = (jnp.exp(last_x - sums_x) * step_x * inp).astype(BF16)
        inp_b = inp.astype(BF16)
        grow = jnp.exp(sums_x)
        direct = skip_x[l] * inp
        gate = gate * jax.nn.sigmoid(gate)
        rows_sum = sum(dot(ext, piece, 1, 1) for piece in sums_parts)
        segs = []
        for h in range(heads):
            gap = sums[:, h : h + 1] - sums_t[h : h + 1, :]
            segs.append(jnp.exp(jnp.where(causal, gap, -jnp.inf)) * step_t[h : h + 1, :])

        if l == 0:
            state_copy.wait()
            wout_copy.wait()
        for k in range(1, n_tp):
            src = lax.rem(tp + n_tp - k, n_tp)
            copy(m_send.at[l, 0], m_recv.at[l, src], m_ss.at[l, 0], m_rs.at[l, src], {"tp": src}).wait_recv()
        got = m_recv[l].astype(F32).reshape(n_tp * 2 * ng, rows)
        both_maps = dot(got.T.astype(BF16), sel2).astype(BF16)
        b_map, c_map = both_maps[:, :n_state], both_maps[:, n_state:]
        cross = dot(c_map, b_map, 1, 1)
        within = jnp.concatenate(
            [
                dot((cross * segs[h]).astype(BF16), inp_b[:, h * head_size : (h + 1) * head_size])
                for h in range(heads)
            ],
            axis=1,
        )
        carried = jnp.concatenate(
            [
                dot(c_map[s * slots : (s + 1) * slots], state[l, s].astype(BF16), 1, 1)
                for s in range(seqs)
            ],
            axis=0,
        )
        read = (within + carried * grow + direct) * gate
        power = read * read
        p_hi = power.astype(BF16)
        p_lo = (power - p_hi.astype(F32)).astype(BF16)
        mean = (dot(p_hi, ones) + dot(p_lo, ones)) / head_size
        headout = (read * lax.rsqrt(mean + EPS) * gain[l : l + 1, :] * mask).astype(BF16)
        h_send[l] = headout
        flights = []
        for k in range(1, n_dp):
            to = lax.rem(dp + k, n_dp)
            c = copy(h_send.at[l], h_recv.at[l, k - 1], h_ss.at[l, k - 1], h_rs.at[l, k - 1], {"dp": to})
            c.start()
            flights.append(c)
        sends += flights

        def push(value, block):
            out = dot(value, wout[l]).astype(BF16)
            for i in range(per):
                to = block * per + i
                o_send[l, to] = out[i * cut : (i + 1) * cut]

                @pl.when(to != tp)
                def _():
                    copy(o_send.at[l, to], o_recv.at[l, tp], o_ss.at[l, to], o_rs.at[l, tp], {"tp": to}).start()

        push(headout, dp)
        for s in range(seqs):
            at = slice(s * slots, (s + 1) * slots)
            fresh = dot(weighted[at], b_map[at], 0, 0)
            end = (s + 1) * slots - 1
            ssm[l, s] = jnp.exp(rows_sum[:, end : end + 1]) * state[l, s] + fresh
        for k, c in enumerate(flights):
            c.wait_recv()
            push(h_recv[l, k], lax.rem(dp + n_dp - k - 1, n_dp))
        total = o_send[l, tp].astype(F32)
        for k in range(1, n_tp):
            src = lax.rem(tp + n_tp - k, n_tp)
            copy(o_send.at[l, src], o_recv.at[l, src], o_ss.at[l, src], o_rs.at[l, src], {"tp": src}).wait_recv()
            total = total + o_recv[l, src].astype(F32)
        fresh = total.astype(BF16)
        n_send[l] = fresh
        n_recv[l, tp] = fresh
        for k in range(n_tp - 1):
            to = far_first(k, tp, n_tp)
            c = copy(n_send.at[l], n_recv.at[l, tp], n_ss.at[l, k], n_rs.at[l, tp], {"tp": to})
            c.start()
            sends.append(c)
        for k in range(1, n_tp):
            src = lax.rem(tp + n_tp - k, n_tp)
            copy(n_send.at[l], n_recv.at[l, src], n_ss.at[l, 0], n_rs.at[l, src], {"tp": src}).wait_recv()
        stream[...] += n_recv[l].astype(F32).reshape(stream.shape)

    for c in sends:
        c.wait_send()
    for l in range(layers):
        for k in range(1, n_tp):
            to = lax.rem(tp + k, n_tp)
            copy(o_send.at[l, to], o_recv.at[l, tp], o_ss.at[l, to], o_rs.at[l, tp], {"tp": to}).wait_send()


def general_body(
    n_tp, n_dp,
    tokens, lengths, input_norm_scale, gate_input_weight, maps_weight, step_weight,
    input_tap_weight, map_tap_weight, step_size_bias, decay_rate_logarithm, direct_path_weight,
    head_norm_scale, output_weight, convolution_input_cache, convolution_map_cache,
    recurrent_state, extra_log_decay,
):
    layers, seqs, slots, heads = extra_log_decay.shape
    head_size, n_state = recurrent_state.shape[3:]
    hp_cols = heads * head_size
    map_cols = maps_weight.shape[3]
    groups = map_cols * n_tp // n_state
    ng = map_cols // groups
    rows = seqs * slots
    d_here = tokens.shape[1]
    keep = convolution_input_cache.shape[2]

    def wide(a):
        pad = up(a.shape[-1]) - a.shape[-1]
        return a if pad == 0 else jnp.pad(a, [(0, 0)] * (a.ndim - 1) + [(0, pad)])

    w_pair = wide(gate_input_weight.reshape(layers, 2 * d_here, hp_cols))
    w_maps = jnp.transpose(maps_weight, (0, 2, 3, 1)).reshape(layers, 2 * map_cols, d_here)
    if up(2 * map_cols) > 2 * map_cols:
        w_maps = jnp.pad(w_maps, ((0, 0), (0, up(2 * map_cols) - 2 * map_cols), (0, 0)))
    w_step = jnp.transpose(step_weight, (0, 2, 1))
    cache_u = jnp.transpose(convolution_input_cache, (0, 2, 1, 3))
    extra_t = jnp.transpose(extra_log_decay, (0, 1, 3, 2))
    state = recurrent_state.reshape(layers, seqs, hp_cols, n_state)

    vmem = pl.BlockSpec(memory_space=pltpu.VMEM)
    wide_cols = 2 * up(hp_cols) + up(2 * map_cols) + LANES
    anywhere = pl.BlockSpec(memory_space=pl.ANY)
    conv_w = up(hp_cols) + up(2 * map_cols)
    cut = tokens.shape[0] // n_tp
    sems = lambda n: pltpu.SemaphoreType.DMA((layers, n))
    args = [tokens, input_norm_scale, w_pair, w_maps, w_step, input_tap_weight,
        map_tap_weight, step_size_bias, decay_rate_logarithm, direct_path_weight, head_norm_scale,
        cache_u, convolution_map_cache, extra_t]
    stream, kept, ssm = pl.pallas_call(
        functools.partial(
            general_kernel, n_tp, n_dp, d_here * n_dp, heads, groups, slots, seqs, hp_cols, map_cols
        ),
        out_shape=(
            jax.ShapeDtypeStruct(tokens.shape, F32),
            jax.ShapeDtypeStruct((layers, seqs, 8, conv_w), BF16),
            jax.ShapeDtypeStruct(state.shape, F32),
        ),
        in_specs=[pl.BlockSpec(memory_space=pltpu.SMEM)] + [vmem] * len(args) + [anywhere] * 2,
        out_specs=(vmem, vmem, vmem),
        scratch_shapes=[
            pltpu.VMEM((layers, n_dp, rows, wide_cols), BF16),
            pltpu.VMEM((layers, n_dp - 1, rows, wide_cols), BF16),
            pltpu.VMEM((layers, groups, 2 * ng, rows), BF16),
            pltpu.VMEM((layers, n_tp, 2 * ng, rows), BF16),
            pltpu.VMEM((layers, rows, hp_cols), BF16),
            pltpu.VMEM((layers, n_dp - 1, rows, hp_cols), BF16),
            pltpu.VMEM((layers, n_tp, cut, d_here), BF16),
            pltpu.VMEM((layers, n_tp, cut, d_here), BF16),
            pltpu.VMEM((layers, cut, d_here), BF16),
            pltpu.VMEM((layers, n_tp, cut, d_here), BF16),
            pltpu.VMEM((seqs, FRONT + slots, conv_w), F32),
            pltpu.VMEM((layers, LANES, d_here), BF16),
            pltpu.VMEM(state.shape, F32),
            pltpu.VMEM(output_weight.shape, BF16),
            pltpu.VMEM((layers, 8, conv_w), F32),
            pltpu.VMEM((layers, 8, LANES), F32),
            pltpu.VMEM((layers, LANES, LANES), F32),
            sems(n_dp - 1), sems(n_dp - 1), sems(n_tp - 1), sems(n_tp), sems(n_dp - 1),
            sems(n_dp - 1), sems(n_tp), sems(n_tp), sems(n_tp - 1), sems(n_tp),
            pltpu.SemaphoreType.DMA, pltpu.SemaphoreType.DMA,
        ],
        compiler_params=pltpu.CompilerParams(
            collective_id=0, has_side_effects=True, vmem_limit_bytes=48 * 2**20
        ),
        name="mixer",
    )(lengths, *args, state, output_weight)
    conv_in = kept[:, :, :keep, :hp_cols]
    start = conv_w - up(2 * map_cols)
    conv_maps = kept[:, :, :keep, start : start + 2 * map_cols].reshape(
        layers, seqs, keep, 2, map_cols
    )
    return stream, conv_in, conv_maps, ssm.reshape(recurrent_state.shape)


def peers(n, order):
    return [k for k in order if 0 < k < n] + [k for k in range(1, n) if k not in order]


def kernel(
    n_tp, n_dp, d_model, groups, shapes,
    *refs,
):
    names = (
        "lens", "x", "scale", "gate", "w_maps", "w_step", "tap_u", "tap_m", "bias", "rate", "skip", "gain",
        "cache_u", "cache_m", "extra_t", "state", "wout",
    )
    hbm = dict(zip(names, refs[: len(names)]))
    (
        stream, kept_u, kept_m, ssm,
        lens, x, scale, w_gate, w_maps, w_step, tap_u, tap_m, bias, rate, skip, gain, cache_u, cache_m, extra_t, state,
        wout, g_sem, state_b,
        t_send, t_recv, u_send, u_recv, z_send, z_recv, q_send, q_recv, m_send, m_recv, c_send, c_recv, h_recv, o_send, o_recv, nb,
        padded, padded_m, mrow, mrows, w_rows, w_sorted, w_flat, w_turned, taps, par, extra,
        out_sem, a_rs, m_rs, c_rs, h_rs, o_rs, n_rs, w_rs, f_rs,
    ) = refs[len(names) :]
    layers, seqs, slots, heads, head_size, n_state, hp_cols, map_cols = shapes
    tp, dp = lax.axis_index("tp"), lax.axis_index("dp")
    rows = seqs * slots
    taps_n = tap_u.shape[1]
    keep = taps_n - 1
    ng = map_cols // groups
    pair_cols = 2 * ng
    quads = LANES // pair_cols
    d_here = x.shape[1]
    half = d_here // 2
    tokens = x.shape[0]
    side = lax.rem(tp, 2)
    zed = lax.div(tp, 2)
    n_z = n_tp // 2
    every = n_tp * n_dp
    me = dp * n_tp + tp
    dp_peers = peers(n_dp, (3, 1, 2))
    turns = peers(n_dp, (1, 2, 3))
    z_peers = peers(n_z, (3, 2, 1))

    def remote(src, dst, arrived, where):
        return pltpu.make_async_remote_copy(
            src_ref=src, dst_ref=dst, send_sem=out_sem, recv_sem=arrived, device_id=where
        )

    def landed(block, arrived):
        remote(block, block, arrived, {"tp": jnp.bitwise_xor(tp, 1)}).wait_recv()

    barrier = pltpu.get_barrier_semaphore()
    others = [
        (i, j) for i in [*peers(n_tp, (6, 7, 4, 5, 2, 3, 1)), 0] for j in [*dp_peers, 0] if i or j
    ]

    def at(i, j):
        return {"tp": jnp.bitwise_xor(tp, i), "dp": jnp.bitwise_xor(dp, j)}

    spare = [
        *[o_rs.at[layers - 1, k] for k in range(n_dp)], *[h_rs.at[layers - 1, k] for k in range(n_dp)],
        *[n_rs.at[layers - 1, k] for k in range(n_dp)], *[a_rs.at[layers - 1, p] for p in range(4)],
        f_rs.at[0], w_rs,
    ]
    local = {}
    pairs = dict(
        x=x, scale=scale, w_maps=w_maps, w_step=w_step, lens=lens, tap_u=tap_u, tap_m=tap_m, bias=bias, rate=rate,
        skip=skip, gain=gain, cache_u=cache_u, cache_m=cache_m, extra_t=extra_t, state=state,
    )
    for n, name in enumerate(pairs):
        local[name] = pltpu.make_async_copy(hbm[name], pairs[name], spare[n])
    mine = pl.ds(pl.multiple_of(side * half, LANES), half)
    theirs = pl.ds(pl.multiple_of((1 - side) * half, LANES), half)
    local["wout"] = pltpu.make_async_copy(hbm["wout"].at[:, :, mine], wout.at[:, 0], spare[len(pairs)])
    gate_copies = [
        [
            pltpu.make_async_copy(
                hbm["gate"].at[l, :, :, i : i + LANES], w_gate.at[l, i // LANES], g_sem.at[l]
            )
            for i in range(0, hp_cols, LANES)
        ]
        for l in range(layers)
    ]
    first = ("x", "scale", "w_maps", "w_step")
    for name in first:
        local[name].start()
    for c in gate_copies[0]:
        c.start()
    for i, j in others:
        pl.semaphore_signal(barrier, inc=1, device_id=at(i, j))
    for name in local:
        if name not in first:
            local[name].start()
    for l in range(1, layers):
        for c in gate_copies[l]:
            c.start()

    lane = lax.broadcasted_iota(jnp.int32, (1, LANES), 1)
    r, c = grid(LANES, 4 * LANES)
    spread = ones_where(c == jnp.where(c < 2 * LANES, 2 * r, 2 * LANES + 2 * r + 1))
    r, c = grid(LANES, LANES)
    place = (c + LANES - ng * tp) & (LANES - 1)
    wanted = (over(place, ng) & 1) * map_cols + groups * (place & (ng - 1)) + over(place, pair_cols)
    sorter = ones_where(r == wanted)
    home = over((lane + LANES - ng * tp) & (LANES - 1), pair_cols)
    for l in range(layers):
        w_rows[l, :LANES] = jnp.zeros_like(w_rows[l, :LANES])
    gate_rows = w_gate.reshape(layers, hp_cols // LANES, 2 * d_here, LANES)

    def group_of(rank):
        return rank * groups // n_tp

    def with_squares(tail, squares):
        high = squares.astype(BF16).astype(F32)
        return jnp.where(lane == LANES - 2, high, jnp.where(lane == LANES - 1, squares - high, tail))

    def fill(buffer, l, value):
        for b in range(n_dp):
            buffer[l, b, :, : value.shape[1]] = value[b * rows : (b + 1) * rows].astype(BF16)

    def pack_maps(l, raw):
        turned = [raw if k == 0 else pltpu.roll(raw, k * pair_cols, 1) for k in range(quads)]
        turned = [t.reshape(n_dp, quads, 8, LANES) for t in turned]
        for g in range(groups):
            piece = turned[(0 - g) % quads][:, 0]
            for q in range(1, quads):
                piece = jnp.where((home == q)[None], turned[(q - g) % quads][:, q], piece)
            m_send[l, g] = piece.astype(BF16)

    def send_maps(l):
        for i, j in others:
            to = at(i, j)
            remote(
                m_send.at[l, group_of(to["tp"]), to["dp"]], m_recv.at[l, me], m_rs, to
            ).start()
        m_recv[l, me] = m_send[l, group_of(tp), dp]

    def rows_of(rank, which):
        return pl.ds(pl.multiple_of(LANES + which * n_state + ng * rank, ng), ng)

    def pick_rows(rank, which):
        return pl.ds(pl.multiple_of(pair_cols * group_of(rank) + which * ng, ng), ng)

    def fetch(i, k, which):
        to = jnp.bitwise_xor(tp, k)
        n = 2 * (i - 1) + (k == 1)
        return remote(
            w_sorted.at[i, pick_rows(to, which)], w_rows.at[i, rows_of(tp, which)], f_rs.at[n], {"tp": to}
        )

    def relay(i, j, which):
        n = 2 * (i - 1) + 1
        block = w_rows.at[i, rows_of(jnp.bitwise_xor(tp, 2 * j), which)]
        return remote(block, block, f_rs.at[n], at(1, 0))

    def fetched(i, far):
        n = 2 * (i - 1) + 1 - far
        landed(w_rows.at[i, pl.ds(LANES, 2 * ng * (n_z - 1 if far else n_z))], f_rs.at[n])

    parts_of = ((t_send, t_recv), (u_send, u_recv), (z_send, z_recv), (q_send, q_recv))

    def part(l, p, k):
        send, recv = parts_of[p]
        to = jnp.bitwise_xor(dp, k)
        src, dst = send.at[l, to], recv.at[l, k - 1]
        if p == 0 and l == 0:
            src, dst = src.at[:, :LANES], dst.at[:, :LANES]
        return remote(src, dst, a_rs.at[l, p], {"dp": to})

    def send_part(l, p):
        for k in dp_peers:
            part(l, p, k).start()

    def await_part(l, p):
        send, recv = parts_of[p]
        width = LANES if p == 0 and l == 0 else send.shape[-1]
        landed(recv.at[l, :, :, :width], a_rs.at[l, p])
        acc = send[l, dp, :, :width].astype(F32)
        for k in range(1, n_dp):
            acc = acc + recv[l, k - 1, :, :width].astype(F32)
        return acc

    def flat_weight(l):
        return jnp.concatenate([gate_rows[l, i] for i in range(hp_cols // LANES)], axis=1)

    sends = []
    for name in first:
        local[name].wait()
    for l in range(layers):
        w_rows[l, :heads, :] = w_step[l]
    w_sorted[0] = dot(sorter, w_maps[0], 0, 0).astype(BF16)
    stream[...] = x[...].astype(F32)

    for l in range(layers):
        if l == 0:
            st = stream[...]
            squares = jnp.sum(st * st, axis=1, keepdims=True)
            normed = (st * scale[l : l + 1, :]).astype(BF16)
            raw = dot(normed, w_sorted[l], 1, 1)
            pack_maps(l, raw)
            fill(t_send, l, with_squares(dot(normed, w_rows[l, :LANES], 1, 1), squares))
            spreads = [dot(normed[:, i : i + LANES], spread).astype(BF16) for i in range(0, d_here, LANES)]
            even = jnp.concatenate([s[:, : 2 * LANES] for s in spreads], axis=1)
            odd = jnp.concatenate([s[:, 2 * LANES :] for s in spreads], axis=1)
            pltpu.make_async_copy(w_gate.at[l], w_gate.at[l], g_sem.at[l]).wait()
            both = dot(jnp.concatenate([odd, even], axis=0), flat_weight(l))
            fill(u_send, l, both[:tokens])
            fill(z_send, l, both[tokens:])
            fill(q_send, l, raw)
            pl.semaphore_wait(barrier, every - 1)
            send_maps(l)
            for p in range(4):
                send_part(l, p)

        if l == 0:
            for n in range(len(pairs) + 1):
                name = [*pairs, "wout"][n]
                if name not in first:
                    local[name].wait()
            swap = remote(hbm["wout"].at[:, :, theirs], wout.at[:, 1], w_rs, {"tp": jnp.bitwise_xor(tp, 1)})
            swap.start()
            per_layer = seqs * keep + taps_n
            mrow[...] = jnp.zeros_like(mrow)
            for i in range(layers):
                for s in range(seqs):
                    for t in range(keep):
                        pair = cache_m[i, s, t].astype(F32)
                        n = i * per_layer + s * keep + t
                        for which in range(2):
                            mrow[which, n : n + 1, :map_cols] = pair[which : which + 1]
                for t in range(taps_n):
                    pair = tap_m[i, t].astype(F32)
                    n = i * per_layer + seqs * keep + t
                    for which in range(2):
                        mrow[which, n : n + 1, :map_cols] = pair[which : which + 1]
            n_rows = mrow.shape[1]
            r, c = grid(LANES, groups * LANES)
            n = (c & (LANES - 1)) - ng * tp
            chosen = (n >= 0) & (n < ng) & (r == groups * n + over(c, LANES))
            packed = dot(mrow[...].reshape(2 * n_rows, LANES).astype(BF16), ones_where(chosen)).astype(BF16)
            for g in range(groups):
                c_send[g] = packed[:, g * LANES : (g + 1) * LANES]
            for k in peers(n_tp, (6, 7, 4, 5, 2, 3, 1)):
                to = jnp.bitwise_xor(tp, k)
                c = remote(c_send.at[group_of(to)], c_recv.at[k], c_rs, {"tp": to})
                c.start()
                sends.append(c)
            c_recv[0] = c_send[group_of(tp)]
            r, c = grid(LANES, LANES)
            resort = ones_where(r == (over(c, ng) & 1) * map_cols + groups * (c & (ng - 1)) + over(c, pair_cols))
            for i in range(1, layers):
                w_sorted[i] = dot(resort, w_maps[i], 0, 0).astype(BF16)

            slot = lax.broadcasted_iota(jnp.int32, (slots, 1), 0)
            mask = jnp.concatenate([(slot < lens[s]).astype(F32) for s in range(seqs)], axis=0)
            r, c = grid(rows, rows)
            causal = (over(r, slots) == over(c, slots)) & (c <= r)
            within_sequence = lax.broadcasted_iota(jnp.int32, (rows, LANES), 0) & (slots - 1)
            r, c = grid(LANES, hp_cols)
            ex = ones_where(r == over(c, head_size))
            r, c = grid(hp_cols, LANES)
            ext = ones_where(c == over(r, head_size))
            r, c = grid(hp_cols, hp_cols)
            ones = ones_where(over(r, head_size) == over(c, head_size))
            padded[...] = jnp.zeros_like(padded)
            padded_m[...] = jnp.zeros_like(padded_m)
            taps[...] = jnp.zeros_like(taps)
            par[...] = jnp.zeros_like(par)
            extra[...] = jnp.zeros_like(extra)
            for i in range(layers):
                taps[i, :taps_n, :] = tap_u[i].astype(F32)
                par[i, 0:1, :heads] = bias[i : i + 1, :]
                par[i, 1:2, :heads] = rate[i : i + 1, :]
                par[i, 2:3, :heads] = skip[i : i + 1, :]
                for s in range(seqs):
                    extra[i, :heads, s * slots : (s + 1) * slots] = extra_t[i, s]
                    for t in range(keep):
                        n = FRONT - keep + t
                        padded[i, s, n : n + 1, :] = cache_u[i, t].astype(F32)[s : s + 1]
            state_b[...] = state[...].astype(BF16)
            extra_rows = [extra[i].T[:rows] for i in range(layers)]
            skip_x = [sum(dot(piece, ex) for piece in thirds(par[i]))[2:3] for i in range(layers)]

        def convolve(pad, weights):
            pieces = []
            for s in range(seqs):
                total = pad[l, s, FRONT - keep : FRONT - keep + slots, :] * weights[0:1]
                for t in range(1, taps_n):
                    n = FRONT - keep + t
                    total = total + pad[l, s, n : n + slots, :] * weights[t : t + 1]
                pieces.append(total)
            out = jnp.concatenate(pieces, axis=0)
            return out * jax.nn.sigmoid(out)

        acc = await_part(l, 0)
        tail = acc[:, :LANES]
        squares = tail[:, LANES - 2 : LANES - 1] + tail[:, LANES - 1 : LANES]
        factor = lax.rsqrt(squares / d_model + EPS)
        raw_step = (tail * factor).astype(BF16).astype(F32) + par[l, 0:1, :]
        step = (jnp.maximum(raw_step, 0.0) + jnp.log1p(jnp.exp(-jnp.abs(raw_step)))) * mask
        step = jnp.where(lane < heads, step, 0.0)
        logdec = extra_rows[l] * mask - step * jnp.exp(par[l, 1:2, :])
        logdec = jnp.where(lane < heads, logdec, 0.0)
        sums = logdec
        for n in [2**i for i in range(slots.bit_length()) if 2**i < slots]:
            sums = sums + jnp.where(within_sequence >= n, pltpu.roll(sums, n, 0), 0.0)
        sums_t = sums.T
        step_t = step.T
        sums_parts, step_parts = thirds(sums), thirds(step)
        both = dot(jnp.concatenate(sums_parts + step_parts, axis=0), ex)
        sums_x = both[:rows] + both[rows : 2 * rows] + both[2 * rows : 3 * rows]
        step_x = both[3 * rows : 4 * rows] + both[4 * rows : 5 * rows] + both[5 * rows :]
        grow = jnp.exp(sums_x)
        segs = []
        for h in range(heads):
            gap = sums[:, h : h + 1] - sums_t[h : h + 1, :]
            segs.append(jnp.exp(jnp.where(causal, gap, -jnp.inf)) * step_t[h : h + 1, :])

        def filter_inputs(acc):
            proj = (acc * factor).astype(BF16).astype(F32)
            for s in range(seqs):
                padded[l, s, FRONT : FRONT + slots, :] = proj[s * slots : (s + 1) * slots]
            return convolve(padded, taps[l])

        def unpack_maps():
            landed(m_recv.at[l, 0 : every - 1], m_rs)
            got = m_recv[l].astype(F32).reshape(n_dp, n_tp, 8, LANES)
            got = sum(got[b] for b in range(n_dp))
            cell = over(lane, ng)
            columns = []
            for which in range(2):
                blocks = []
                for q in range(quads):
                    n = 2 * q + which
                    piece = got[0]
                    for t in range(1, n_tp):
                        piece = jnp.where(cell == (n + t) % n_tp, got[t], piece)
                    blocks.append(piece if n == 0 else pltpu.roll(piece, LANES - ng * n, 1))
                columns.append(jnp.concatenate(blocks, axis=0))
            return jnp.concatenate(columns, axis=1)

        def filter_maps(raw):
            proj = (raw * factor).astype(BF16).astype(F32)
            for s in range(seqs):
                padded_m[l, s, FRONT : FRONT + slots, :] = proj[s * slots : (s + 1) * slots]
            n = l * per_layer + seqs * keep
            maps = convolve(padded_m, mrows[n : n + taps_n, :]).astype(BF16)
            b_map, c_map = maps[:, :n_state], maps[:, n_state:]
            carried = jnp.concatenate(
                [
                    dot(c_map[s * slots : (s + 1) * slots], state_b[l, s], 1, 1)
                    for s in range(seqs)
                ],
                axis=0,
            )
            return b_map, dot(c_map, b_map, 1, 1), carried * grow

        def gate_of(acc):
            gate = (acc * factor).astype(BF16).astype(F32)
            return gate * jax.nn.sigmoid(gate)

        if l == 0:
            inp = filter_inputs(await_part(l, 1))
            gate = gate_of(await_part(l, 2))
            landed(c_recv.at[1:n_tp], c_rs)
            total = c_recv[0].astype(F32)
            for k in range(1, n_tp):
                total = total + c_recv[k].astype(F32)
            mrows[...] = jnp.concatenate([total[:n_rows], total[n_rows:]], axis=1)
            for i in range(layers):
                for s in range(seqs):
                    n = i * per_layer + s * keep
                    padded_m[i, s, FRONT - keep : FRONT, :] = mrows[n : n + keep, :]
            maps_in = unpack_maps()
            for i in range(1, layers):
                for k in [*[2 * j for j in z_peers], 1]:
                    for which in range(2):
                        fetch(i, k, which).start()
                for which in range(2):
                    w_rows[i, rows_of(tp, which), :] = w_sorted[i, pick_rows(tp, which), :]
            b_map, cross, carried = filter_maps(maps_in)
        else:
            b_map, cross, carried = filter_maps(acc[:, LANES:])
            inp = filter_inputs(await_part(l, 1))
        inp_b = inp.astype(BF16)
        within = jnp.concatenate(
            [
                dot((cross * segs[h]).astype(BF16), inp_b[:, h * head_size : (h + 1) * head_size])
                for h in range(heads)
            ],
            axis=1,
        )
        inner = within + carried + skip_x[l] * inp
        if l > 0:
            gate = gate_of(await_part(l, 2))
        read = inner * gate
        power = read * read
        p_hi = power.astype(BF16)
        p_lo = (power - p_hi.astype(F32)).astype(BF16)
        mean = (dot(p_hi, ones) + dot(p_lo, ones)) / head_size
        headout = (read * lax.rsqrt(mean + EPS) * gain[l : l + 1, :] * mask).astype(BF16)
        h_recv[l, 0, 0] = headout
        own = h_recv.at[l, 0, 0]
        targets = [(1, 0)] + [(i, k) for k in turns for i in (0, 1)]
        for i, k in targets:
            remote(own, h_recv.at[l, i, k], h_rs.at[l, k], at(i, k)).start()

        def push(k):
            value = jnp.concatenate([h_recv[l, 0, k], h_recv[l, 1, k]], axis=1)
            block = jnp.bitwise_xor(dp, k)
            o_send[l, k] = dot(value, wout[l].reshape(2 * hp_cols, half)).astype(BF16)
            for j in z_peers:
                remote(
                    o_send.at[l, k], o_recv.at[l, j, k], o_rs.at[l, k],
                    {"tp": jnp.bitwise_xor(tp, 2 * j)},
                ).start()

        if l == 0:
            swap.wait_recv()
        landed(h_recv.at[l, 1, 0], h_rs.at[l, 0])
        push(0)
        last_x = jnp.concatenate(
            [
                jnp.broadcast_to(sums_x[(s + 1) * slots - 1 : (s + 1) * slots, :], (slots, hp_cols))
                for s in range(seqs)
            ],
            axis=0,
        )
        weighted = (jnp.exp(last_x - sums_x) * step_x * inp).astype(BF16)
        rows_sum = sum(dot(ext, piece, 1, 1) for piece in sums_parts)
        for s in range(seqs):
            span = slice(s * slots, (s + 1) * slots)
            fresh = dot(weighted[span], b_map[span], 0, 0)
            end = (s + 1) * slots - 1
            ssm[l, s] = jnp.exp(rows_sum[:, end : end + 1]) * state[l, s] + fresh
        if l + 1 < layers:
            pltpu.make_async_copy(w_gate.at[l + 1], w_gate.at[l + 1], g_sem.at[l + 1]).wait()
            weight = flat_weight(l + 1)
            r, c = grid(LANES, 2 * LANES)
            for which in range(2):
                picker = ones_where(c == 2 * r + which)
                for n in range(0, d_here, LANES):
                    w_flat[l, which, n : n + LANES] = dot(picker, weight[2 * n : 2 * (n + LANES)]).astype(BF16)
        for k in turns:
            landed(h_recv.at[l, :, k], h_rs.at[l, k])
            push(k)

        r, c = grid(LANES, LANES)
        if l == 0:
            r = (r + LANES - ng * tp) & (LANES - 1)
        unsort = ones_where(
            c == (over(r, ng) & 1) * map_cols + groups * (r & (ng - 1)) + over(r, pair_cols)
        )
        own_maps = dot((await_part(l, 3) * factor).astype(BF16), unsort)
        for s in range(seqs):
            pick = lax.broadcasted_iota(jnp.int32, (8, FRONT + slots), 0)
            spot = lax.broadcasted_iota(jnp.int32, (8, FRONT + slots), 1)
            chooser = ((spot == pick + lens[s] + (FRONT - keep)) & (pick < keep)).astype(BF16)
            kept = dot(chooser, padded[l, s].astype(BF16)).astype(BF16)
            r, c = grid(8, slots)
            later_pick = ones_where((c == r + lens[s] - keep) & (r < keep))
            maps_kept = dot(later_pick, own_maps[s * slots : (s + 1) * slots].astype(BF16))
            for t in range(keep):
                kept_u[l, t, s : s + 1, :] = kept[t : t + 1]
                old = jnp.zeros((1, LANES), F32)
                for n in range(keep):
                    flat = jnp.concatenate(
                        [cache_m[l, s, n].astype(F32)[which : which + 1] for which in range(2)], axis=1
                    )
                    old = jnp.where(t + lens[s] == n, flat, old)
                line = (maps_kept[t : t + 1] + old).astype(BF16)
                for which in range(2):
                    kept_m[l, s, t, which : which + 1, :] = line[:, which * map_cols : (which + 1) * map_cols]

        def gather(k):
            landed(o_recv.at[l, 1:n_z, k], o_rs.at[l, k])
            o_recv[l, 0, k] = o_send[l, k]
            block = jnp.bitwise_xor(dp, k)
            total = o_recv[l, zed, k].astype(F32)
            for z in range(1, n_z):
                total = total + o_recv[l, jnp.bitwise_xor(zed, z), k].astype(F32)
            nb[l, side, block] = total.astype(BF16)
            remote(
                nb.at[l, side, block], nb.at[l, side, block], n_rs.at[l, k], at(1, 0)
            ).start()

        if l == 0:
            for i in range(1, layers):
                fetched(i, 1)
                for j in z_peers:
                    for which in range(2):
                        relay(i, j, which).start()
        def receive(k):
            landed(nb.at[l, 1 - side, jnp.bitwise_xor(dp, k)], n_rs.at[l, k])
            block = jnp.bitwise_xor(dp, k)
            span = pl.ds(pl.multiple_of(block * rows, rows), rows)
            st = stream[span, :] + jnp.concatenate([nb[l, h, block].astype(F32) for h in range(2)], axis=1)
            stream[span, :] = st
            n = l + 1
            if n == layers:
                return
            squares = jnp.sum(st * st, axis=1, keepdims=True)
            normed = (st * scale[n : n + 1, :]).astype(BF16)
            tail = dot(normed, w_turned[l, :, : w_rows.shape[1]])
            tail = jnp.concatenate([with_squares(tail[:, :LANES], squares), tail[:, LANES:]], axis=1)
            t_send[n, block] = tail.astype(BF16)
            if k:
                part(n, 0, k).start()
            u_send[n, block] = dot(normed, w_flat[l, 1]).astype(BF16)
            if k:
                part(n, 1, k).start()
            z_send[n, block] = dot(normed, w_flat[l, 0]).astype(BF16)
            if k:
                part(n, 2, k).start()
            q_send[n, block] = dot(normed, w_turned[l, :, w_rows.shape[1] :]).astype(BF16)
            if k:
                part(n, 3, k).start()

        order = [0, *turns]
        gather(order[0])
        if l + 1 < layers:
            fetched(l + 1, 0)
            w_turned[l, :, : w_rows.shape[1]] = w_rows[l + 1].T
            w_turned[l, :, w_rows.shape[1] :] = w_sorted[l + 1].T
        receive(order[0])
        gather(order[1])
        for n in range(2, len(order)):
            gather(order[n])
            receive(order[n - 1])
        receive(order[-1])

    for c in sends:
        c.wait_send()
    swap.wait_send()
    for l in range(layers):
        if l == 0:
            for i, j in others:
                remote(m_send.at[l, 0, 0], m_recv.at[l, 0], m_rs, at(i, j)).wait_send()
        else:
            for which in range(2):
                for k in [*[2 * j for j in z_peers], 1]:
                    fetch(l, k, which).wait_send()
                for j in z_peers:
                    relay(l, j, which).wait_send()
        for k in dp_peers:
            for p in range(4):
                part(l, p, k).wait_send()
        for i, k in [(1, 0)] + [(i, k) for k in turns for i in (0, 1)]:
            remote(
                h_recv.at[l, 0, 0], h_recv.at[l, i, k], h_rs.at[l, k], at(i, k)
            ).wait_send()
        for k in range(n_dp):
            for j in z_peers:
                remote(
                    o_send.at[l, k], o_recv.at[l, j, k], o_rs.at[l, k], at(2 * j, 0)
                ).wait_send()
            remote(nb.at[l, 0, 0], nb.at[l, 0, 0], n_rs.at[l, k], at(1, 0)).wait_send()


def finish(stream, kept_u, kept_m, ssm, stream_out, kept_u_out, kept_m_out, ssm_out, sems):
    pairs = ((ssm, ssm_out), (stream, stream_out), (kept_u, kept_u_out), (kept_m, kept_m_out))
    step = stream.shape[0] // 4
    for i, j in [(i, j) for i in range(ssm.shape[0]) for j in range(ssm.shape[1])]:
        pltpu.make_async_copy(ssm.at[i, j], ssm_out.at[i, j], sems.at[0]).start()
    for i in range(0, stream.shape[0], step):
        pltpu.make_async_copy(stream.at[i : i + step], stream_out.at[i : i + step], sems.at[1]).start()
    for i in (2, 3):
        pltpu.make_async_copy(*pairs[i], sems.at[i]).start()
    for i, pair in enumerate(pairs):
        pltpu.make_async_copy(*pair, sems.at[i]).wait()


def fits(layers, n_tp, n_dp, heads, hp_cols, map_cols, n_state, rows, d_here, keep):
    groups = map_cols * n_tp // n_state
    powers = all(n & (n - 1) == 0 for n in (n_tp, n_dp, groups, map_cols // groups))
    return (
        powers and layers > 1 and n_tp > 2 and n_dp > 2 and n_tp * n_dp <= 64 and n_tp % groups == 0 and map_cols % groups == 0
        and hp_cols % LANES == 0 and 2 * map_cols == LANES and n_state == LANES
        and rows * 2 * (map_cols // groups) == 8 * LANES and d_here % (2 * LANES) == 0
        and keep <= FRONT and heads <= LANES - 2
    )


def body(n_tp, n_dp, *args):
    (
        tokens, lengths, input_norm_scale, gate_input_weight, maps_weight, step_weight,
        input_tap_weight, map_tap_weight, step_size_bias, decay_rate_logarithm, direct_path_weight,
        head_norm_scale, output_weight, convolution_input_cache, convolution_map_cache,
        recurrent_state, extra_log_decay,
    ) = args
    layers, seqs, slots, heads = extra_log_decay.shape
    head_size, n_state = recurrent_state.shape[3:]
    hp_cols = heads * head_size
    map_cols = maps_weight.shape[3]
    rows = seqs * slots
    d_here = tokens.shape[1]
    keep = convolution_input_cache.shape[2]
    if not fits(layers, n_tp, n_dp, heads, hp_cols, map_cols, n_state, rows, d_here, keep):
        return general_body(n_tp, n_dp, *args)
    groups = map_cols * n_tp // n_state
    n_z = n_tp // 2
    taps_n = keep + 1
    n_rows = -(-layers * (seqs * keep + taps_n) // 8) * 8

    state = recurrent_state.reshape(layers, seqs, hp_cols, n_state)
    operands = [
        lengths, tokens, input_norm_scale, gate_input_weight,
        jnp.transpose(maps_weight, (0, 2, 3, 1)).reshape(layers, 2 * map_cols, d_here),
        jnp.transpose(step_weight, (0, 2, 1)),
        input_tap_weight, map_tap_weight, step_size_bias, decay_rate_logarithm, direct_path_weight, head_norm_scale,
        jnp.transpose(convolution_input_cache, (0, 2, 1, 3)), convolution_map_cache,
        jnp.transpose(extra_log_decay, (0, 1, 3, 2)), state, output_weight,
    ]
    vmem = pl.BlockSpec(memory_space=pltpu.VMEM)
    hbm = pl.BlockSpec(memory_space=pltpu.HBM)
    sems = lambda *n: pltpu.SemaphoreType.DMA((layers, *n))
    held = [pltpu.VMEM(a.shape, a.dtype) for a in operands[1:-1]]
    held[2] = pltpu.VMEM((layers, hp_cols // LANES, d_here, 2, LANES), BF16)
    results = (
        jax.ShapeDtypeStruct(tokens.shape, F32),
        jax.ShapeDtypeStruct((layers, keep, seqs, hp_cols), BF16),
        jax.ShapeDtypeStruct((layers, seqs, keep, 2, map_cols), BF16),
        jax.ShapeDtypeStruct(state.shape, F32),
    )
    made = pl.pallas_call(
        functools.partial(
            kernel, n_tp, n_dp, d_here * n_dp, groups,
            (layers, seqs, slots, heads, head_size, n_state, hp_cols, map_cols),
        ),
        out_shape=results,
        in_specs=[hbm] * len(operands),
        out_specs=(vmem,) * len(results),
        scratch_shapes=[
            pltpu.SMEM(lengths.shape, jnp.int32),
            *held,
            pltpu.VMEM((layers, 2, hp_cols, d_here // 2), BF16),
            sems(),
            pltpu.VMEM(state.shape, BF16),
            *[
                pltpu.VMEM((layers, n, rows, width), BF16)
                for width in (LANES + 2 * n_state, hp_cols, hp_cols, LANES)
                for n in (n_dp, n_dp - 1)
            ],
            pltpu.VMEM((layers, groups, n_dp, 8, LANES), BF16),
            pltpu.VMEM((layers, n_dp * n_tp, 8, LANES), BF16),
            pltpu.VMEM((groups, 2 * n_rows, LANES), BF16),
            pltpu.VMEM((n_tp, 2 * n_rows, LANES), BF16),
            pltpu.VMEM((layers, 2, n_dp, rows, hp_cols), BF16),
            pltpu.VMEM((layers, n_dp, rows, d_here // 2), BF16),
            pltpu.VMEM((layers, n_z, n_dp, rows, d_here // 2), BF16),
            pltpu.VMEM((layers, 2, n_dp, rows, d_here // 2), BF16),
            pltpu.VMEM((layers, seqs, FRONT + slots, hp_cols), F32),
            pltpu.VMEM((layers, seqs, FRONT + slots, 2 * n_state), F32),
            pltpu.VMEM((2, n_rows, LANES), F32),
            pltpu.VMEM((n_rows, 2 * n_state), F32),
            pltpu.VMEM((layers, LANES + 2 * n_state, d_here), BF16),
            pltpu.VMEM((layers, LANES, d_here), BF16),
            pltpu.VMEM((layers - 1, 2, d_here, hp_cols), BF16),
            pltpu.VMEM((layers - 1, d_here, 2 * LANES + 2 * n_state), BF16),
            pltpu.VMEM((layers, 8, hp_cols), F32),
            pltpu.VMEM((layers, 8, LANES), F32),
            pltpu.VMEM((layers, LANES, LANES), F32),
            pltpu.SemaphoreType.DMA,
            sems(4),
            pltpu.SemaphoreType.DMA,
            pltpu.SemaphoreType.DMA,
            sems(n_dp),
            sems(n_dp),
            sems(n_dp),
            pltpu.SemaphoreType.DMA,
            pltpu.SemaphoreType.DMA((2 * (layers - 1),)),
        ],
        compiler_params=pltpu.CompilerParams(
            collective_id=0, has_side_effects=True, vmem_limit_bytes=32 * 2**20
        ),
        name="mixer",
    )(*[pltpu.with_memory_space_constraint(a, pltpu.HBM) for a in operands])
    stream, conv_in, conv_maps, ssm = pl.pallas_call(
        finish,
        out_shape=results,
        in_specs=[vmem] * len(results),
        out_specs=(hbm,) * len(results),
        scratch_shapes=[pltpu.SemaphoreType.DMA((len(results),))],
        compiler_params=pltpu.CompilerParams(vmem_limit_bytes=2**20),
        name="finish",
    )(*made)
    return stream, jnp.transpose(conv_in, (0, 2, 1, 3)), conv_maps, ssm.reshape(recurrent_state.shape)


def solution(mesh):
    placed = (
        P(None, "dp"),
        P("dp"),
        P(None, "dp"),
        P(None, "dp", None, "tp"),
        P(None, "dp", None, "tp"),
        P(None, "dp", "tp"),
        P(None, None, "tp"),
        P(None, None, None, "tp"),
        P(None, "tp"),
        P(None, "tp"),
        P(None, "tp"),
        P(None, "tp"),
        P(None, "tp", "dp"),
        P(None, "dp", None, "tp"),
        P(None, "dp", None, None, "tp"),
        P(None, "dp", "tp", None, None),
        P(None, "dp", None, "tp"),
    )
    return jax.shard_map(
        functools.partial(body, mesh.shape["tp"], mesh.shape["dp"]),
        mesh=mesh,
        in_specs=placed,
        out_specs=(
            P(None, "dp"),
            P(None, "dp", None, "tp"),
            P(None, "dp", None, None, "tp"),
            P(None, "dp", "tp", None, None),
        ),
        check_vma=False,
    )
```
